512 devices in a mesh: sp: 64 (over z, y), tp: 8 (over x, core).
Axes of the slice: x: 4, y: 4, z: 16, core: 2. Of those that a mesh axis runs over, the one named last changes fastest.
Arguments:
- tokens: bfloat16 [49152, 2048], P(('sp', 'tp')), may hold values from -6 to 6
- input_gain: float32 [2048], replicated, may hold values from 0.1 to 1.9
- branch_value: bfloat16 [2048, 1024], P('sp', 'tp'), may hold values from -0.125 to 0.125
- branch_gate: bfloat16 [2048, 1024], P('sp', 'tp'), may hold values from -0.125 to 0.125
- query_weight: bfloat16 [2048, 1024], P('sp', 'tp'), may hold values from -0.125 to 0.125
- key_weight: bfloat16 [2048, 1024], P('sp', 'tp'), may hold values from -0.125 to 0.125
- value_weight: bfloat16 [2048, 1024], P('sp', 'tp'), may hold values from -0.125 to 0.125
- swish_weight: bfloat16 [2048, 1024], P('sp', 'tp'), may hold values from -0.125 to 0.125
- kernel_taps: float32 [31, 1024], P(None, 'tp'), may hold values from -8 to 8
- channel_gain: float32 [1024], P('tp'), may hold values from 0.1 to 1.9
- decay_logs: float32 [16, 49152], P('tp', 'sp'), may hold values from -1.5 to 0
- start_state: float32 [2, 16, 64, 64], P(None, 'tp')
- head_gain: float32 [1024], P('tp'), may hold values from 0.1 to 1.9
- output_conv: bfloat16 [1024, 2048], P('tp', 'sp'), may hold values from -0.125 to 0.125
- output_heads: bfloat16 [1024, 2048], P('tp', 'sp'), may hold values from -0.125 to 0.125
Outputs:
- mixed: bfloat16 [49152, 2048], P(('sp', 'tp'))
The draws below stay inside these ranges and needn't reach their ends.
All inputs are finite; a program needn't handle non-finite values.
Results may differ from the reference program's by a relative error of at most 0.018.
Values may be sent and summed in bfloat16 or wider, within the bound.
No kernel may reach another device: no remote copies, remote signals or barrier semaphores. Data moves between devices by JAX's collectives and lax.ppermute only.
A program may use at most 64 MiB of HBM per device.

```python
import math
import jax
import jax.numpy as jnp
from jax import lax

D = 2048
DC = 1024
HEADS = 16
HD = 64
TAPS = 31
BLOCK = 256
TOKENS = 49152
N_TP = 8


def draw_kernel_taps(key, part):
    first_key = jax.random.fold_in(key, 0)
    ramp = jnp.exp(math.log(10.0) * jnp.arange(DC, dtype=jnp.float32) / (DC - 1))
    base = jnp.clip(jax.random.normal(first_key, (TAPS, DC), jnp.float32), -4.0, 4.0)
    return base * ramp[None, :] / math.sqrt(TAPS)


def draw_decay_logs(key, part):
    subkeys = jax.random.split(key, 6)
    ranking = jax.random.permutation(subkeys[0], HEADS)
    fast_count = HEADS // 2
    fast_mask = ranking < fast_count
    fast_rate = jnp.exp(jax.random.uniform(subkeys[1], (HEADS,), jnp.float32, math.log(0.01), math.log(1.0 / 30.0)))
    slow_rate = jnp.exp(jax.random.uniform(subkeys[2], (HEADS,), jnp.float32, math.log(0.15), math.log(0.4))) / TOKENS
    base_rate = jnp.where(fast_mask, fast_rate, slow_rate)
    block_count = TOKENS // BLOCK
    factor = jnp.exp(jax.random.uniform(subkeys[3], (HEADS, block_count), jnp.float32, math.log(0.5), math.log(2.0)))
    decay_factors = jnp.repeat(base_rate[:, None] * factor, BLOCK, axis=1)
    segment_locations = jax.random.randint(subkeys[4], (HEADS, 2), 0, TOKENS)
    decay_amounts = jnp.log(jax.random.uniform(subkeys[5], (HEADS, 2), jnp.float32, 0.5, 0.8))
    token_positions = jnp.arange(TOKENS, dtype=jnp.int32)
    token_segments = jnp.sum(jnp.where(token_positions[None, None, :] == segment_locations[:, :, None], decay_amounts[:, :, None], 0.0), axis=1)
    return token_segments - decay_factors


def draw_start_state(key, part):
    magnitude = math.sqrt(TOKENS) / 4.0
    base = jnp.clip(jax.random.normal(key, (2, HEADS, HD, HD), jnp.float32), -4.0, 4.0)
    return base * magnitude


def shard_levels(rng, extent, cuts, least, largest):
    factor_of = 1.0
    for position, shards_of in cuts:
        draws = jax.random.uniform(jax.random.fold_in(jax.random.fold_in(rng, 6), position), (shards_of,), jnp.float32, least / len(cuts), largest / len(cuts))
        factor_of = factor_of * jnp.repeat(jnp.exp(draws), extent[position] // shards_of).reshape((-1,) + (1,) * (len(extent) - 1 - position))
    return factor_of


def scatter_about(own_key, extent, scale, limit, shards=(), kind=jnp.bfloat16):
    gain = shard_levels(own_key, extent, shards, -0.22, 0.18) if shards else 1.0
    values = jax.random.normal(own_key, extent, jnp.float32) * scale * gain
    return jnp.minimum(jnp.maximum(values, -limit), limit).astype(kind)


def setup_inputs(seed: int = 0) -> dict:
    key_list = jax.random.split(jax.random.key(seed), 16)
    tokens = scatter_about(key_list[0], (TOKENS, D), 1.0, 6.0, ((0, 512),))
    input_gain = jnp.clip(1.0 + 0.18 * jax.random.normal(key_list[1], (D,), jnp.float32), 0.1, 1.9)
    branch_value = scatter_about(key_list[2], (D, DC), D ** -0.5, 0.125, ((0, 64), (1, 8)))
    branch_gate = scatter_about(key_list[3], (D, DC), D ** -0.5, 0.125, ((0, 64), (1, 8)))
    query_weight = scatter_about(key_list[4], (D, HEADS * HD), D ** -0.5, 0.125, ((0, 64), (1, 8)))
    key_weight = scatter_about(key_list[5], (D, HEADS * HD), D ** -0.5, 0.125, ((0, 64), (1, 8)))
    value_weight = scatter_about(key_list[6], (D, HEADS * HD), D ** -0.5, 0.125, ((0, 64), (1, 8)))
    swish_weight = scatter_about(key_list[7], (D, HEADS * HD), D ** -0.5, 0.125, ((0, 64), (1, 8)))
    kernel_taps = draw_kernel_taps(jax.random.fold_in(key_list[15], 71), 0)
    channel_gain = jnp.clip(1.0 + 0.18 * jax.random.normal(key_list[9], (DC,), jnp.float32), 0.1, 1.9)
    decay_logs = draw_decay_logs(jax.random.fold_in(key_list[15], 71), 0)
    start_state = draw_start_state(jax.random.fold_in(key_list[15], 71), 0)
    head_gain = jnp.clip(1.0 + 0.18 * jax.random.normal(key_list[12], (HEADS * HD,), jnp.float32), 0.1, 1.9)
    output_conv = scatter_about(key_list[13], (DC, D), (DC + HEADS * HD) ** -0.5, 0.125, ((0, 8), (1, 64)))
    output_heads = scatter_about(key_list[14], (HEADS * HD, D), (DC + HEADS * HD) ** -0.5, 0.125, ((0, 8), (1, 64)))
    return dict(tokens=tokens, input_gain=input_gain, branch_value=branch_value, branch_gate=branch_gate, query_weight=query_weight, key_weight=key_weight, value_weight=value_weight, swish_weight=swish_weight, kernel_taps=kernel_taps, channel_gain=channel_gain, decay_logs=decay_logs, start_state=start_state, head_gain=head_gain, output_conv=output_conv, output_heads=output_heads)


EPSILON = 1e-06
HIGHEST = lax.Precision.HIGHEST

def block_states(scaled_keys, values_block, running):
    closing = running[:, :, -1:]
    totals = jnp.exp(closing[:, :, 0])
    toward_end = jnp.exp(closing - running).transpose(0, 2, 1)[:, :, :, None]
    from_start = jnp.exp(running).transpose(0, 2, 1)[:, :, :, None]
    forward = jnp.einsum('nshd,nshe->nhde', scaled_keys * toward_end, values_block, precision=HIGHEST)
    backward = jnp.einsum('nshd,nshe->nhde', scaled_keys * from_start, values_block, precision=HIGHEST)
    return (totals, forward, backward)

def block_outputs(queries, scaled_keys, values_block, running, forward_in, backward_in):
    length = queries.shape[1]
    scores = jnp.einsum('nthd,nshd->nhts', queries, scaled_keys, precision=HIGHEST)
    distance = jnp.abs(running[:, :, :, None] - running[:, :, None, :])
    weights = jnp.exp(-distance) + jnp.eye(length, dtype=jnp.float32)
    within = jnp.einsum('nhts,nshe->nthe', scores * weights, values_block, precision=HIGHEST)
    from_start = jnp.exp(running).transpose(0, 2, 1)[:, :, :, None]
    toward_end = jnp.exp(running[:, :, -1:] - running).transpose(0, 2, 1)[:, :, :, None]
    earlier = jnp.einsum('nthd,nhde->nthe', queries, forward_in, precision=HIGHEST)
    after_part = jnp.einsum('nthd,nhde->nthe', queries, backward_in, precision=HIGHEST)
    return within + from_start * earlier + toward_end * after_part

def head_output(retained, gates_in, head_gain):
    row_count = retained.shape[0]
    centred = retained - lax.optimization_barrier(jnp.mean(retained, axis=2, keepdims=True))
    scaled = centred * lax.rsqrt(lax.optimization_barrier(jnp.mean(centred * centred, axis=2, keepdims=True)) + EPSILON)
    flattened = scaled.reshape(row_count, -1) * head_gain[None, :]
    return (flattened * jax.nn.silu(gates_in.astype(jnp.float32))).astype(jnp.bfloat16)

def reference(tokens, input_gain, branch_value, branch_gate, query_weight, key_weight, value_weight, swish_weight, kernel_taps, channel_gain, decay_logs, start_state, head_gain, output_conv, output_heads):
    widened = tokens.astype(jnp.float32)
    inverse = lax.rsqrt(lax.optimization_barrier(jnp.mean(widened * widened, axis=1, keepdims=True)) + EPSILON)
    normed = (widened * inverse * input_gain[None, :]).astype(jnp.bfloat16)

    def project(weight):
        return jnp.dot(normed, weight, preferred_element_type=jnp.float32)
    gated_rows = (project(branch_value) * jax.nn.sigmoid(project(branch_gate))).astype(jnp.bfloat16)
    queries_in = project(query_weight).astype(jnp.bfloat16)
    keys_in = project(key_weight).astype(jnp.bfloat16)
    values_in = project(value_weight).astype(jnp.bfloat16)
    gates_in = project(swish_weight).astype(jnp.bfloat16)
    half_width = TAPS // 2
    padded = jnp.pad(gated_rows.astype(jnp.float32), ((half_width, half_width), (0, 0)))
    convolved = jnp.zeros((TOKENS, DC), jnp.float32)
    for offset in range(TAPS):
        convolved = convolved + kernel_taps[offset][None, :] * padded[offset:offset + TOKENS]
    average = lax.optimization_barrier(jnp.mean(convolved, axis=1, keepdims=True))
    squares = lax.optimization_barrier(jnp.mean(convolved * convolved, axis=1, keepdims=True))
    normalized = (convolved - average) * lax.rsqrt(squares - average * average + EPSILON)
    branch_out = jax.nn.silu(normalized * channel_gain[None, :]).astype(jnp.bfloat16)
    blocks = TOKENS // BLOCK

    def split_heads(matrix):
        return matrix.astype(jnp.float32).reshape(blocks, BLOCK, HEADS, HD)
    query_blocks = split_heads(queries_in)
    key_blocks = split_heads(keys_in) * HD ** (-0.5)
    value_blocks = split_heads(values_in)
    running = jnp.cumsum(decay_logs.reshape(HEADS, blocks, BLOCK).transpose(1, 0, 2), axis=2)
    totals, forward, backward = block_states(key_blocks, value_blocks, running)

    def carry_step(carried, member):
        return (member[0][:, None, None] * carried + member[1], carried)
    final_forward, forward_in = lax.scan(carry_step, start_state[0], (totals, forward))
    final_backward, backward_in = lax.scan(carry_step, start_state[1], (totals, backward), reverse=True)

    def one_block(member):
        result = block_outputs(member[0][None], member[1][None], member[2][None], member[3][None], member[4][None], member[5][None])
        return result[0]
    retained = lax.map(one_block, (query_blocks, key_blocks, value_blocks, running, forward_in, backward_in))
    retained = retained.reshape(TOKENS, HEADS, HD)
    heads_out = head_output(retained, gates_in, head_gain)
    conv_group = DC // N_TP
    head_group = HEADS * HD // N_TP
    summed = jnp.zeros((TOKENS, D), jnp.float32)
    for group_index in range(N_TP):
        conv_slice = slice(group_index * conv_group, (group_index + 1) * conv_group)
        head_slice = slice(group_index * head_group, (group_index + 1) * head_group)
        partial_sum = jnp.dot(branch_out[:, conv_slice], output_conv[conv_slice], preferred_element_type=jnp.float32)
        partial_sum = partial_sum + jnp.dot(heads_out[:, head_slice], output_heads[head_slice], preferred_element_type=jnp.float32)
        rounded = lax.optimization_barrier(partial_sum.astype(jnp.bfloat16))
        summed = summed + rounded.astype(jnp.float32)
    return summed.astype(jnp.bfloat16)
```

```python
import jax
import jax.numpy as jnp
from jax import lax
from jax.experimental import pallas as pl
from jax.experimental.pallas import tpu as pltpu
from jax.sharding import Mesh
from jax.sharding import PartitionSpec as P

DC = 1024
EPSILON = 1e-06
F32 = jnp.float32
BF16 = jnp.bfloat16
SP = ("zh", "zl", "y")
ALL = ("zh", "zl", "y", "x", "c")
NT = (((1,), (1,)), ((), ()))
TN = (((0,), (0,)), ((), ()))
VMEM = pl.BlockSpec(memory_space=pltpu.VMEM)
SMEM = pl.BlockSpec(memory_space=pltpu.SMEM)


def call(kernel, out_shape, scalars, arrays, scratch=(), name=None):
    return pl.pallas_call(
        kernel,
        out_shape=out_shape,
        in_specs=[SMEM] * len(scalars) + [VMEM] * len(arrays),
        out_specs=jax.tree.map(lambda _: VMEM, out_shape),
        scratch_shapes=scratch,
        compiler_params=pltpu.CompilerParams(vmem_limit_bytes=56 * 1024 * 1024),
        name=name,
    )(*scalars, *arrays)


def shape(dims, dtype):
    return jax.ShapeDtypeStruct(dims, dtype)


def swap_groups(read, write, rows):
    group = lax.broadcasted_iota(jnp.int32, (rows, 128), 1) // 32
    for outer in range(4):
        for inner in range(4):
            made = None
            for k in range(4):
                moved = read(outer, k)
                turn = ((k - inner) * 32) % 128
                if turn:
                    moved = pltpu.roll(moved, turn, 1)
                made = moved if made is None else jnp.where(group == k, moved, made)
            write(outer, inner, made)


def norm_kernel(tokens, gain, out):
    rows = 16

    def step(i, carry):
        at = pl.ds(pl.multiple_of(i * rows, rows), rows)
        x = tokens[at, :].astype(F32)
        inverse = lax.rsqrt(jnp.mean(x * x, axis=1, keepdims=True) + EPSILON)
        normed = x * inverse * gain[...]

        def read(zq, zi):
            z = zq * 4 + zi
            return normed[:, z * 128 : z * 128 + 128]

        def write(zq, y, made):
            where = (y * 4 + zq) * 128
            made = made.astype(BF16)
            for copy in range(4):
                out[copy, at, where : where + 128] = made

        swap_groups(read, write, rows)
        return carry

    lax.fori_loop(0, 6, step, 0)


def last_kernel(parts, out):
    rows = 16

    def step(i, carry):
        at = pl.ds(pl.multiple_of(i * rows, rows), rows)
        total = parts[0, at, :].astype(F32)
        for k in range(1, 4):
            total = total + parts[k, at, :].astype(F32)

        def read(zq, y):
            where = (y * 4 + zq) * 128
            return total[:, where : where + 128]

        def write(zq, zi, made):
            where = (zq * 4 + zi) * 128
            out[at, where : where + 128] = made.astype(BF16)

        swap_groups(read, write, rows)
        return carry

    lax.fori_loop(0, 6, step, 0)


def lane_is_second(rows):
    return lax.broadcasted_iota(jnp.int32, (rows, 128), 1) >= 64


def by_lane(running):
    turned = jnp.transpose(running)
    return jnp.where(lane_is_second(turned.shape[0]), turned[:, 1:2], turned[:, 0:1])


def put_rows(core, own, other, targets):
    for k in range(4):
        mine = pl.ds(pl.multiple_of(k * 192 + core * 96, 32), 96)
        theirs = pl.ds(pl.multiple_of(k * 192 + (1 - core) * 96, 32), 96)
        part = slice(k * 96, k * 96 + 96)
        for n, target in enumerate(targets):
            lanes = slice(n * 128, n * 128 + 128)
            target[mine, :] = own[part, lanes].astype(BF16)
            target[theirs, :] = other[part, lanes].astype(BF16)


def states_kernel(core, own, other, weight, running, keys, values, message):
    w = weight[...]
    put_rows(
        core[0],
        jnp.dot(own[...], w, preferred_element_type=F32),
        jnp.dot(other[...], w, preferred_element_type=F32),
        (keys, values),
    )
    logs = by_lane(running[...])
    closing = logs[767:768, :]
    k = keys[...].astype(F32) * 0.125
    v = values[...]
    second = lane_is_second(64)
    ahead = lax.dot_general(
        (k * jnp.exp(closing - logs)).astype(BF16), v, TN, preferred_element_type=F32
    )
    back = lax.dot_general((k * jnp.exp(logs)).astype(BF16), v, TN, preferred_element_type=F32)
    message[0:64, :] = jnp.where(second, ahead[64:, :], ahead[:64, :]).astype(BF16)
    message[64:128, :] = jnp.where(second, back[64:, :], back[:64, :]).astype(BF16)
    message[128:144, :] = log_rows(closing)


def log_rows(log):
    high = log.astype(BF16)
    low = (log - high.astype(F32)).astype(BF16)
    first = lax.broadcasted_iota(jnp.int32, (16, 128), 0) < 8
    return jnp.where(first, high.astype(F32), low.astype(F32)).astype(BF16)


def scan_states(gathered, count, position):
    def log_of(m):
        return gathered[m, 128:129, :].astype(F32) + gathered[m, 136:137, :].astype(F32)

    def one_way(order, rows):
        state = jnp.zeros((64, 128), F32)
        log = jnp.zeros((1, 128), F32)
        held, held_log = state, log
        for m in order:
            here = position == m
            held = jnp.where(here, state, held)
            held_log = jnp.where(here, log, held_log)
            own = log_of(m)
            state = jnp.exp(own) * state + gathered[m, rows, :].astype(F32)
            log = log + own
        return held, held_log, state, log

    ahead = one_way(range(count), slice(0, 64))
    back = one_way(reversed(range(count)), slice(64, 128))
    return ahead, back


def level_kernel(position, gathered, inside, message):
    ahead, back = scan_states(gathered, 16, position[0])
    inside[0:64, :] = ahead[0]
    inside[64:128, :] = back[0]
    inside[128:136, :] = jnp.broadcast_to(ahead[1], (8, 128))
    inside[136:144, :] = jnp.broadcast_to(back[1], (8, 128))
    message[0:64, :] = ahead[2].astype(BF16)
    message[64:128, :] = back[2].astype(BF16)
    message[128:144, :] = log_rows(ahead[3])


def column_block(position, shift):
    return pl.ds(pl.multiple_of(((position + 4 - shift) % 4) * 512, 512), 512)


def by_piece(y, rows, pieces, lanes):
    total = None
    for shift, piece in enumerate(pieces):
        part = jnp.dot(
            rows[:, column_block(y, shift)], piece[:, lanes], preferred_element_type=F32
        )
        total = part if total is None else total + part
    return total


def gate_kernel(core, y, own, other, p0, p1, p2, p3, gated):
    pieces = (p0, p1, p2, p3)

    def rows_of(rows):
        both = by_piece(y[0], rows, pieces, slice(0, 256))
        return both[:, :128] * jax.nn.sigmoid(both[:, 128:])

    put_rows(core[0], rows_of(own), rows_of(other), (gated,))


def conv_kernel(before, gated, after, taps, convolved, moments, padded):
    padded[0:16, :] = before[...].astype(F32)
    padded[16:784, :] = gated[...].astype(F32)
    padded[784:800, :] = after[...].astype(F32)
    ones = jnp.ones((8, 128), F32)
    rows = 128
    for i in range(6):
        total = None
        for j in range(31):
            start = i * rows + j + 1
            term = taps[j : j + 1, :] * padded[start : start + rows, :]
            total = term if total is None else total + term
        convolved[i * rows : (i + 1) * rows, :] = total
        highest = lax.Precision.HIGHEST
        s1 = lax.dot_general(ones, total, NT, precision=highest, preferred_element_type=F32)
        s2 = lax.dot_general(ones, total * total, NT, precision=highest, preferred_element_type=F32)
        moments[0:1, i * rows : (i + 1) * rows] = s1[0:1]
        moments[1:2, i * rows : (i + 1) * rows] = s2[0:1]


def within_kernel(
    core, y, own, other, p0, p1, p2, p3, keys, values, running, queries, gates, within
):
    pieces = (p0, p1, p2, p3)
    put_rows(
        core[0],
        by_piece(y[0], own, pieces, slice(0, 256)),
        by_piece(y[0], other, pieces, slice(0, 256)),
        (queries, gates),
    )
    logs = running[...]
    turned = jnp.transpose(logs)
    k = (keys[...].astype(F32) * 0.125).astype(BF16)
    v = values[...]
    rows = 128
    zero = jnp.zeros((), BF16)
    masks = [lane_is_second(768) == bool(h) for h in range(2)]
    head_values = [jnp.where(mask, v, zero) for mask in masks]
    for i in range(6):
        at = slice(i * rows, (i + 1) * rows)
        q = queries[at, :]
        diagonal = lax.broadcasted_iota(jnp.int32, (rows, 768), 1) == (
            lax.broadcasted_iota(jnp.int32, (rows, 768), 0) + i * rows
        )
        total = None
        for h in range(2):
            scores = lax.dot_general(
                jnp.where(masks[h][:rows], q, zero), k, NT, preferred_element_type=F32
            )
            distance = jnp.abs(turned[at, h : h + 1] - logs[h : h + 1, :])
            weights = jnp.exp(-distance) + jnp.where(diagonal, 1.0, 0.0)
            part = jnp.dot(
                (scores * weights).astype(BF16), head_values[h], preferred_element_type=F32
            )
            total = part if total is None else total + part
        within[at, :] = total


def out_rows(y, rows, pieces, write):
    for shift, piece in enumerate(pieces):
        part = lax.dot_general(rows, piece[:, 256:512], NT, preferred_element_type=F32)
        write(column_block(y, shift), part)


def mixers_kernel(
    core,
    y,
    position,
    queries,
    gates,
    within,
    running,
    gathered,
    inside,
    start,
    head_gain,
    convolved,
    moments,
    channel_gain,
    p0,
    p1,
    p2,
    p3,
    mine,
    sent,
    rows_in,
):
    ahead, back = scan_states(gathered, 4, position[0])
    forward = inside[0:64, :] + jnp.exp(inside[128:129, :]) * (
        ahead[0] + jnp.exp(ahead[1]) * start[0:64, :]
    )
    backward = inside[64:128, :] + jnp.exp(inside[136:137, :]) * (
        back[0] + jnp.exp(back[1]) * start[64:128, :]
    )
    second = lane_is_second(64)

    def diagonal_blocks(state):
        return jnp.concatenate(
            [jnp.where(second, 0.0, state), jnp.where(second, state, 0.0)], axis=0
        ).astype(BF16)

    forward, backward = diagonal_blocks(forward), diagonal_blocks(backward)
    logs = by_lane(running[...])
    closing = logs[767:768, :]
    sums = moments[0]
    for k in range(1, 8):
        sums = sums + moments[k]
    sums = jnp.transpose(jnp.concatenate([sums, jnp.zeros((6, 768), F32)], axis=0)) / DC
    rows = 128
    half = lane_is_second(rows)

    def head_mean(x):
        low = jnp.sum(jnp.where(half, 0.0, x), axis=1, keepdims=True)
        high = jnp.sum(jnp.where(half, x, 0.0), axis=1, keepdims=True)
        return jnp.where(half, high, low) / 64

    for i in range(6):
        at = slice(i * rows, (i + 1) * rows)
        average, squares = sums[at, 0:1], sums[at, 1:2]
        scaled = (convolved[at, :] - average) * lax.rsqrt(squares - average * average + EPSILON)
        rows_in[at, 0:128] = jax.nn.silu(scaled * channel_gain[...]).astype(BF16)
        q = queries[at, :]
        log = logs[at, :]
        retained = (
            within[at, :]
            + jnp.exp(log) * jnp.dot(q, forward, preferred_element_type=F32)
            + jnp.exp(closing - log) * jnp.dot(q, backward, preferred_element_type=F32)
        )
        centred = retained - head_mean(retained)
        normed = centred * lax.rsqrt(head_mean(centred * centred) + EPSILON)
        gate = jax.nn.silu(gates[at, :].astype(F32))
        rows_in[at, 128:256] = (normed * head_gain[...] * gate).astype(BF16)

    def half_of(which):
        return jnp.concatenate(
            [
                rows_in[pl.ds(pl.multiple_of(k * 192 + which * 96, 32), 96), :]
                for k in range(4)
            ],
            axis=0,
        )

    mine[...] = half_of(core[0])

    def write(lanes, part):
        sent[:, lanes] = part.astype(BF16)

    out_rows(y[0], half_of(1 - core[0]), (p0, p1, p2, p3), write)


def join_kernel(y, mine, arrived, p0, p1, p2, p3, out):
    def write(lanes, part):
        out[:, lanes] = (part + arrived[:, lanes].astype(F32)).astype(BF16)

    out_rows(y[0], mine[...], (p0, p1, p2, p3), write)


def ring(x, axis, shift):
    count = lax.axis_size(axis)
    return lax.ppermute(x, axis, [(i, (i + shift) % count) for i in range(count)])


def copies(x, axes, count):
    return lax.all_to_all(
        jnp.broadcast_to(x[None], (count, *x.shape)), axes, 0, 0, tiled=True
    )


def body(
    tokens,
    input_gain,
    branch_value,
    branch_gate,
    query_weight,
    key_weight,
    value_weight,
    swish_weight,
    kernel_taps,
    channel_gain,
    decay_logs,
    start_state,
    head_gain,
    output_conv,
    output_heads,
):
    core = lax.axis_index("c").astype(jnp.int32)[None]
    y = lax.axis_index("y").astype(jnp.int32)[None]
    high = lax.axis_index("zh").astype(jnp.int32)[None]
    low = lax.axis_index(("zl", "y")).astype(jnp.int32)[None]

    normed = call(
        norm_kernel,
        shape((4, 96, 2048), BF16),
        (),
        (tokens, input_gain[None]),
        name="norm",
    )
    own = lax.all_to_all(normed, "x", 0, 0, tiled=True).reshape(384, 2048)
    shard = jnp.concatenate(
        [
            key_weight,
            value_weight,
            branch_value,
            branch_gate,
            query_weight,
            swish_weight,
            output_conv.T,
            output_heads.T,
        ],
        axis=1,
    )
    rows = lax.all_gather(shard, ("zh", "zl"), axis=0, tiled=True)
    other = ring(own, "c", 1)
    state_weight = copies(rows[:, :256], "y", 4).reshape(2048, 256)
    gate_piece, rest_piece = rows[:, 256:512], rows[:, 512:]
    gate_pieces = (gate_piece,) + tuple(ring(gate_piece, "y", d) for d in (1, 2, 3))
    rest_pieces = (rest_piece,) + tuple(ring(rest_piece, "y", d) for d in (1, 2, 3))

    running = jnp.cumsum(decay_logs, axis=1)
    running = jnp.concatenate([running, jnp.zeros((6, 768), F32)], axis=0)
    start = start_state.transpose(0, 2, 1, 3).reshape(128, 128)

    half = shape((768, 128), BF16)
    full = shape((768, 128), F32)
    message = shape((144, 128), BF16)
    keys, values, sent = call(
        states_kernel,
        (half, half, message),
        (core,),
        (own, other, state_weight, running),
        name="states",
    )
    inside, sent = call(
        level_kernel,
        (shape((144, 128), F32), message),
        (low,),
        (copies(sent, ("zl", "y"), 16),),
        name="level",
    )
    gathered = copies(sent, "zh", 4)

    gated = call(
        gate_kernel, half, (core, y), (own, other, *gate_pieces), name="gate"
    )
    count = lax.axis_size(SP)
    before = lax.ppermute(gated[752:], SP, [(i, i + 1) for i in range(count - 1)])
    after = lax.ppermute(gated[:16], SP, [(i + 1, i) for i in range(count - 1)])
    convolved, moments = call(
        conv_kernel,
        (full, shape((2, 768), F32)),
        (),
        (before, gated, after, kernel_taps),
        scratch=(pltpu.VMEM((800, 128), F32),),
        name="conv",
    )
    moments = copies(moments, ("x", "c"), 8)
    queries, gates, within = call(
        within_kernel,
        (half, half, full),
        (core, y),
        (own, other, *rest_pieces, keys, values, running),
        name="within",
    )
    mine, sent = call(
        mixers_kernel,
        (shape((384, 256), BF16), shape((384, 2048), BF16)),
        (core, y, high),
        (
            queries,
            gates,
            within,
            running,
            gathered,
            inside,
            start,
            head_gain[None],
            convolved,
            moments,
            channel_gain[None],
            *rest_pieces,
        ),
        scratch=(pltpu.VMEM((768, 256), BF16),),
        name="mixers",
    )
    arrived = ring(sent, "c", 1)
    joined = call(
        join_kernel,
        shape((384, 2048), BF16),
        (y,),
        (mine, arrived, *rest_pieces),
        name="join",
    )
    parts = lax.all_to_all(joined.reshape(4, 96, 2048), "x", 0, 0, tiled=True)
    return call(last_kernel, shape((96, 2048), BF16), (), (parts,), name="last")


def solution(mesh):
    split = Mesh(mesh.devices.reshape(4, 4, 4, 4, 2), ALL)
    in_specs = (
        P(ALL, None),
        P(),
        P(SP, ("x", "c")),
        P(SP, ("x", "c")),
        P(SP, ("x", "c")),
        P(SP, ("x", "c")),
        P(SP, ("x", "c")),
        P(SP, ("x", "c")),
        P(None, ("x", "c")),
        P(("x", "c")),
        P(("x", "c"), SP),
        P(None, ("x", "c"), None, None),
        P(("x", "c")),
        P(("x", "c"), SP),
        P(("x", "c"), SP),
    )
    return jax.shard_map(
        body, mesh=split, in_specs=in_specs, out_specs=P(ALL, None), check_vma=False
    )
```

```python
import jax
import jax.numpy as jnp
from jax import lax
from jax.experimental import pallas as pl
from jax.experimental.pallas import tpu as pltpu
from jax.sharding import Mesh
from jax.sharding import PartitionSpec as P

DC = 1024
EPSILON = 1e-06
F32 = jnp.float32
BF16 = jnp.bfloat16
SP = ("zh", "zl", "y")
ALL = ("zh", "zl", "y", "x", "c")
NT = (((1,), (1,)), ((), ()))
TN = (((0,), (0,)), ((), ()))
VMEM = pl.BlockSpec(memory_space=pltpu.VMEM)
SMEM = pl.BlockSpec(memory_space=pltpu.SMEM)


def call(kernel, out_shape, scalars, arrays, scratch=()):
    return pl.pallas_call(
        kernel,
        out_shape=out_shape,
        in_specs=[SMEM] * len(scalars) + [VMEM] * len(arrays),
        out_specs=jax.tree.map(lambda _: VMEM, out_shape),
        scratch_shapes=scratch,
        compiler_params=pltpu.CompilerParams(vmem_limit_bytes=56 * 1024 * 1024),
    )(*scalars, *arrays)


def shape(dims, dtype):
    return jax.ShapeDtypeStruct(dims, dtype)


def swap_groups(read, write, rows):
    group = lax.broadcasted_iota(jnp.int32, (rows, 128), 1) // 32
    for outer in range(4):
        for inner in range(4):
            made = None
            for k in range(4):
                moved = read(outer, k)
                turn = ((k - inner) * 32) % 128
                if turn:
                    moved = pltpu.roll(moved, turn, 1)
                made = moved if made is None else jnp.where(group == k, moved, made)
            write(outer, inner, made)


def shard_kernel(k, v, bv, bg, q, s, oc, oh, out):
    for i, part in enumerate((k, v, bv, bg, q, s)):
        out[:, i * 128 : i * 128 + 128] = part[...]
    for i, part in ((6, oc), (7, oh)):
        out[:, i * 128 : i * 128 + 128] = jnp.transpose(part[...].astype(F32)).astype(BF16)


def norm_kernel(tokens, edge, gain, out):
    rows = 16

    def block(source, at, to):
        x = source[at, :].astype(F32)
        inverse = lax.rsqrt(jnp.mean(x * x, axis=1, keepdims=True) + EPSILON)
        normed = x * inverse * gain[...]

        def read(zl, zh):
            z = zh * 4 + zl
            return normed[:, z * 128 : z * 128 + 128]

        def write(zl, y, made):
            where = (y * 4 + zl) * 128
            made = made.astype(BF16)
            for copy in range(4):
                out[copy, to, where : where + 128] = made

        swap_groups(read, write, rows)

    def step(i, carry):
        at = pl.ds(pl.multiple_of(i * rows, rows), rows)
        block(tokens, at, at)
        return carry

    lax.fori_loop(0, 6, step, 0)
    block(edge, slice(0, 16), slice(96, 112))


def last_kernel(parts, out):
    rows = 16

    def step(i, carry):
        at = pl.ds(pl.multiple_of(i * rows, rows), rows)
        total = parts[0, at, :].astype(F32)
        for k in range(1, 4):
            total = total + parts[k, at, :].astype(F32)

        def read(zl, y):
            where = (y * 4 + zl) * 128
            return total[:, where : where + 128]

        def write(zl, zh, made):
            where = (zh * 4 + zl) * 128
            out[at, where : where + 128] = made.astype(BF16)

        swap_groups(read, write, rows)
        return carry

    lax.fori_loop(0, 6, step, 0)


def lane_is_second(rows):
    return lax.broadcasted_iota(jnp.int32, (rows, 128), 1) >= 64


def by_lane(running):
    turned = jnp.transpose(running)
    return jnp.where(lane_is_second(turned.shape[0]), turned[:, 1:2], turned[:, 0:1])


def put_rows(core, own, other, targets):
    for k in range(4):
        mine = pl.ds(pl.multiple_of(k * 192 + core * 96, 32), 96)
        theirs = pl.ds(pl.multiple_of(k * 192 + (1 - core) * 96, 32), 96)
        part = slice(k * 112, k * 112 + 96)
        for n, target in enumerate(targets):
            lanes = slice(n * 128, n * 128 + 128)
            target[mine, :] = own[part, lanes].astype(BF16)
            target[theirs, :] = other[part, lanes].astype(BF16)


def states_kernel(core, own, other, weight, running, tail, keys, values, message):
    w = weight[...]
    put_rows(
        core[0],
        jnp.dot(own[...], w, preferred_element_type=F32),
        jnp.dot(other[...], w, preferred_element_type=F32),
        (keys, values),
    )
    logs = by_lane(running[...])
    closing = logs[767:768, :]
    k = keys[...].astype(F32) * 0.125
    v = values[...]
    second = lane_is_second(64)
    ahead = lax.dot_general(
        (k * jnp.exp(closing - logs)).astype(BF16), v, TN, preferred_element_type=F32
    )
    back = lax.dot_general((k * jnp.exp(logs)).astype(BF16), v, TN, preferred_element_type=F32)
    parts = (
        (slice(0, 64), jnp.where(second, ahead[64:, :], ahead[:64, :]).astype(BF16)),
        (slice(64, 128), jnp.where(second, back[64:, :], back[:64, :]).astype(BF16)),
        (slice(128, 144), log_rows(closing)),
        (slice(144, 160), jnp.transpose(tail[...].astype(F32))[112:128, :].astype(BF16)),
    )
    for at, part in parts:
        for copy in range(16):
            message[copy, at, :] = part


def log_rows(log):
    high = log.astype(BF16)
    low = (log - high.astype(F32)).astype(BF16)
    first = lax.broadcasted_iota(jnp.int32, (16, 128), 0) < 8
    return jnp.where(first, high.astype(F32), low.astype(F32)).astype(BF16)


def scan_states(gathered, count, position):
    def log_of(m):
        return gathered[m, 128:129, :].astype(F32) + gathered[m, 136:137, :].astype(F32)

    def one_way(order, rows):
        state = jnp.zeros((64, 128), F32)
        log = jnp.zeros((1, 128), F32)
        held, held_log = state, log
        for m in order:
            here = position == m
            held = jnp.where(here, state, held)
            held_log = jnp.where(here, log, held_log)
            own = log_of(m)
            state = jnp.exp(own) * state + gathered[m, rows, :].astype(F32)
            log = log + own
        return held, held_log, state, log

    ahead = one_way(range(count), slice(0, 64))
    back = one_way(reversed(range(count)), slice(64, 128))
    return ahead, back


def level_kernel(position, gathered, inside, message, spare):
    ahead, back = scan_states(gathered, 16, position[0])
    inside[0:64, :] = ahead[0]
    inside[64:128, :] = back[0]
    inside[128:136, :] = jnp.broadcast_to(ahead[1], (8, 128))
    inside[136:144, :] = jnp.broadcast_to(back[1], (8, 128))
    parts = (
        (slice(0, 64), ahead[2].astype(BF16)),
        (slice(64, 128), back[2].astype(BF16)),
        (slice(128, 144), log_rows(ahead[3])),
    )
    for at, part in parts:
        for copy in range(4):
            message[copy, at, :] = part

    for y in range(4):
        for zl in range(4):
            where = y * 512 + zl * 128
            spare[:, where : where + 128] = gathered[zl * 4 + y, 144:160, :]


def column_block(position, shift):
    return pl.ds(pl.multiple_of(((position + 4 - shift) % 4) * 512, 512), 512)


def by_piece(y, rows, pieces, lanes):
    total = None
    for shift, piece in enumerate(pieces):
        part = jnp.dot(
            rows[:, column_block(y, shift)], piece[:, lanes], preferred_element_type=F32
        )
        total = part if total is None else total + part
    return total


def conv_kernel(core, y, own, other, p0, p1, p2, p3, taps, convolved, moments, padded):
    pieces = (p0, p1, p2, p3)

    def rows_of(rows):
        both = by_piece(y[0], rows, pieces, slice(0, 256))
        return (both[:, :128] * jax.nn.sigmoid(both[:, 128:])).astype(BF16).astype(F32)

    first, second = rows_of(own), rows_of(other)
    for k in range(4):
        mine = pl.ds(pl.multiple_of(16 + k * 192 + core[0] * 96, 16), 96)
        theirs = pl.ds(pl.multiple_of(16 + k * 192 + (1 - core[0]) * 96, 16), 96)
        padded[mine, :] = first[k * 112 : k * 112 + 96, :]
        padded[theirs, :] = second[k * 112 : k * 112 + 96, :]
    is_second = jnp.full((16, 128), core[0], jnp.int32) == 1
    padded[0:16, :] = jnp.where(is_second, first[432:448, :], second[432:448, :])
    padded[784:800, :] = jnp.where(is_second, second[96:112, :], first[96:112, :])
    ones = jnp.ones((8, 128), F32)
    rows = 128
    for i in range(6):
        total = None
        for j in range(31):
            start = i * rows + j + 1
            term = taps[j : j + 1, :] * padded[start : start + rows, :]
            total = term if total is None else total + term
        convolved[i * rows : (i + 1) * rows, :] = total
        highest = lax.Precision.HIGHEST
        s1 = lax.dot_general(ones, total, NT, precision=highest, preferred_element_type=F32)
        s2 = lax.dot_general(ones, total * total, NT, precision=highest, preferred_element_type=F32)
        moments[0:1, i * rows : (i + 1) * rows] = s1[0:1]
        moments[1:2, i * rows : (i + 1) * rows] = s2[0:1]


def within_kernel(
    core, y, own, other, p0, p1, p2, p3, keys, values, running, queries, gates, within
):
    pieces = (p0, p1, p2, p3)
    put_rows(
        core[0],
        by_piece(y[0], own, pieces, slice(0, 256)),
        by_piece(y[0], other, pieces, slice(0, 256)),
        (queries, gates),
    )
    logs = running[...]
    turned = jnp.transpose(logs)
    k = (keys[...].astype(F32) * 0.125).astype(BF16)
    v = values[...]
    rows = 128
    zero = jnp.zeros((), BF16)
    masks = [lane_is_second(768) == bool(h) for h in range(2)]
    head_values = [jnp.where(mask, v, zero) for mask in masks]
    for i in range(6):
        at = slice(i * rows, (i + 1) * rows)
        q = queries[at, :]
        diagonal = lax.broadcasted_iota(jnp.int32, (rows, 768), 1) == (
            lax.broadcasted_iota(jnp.int32, (rows, 768), 0) + i * rows
        )
        total = None
        for h in range(2):
            scores = lax.dot_general(
                jnp.where(masks[h][:rows], q, zero), k, NT, preferred_element_type=F32
            )
            distance = jnp.abs(turned[at, h : h + 1] - logs[h : h + 1, :])
            weights = jnp.exp(-distance) + jnp.where(diagonal, 1.0, 0.0)
            part = jnp.dot(
                (scores * weights).astype(BF16), head_values[h], preferred_element_type=F32
            )
            total = part if total is None else total + part
        within[at, :] = total


def out_rows(y, rows, pieces, spare, write):
    for shift, piece in enumerate(pieces):
        lanes = column_block(y, shift)
        part = lax.dot_general(rows[:, :240], piece[:, 256:496], NT, preferred_element_type=F32)
        part = part + jnp.dot(rows[:, 240:], spare[:, lanes], preferred_element_type=F32)
        write(lanes, part)


def mixers_kernel(
    core,
    y,
    position,
    queries,
    gates,
    within,
    running,
    gathered,
    inside,
    start,
    head_gain,
    convolved,
    moments,
    channel_gain,
    p0,
    p1,
    p2,
    p3,
    spare,
    mine,
    sent,
    rows_in,
):
    ahead, back = scan_states(gathered, 4, position[0])
    forward = inside[0:64, :] + jnp.exp(inside[128:129, :]) * (
        ahead[0] + jnp.exp(ahead[1]) * start[0:64, :]
    )
    backward = inside[64:128, :] + jnp.exp(inside[136:137, :]) * (
        back[0] + jnp.exp(back[1]) * start[64:128, :]
    )
    second = lane_is_second(64)

    def diagonal_blocks(state):
        return jnp.concatenate(
            [jnp.where(second, 0.0, state), jnp.where(second, state, 0.0)], axis=0
        ).astype(BF16)

    forward, backward = diagonal_blocks(forward), diagonal_blocks(backward)
    logs = by_lane(running[...])
    closing = logs[767:768, :]
    sums = moments[0]
    for k in range(1, 8):
        sums = sums + moments[k]
    sums = jnp.transpose(jnp.concatenate([sums, jnp.zeros((6, 768), F32)], axis=0)) / DC
    rows = 128
    half = lane_is_second(rows)

    def head_mean(x):
        low = jnp.sum(jnp.where(half, 0.0, x), axis=1, keepdims=True)
        high = jnp.sum(jnp.where(half, x, 0.0), axis=1, keepdims=True)
        return jnp.where(half, high, low) / 64

    for i in range(6):
        at = slice(i * rows, (i + 1) * rows)
        average, squares = sums[at, 0:1], sums[at, 1:2]
        scaled = (convolved[at, :] - average) * lax.rsqrt(squares - average * average + EPSILON)
        rows_in[at, 0:128] = jax.nn.silu(scaled * channel_gain[...]).astype(BF16)
        q = queries[at, :]
        log = logs[at, :]
        retained = (
            within[at, :]
            + jnp.exp(log) * jnp.dot(q, forward, preferred_element_type=F32)
            + jnp.exp(closing - log) * jnp.dot(q, backward, preferred_element_type=F32)
        )
        centred = retained - head_mean(retained)
        normed = centred * lax.rsqrt(head_mean(centred * centred) + EPSILON)
        gate = jax.nn.silu(gates[at, :].astype(F32))
        rows_in[at, 128:256] = (normed * head_gain[...] * gate).astype(BF16)

    def half_of(which):
        return jnp.concatenate(
            [
                rows_in[pl.ds(pl.multiple_of(k * 192 + which * 96, 32), 96), :]
                for k in range(4)
            ],
            axis=0,
        )

    mine[...] = half_of(core[0])

    def write(lanes, part):
        sent[:, lanes] = part.astype(BF16)

    out_rows(y[0], half_of(1 - core[0]), (p0, p1, p2, p3), spare, write)


def join_kernel(y, mine, arrived, p0, p1, p2, p3, spare, out):
    def write(lanes, part):
        out[:, lanes] = (part + arrived[:, lanes].astype(F32)).astype(BF16)

    out_rows(y[0], mine[...], (p0, p1, p2, p3), spare, write)


def ring(x, axis, shift):
    count = lax.axis_size(axis)
    return lax.ppermute(x, axis, [(i, (i + shift) % count) for i in range(count)])


def copies(x, axes, count):
    return lax.all_to_all(
        jnp.broadcast_to(x[None], (count, *x.shape)), axes, 0, 0, tiled=True
    )


def body(
    tokens,
    input_gain,
    branch_value,
    branch_gate,
    query_weight,
    key_weight,
    value_weight,
    swish_weight,
    kernel_taps,
    channel_gain,
    decay_logs,
    start_state,
    head_gain,
    output_conv,
    output_heads,
):
    core = lax.axis_index("c").astype(jnp.int32)[None]
    y = lax.axis_index("y").astype(jnp.int32)[None]
    high = lax.axis_index("zh").astype(jnp.int32)[None]
    low = lax.axis_index(("zl", "y")).astype(jnp.int32)[None]

    place = lax.axis_index(("x", "c"))
    count = lax.axis_size(SP)
    edge = lax.ppermute(
        jnp.where(place == 7, tokens[80:96], tokens[0:16]),
        ALL,
        [(i * 8 + 7, i * 8 + 15) for i in range(count - 1)]
        + [(i * 8 + 8, i * 8) for i in range(count - 1)],
    )
    shard = call(
        shard_kernel,
        shape((32, 1024), BF16),
        (),
        (
            key_weight,
            value_weight,
            branch_value,
            branch_gate,
            query_weight,
            swish_weight,
            output_conv,
            output_heads,
        ),
    )
    normed = call(
        norm_kernel, shape((4, 112, 2048), BF16), (), (tokens, edge, input_gain[None])
    )
    shard, normed = lax.optimization_barrier((shard, normed))
    own = lax.all_to_all(normed, "x", 0, 0, tiled=True).reshape(448, 2048)
    rows = lax.all_gather(shard, "zh", axis=0, tiled=True)
    tail = rows[:, 896:]
    rows = lax.all_gather(rows[:, :1008], "zl", axis=0, tiled=True)
    own, rows = lax.optimization_barrier((own, rows))
    other = ring(own, "c", 1)
    state_weight = copies(rows[:, :256], "y", 4).reshape(2048, 256)
    gate_piece, rest_piece = rows[:, 256:512], rows[:, 512:]
    gate_pieces = (gate_piece,) + tuple(ring(gate_piece, "y", d) for d in (1, 2, 3))
    rest_pieces = (rest_piece,) + tuple(ring(rest_piece, "y", d) for d in (1, 2, 3))

    running = jnp.cumsum(decay_logs, axis=1)
    running = jnp.concatenate([running, jnp.zeros((6, 768), F32)], axis=0)
    start = start_state.transpose(0, 2, 1, 3).reshape(128, 128)

    half = shape((768, 128), BF16)
    full = shape((768, 128), F32)
    keys, values, sent = call(
        states_kernel,
        (half, half, shape((16, 160, 128), BF16)),
        (core,),
        (own, other, state_weight, running, tail),
    )
    inside, sent, spare = call(
        level_kernel,
        (shape((144, 128), F32), shape((4, 144, 128), BF16), shape((16, 2048), BF16)),
        (low,),
        (lax.all_to_all(sent, ("zl", "y"), 0, 0, tiled=True),),
    )
    gathered = lax.all_to_all(sent, "zh", 0, 0, tiled=True)

    convolved, moments = call(
        conv_kernel,
        (full, shape((2, 768), F32)),
        (core, y),
        (own, other, *gate_pieces, kernel_taps),
        scratch=(pltpu.VMEM((800, 128), F32),),
    )
    moments = lax.all_gather(moments, ("x", "c"))
    queries, gates, within = call(
        within_kernel,
        (half, half, full),
        (core, y),
        (own, other, *rest_pieces, keys, values, running),
    )
    mine, sent = call(
        mixers_kernel,
        (shape((384, 256), BF16), shape((384, 2048), BF16)),
        (core, y, high),
        (
            queries,
            gates,
            within,
            running,
            gathered,
            inside,
            start,
            head_gain[None],
            convolved,
            moments,
            channel_gain[None],
            *rest_pieces,
            spare,
        ),
        scratch=(pltpu.VMEM((768, 256), BF16),),
    )
    arrived = ring(sent, "c", 1)
    joined = call(
        join_kernel,
        shape((384, 2048), BF16),
        (y,),
        (mine, arrived, *rest_pieces, spare),
    )
    parts = lax.all_to_all(joined.reshape(4, 96, 2048), "x", 0, 0, tiled=True)
    return call(last_kernel, shape((96, 2048), BF16), (), (parts,))


def solution(mesh):
    split = Mesh(mesh.devices.reshape(4, 4, 4, 4, 2), ALL)
    in_specs = (
        P(ALL, None),
        P(),
        P(SP, ("x", "c")),
        P(SP, ("x", "c")),
        P(SP, ("x", "c")),
        P(SP, ("x", "c")),
        P(SP, ("x", "c")),
        P(SP, ("x", "c")),
        P(None, ("x", "c")),
        P(("x", "c")),
        P(("x", "c"), SP),
        P(None, ("x", "c"), None, None),
        P(("x", "c")),
        P(("x", "c"), SP),
        P(("x", "c"), SP),
    )

    return jax.shard_map(
        body, mesh=split, in_specs=in_specs, out_specs=P(ALL, None), check_vma=False
    )
```

```python
import functools

import jax
import jax.numpy as jnp
from jax import lax
from jax.experimental import pallas as pl
from jax.experimental.pallas import tpu as pltpu
from jax.sharding import Mesh
from jax.sharding import PartitionSpec as P

DC = 1024
EPSILON = 1e-06
F32 = jnp.float32
BF16 = jnp.bfloat16
SP = ("zh", "zl", "y")
ALL = ("zh", "zl", "y", "x", "c")
NT = (((1,), (1,)), ((), ()))
TN = (((0,), (0,)), ((), ()))
VMEM = pl.BlockSpec(memory_space=pltpu.VMEM)
SMEM = pl.BlockSpec(memory_space=pltpu.SMEM)


def call(kernel, out_shape, scalars, arrays, scratch=()):
    return pl.pallas_call(
        kernel,
        out_shape=out_shape,
        in_specs=[SMEM] * len(scalars) + [VMEM] * len(arrays),
        out_specs=jax.tree.map(lambda _: VMEM, out_shape),
        scratch_shapes=scratch,
        compiler_params=pltpu.CompilerParams(vmem_limit_bytes=56 * 1024 * 1024),
    )(*scalars, *arrays)


def shape(dims, dtype):
    return jax.ShapeDtypeStruct(dims, dtype)


def swap_groups(read, write, rows):
    group = lax.broadcasted_iota(jnp.int32, (rows, 128), 1) // 32
    for outer in range(4):
        for inner in range(4):
            made = None
            for k in range(4):
                moved = read(outer, k)
                turn = ((k - inner) * 32) % 128
                if turn:
                    moved = pltpu.roll(moved, turn, 1)
                made = moved if made is None else jnp.where(group == k, moved, made)
            write(outer, inner, made)


def shard_kernel(k, v, bv, bg, q, s, oc, oh, out):
    for i, part in enumerate((k, v, bv, bg, q, s, oc)):
        out[:, i * 128 : i * 128 + 128] = part[...]
    out[:, 896:1008] = oh[:, 0:112]


def norm_kernel(tokens, edge, gain, out):
    rows = 16

    def block(source, at, to):
        x = source[at, :].astype(F32)
        inverse = lax.rsqrt(jnp.mean(x * x, axis=1, keepdims=True) + EPSILON)
        normed = x * inverse * gain[...]

        def read(zh, zl):
            z = zh * 4 + zl
            return normed[:, z * 128 : z * 128 + 128]

        def write(zh, y, made):
            where = (y * 4 + zh) * 128
            made = made.astype(BF16)
            for copy in range(4):
                out[copy, to, where : where + 128] = made

        swap_groups(read, write, rows)

    def step(i, carry):
        at = pl.ds(pl.multiple_of(i * rows, rows), rows)
        block(tokens, at, at)
        return carry

    lax.fori_loop(0, 6, step, 0, unroll=2)
    block(edge, slice(0, 16), slice(96, 112))


def last_kernel(y, parts_a, parts_b, out):
    rows = 16
    group = lax.broadcasted_iota(jnp.int32, (rows, 128), 1) // 32

    def step(i, carry):
        at = pl.ds(pl.multiple_of(i * rows, rows), rows)
        totals = []
        for parts in (parts_a, parts_b):
            total = parts[0, at, :].astype(F32)
            for k in range(1, 4):
                total = total + parts[k, at, :].astype(F32)
            totals.append(total)
        for zh in range(4):
            for zl in range(4):
                made = jnp.zeros((rows, 128), F32)
                for d in range(4):
                    source = (y[0] + 4 - d) % 4
                    where = (d % 2) * 512 + zh * 128
                    piece = totals[d // 2][:, where : where + 128]
                    moved = pltpu.roll(piece, ((source + 4 - zl) % 4) * 32, 1)
                    made = jnp.where(group == source, moved, made)
                to = (zh * 4 + zl) * 128
                out[at, to : to + 128] = made.astype(BF16)
        return carry

    lax.fori_loop(0, 6, step, 0)


def lane_is_second(rows):
    return lax.broadcasted_iota(jnp.int32, (rows, 128), 1) >= 64


def by_lane(running):
    turned = jnp.transpose(running)
    return jnp.where(lane_is_second(turned.shape[0]), turned[:, 1:2], turned[:, 0:1])


def put_rows(core, own, other, targets):
    for k in range(4):
        mine = pl.ds(pl.multiple_of(k * 192 + core * 96, 32), 96)
        theirs = pl.ds(pl.multiple_of(k * 192 + (1 - core) * 96, 32), 96)
        part = slice(k * 112, k * 112 + 96)
        for n, target in enumerate(targets):
            lanes = slice(n * 128, n * 128 + 128)
            target[mine, :] = own[part, lanes].astype(BF16)
            target[theirs, :] = other[part, lanes].astype(BF16)


def states_kernel(core, own, other, weight, running, tail, keys, values, message):
    w = weight[...]
    put_rows(
        core[0],
        jnp.dot(own[...], w, preferred_element_type=F32),
        jnp.dot(other[...], w, preferred_element_type=F32),
        (keys, values),
    )
    logs = by_lane(running[...])
    closing = logs[767:768, :]
    k = keys[...].astype(F32) * 0.125
    v = values[...]
    second = lane_is_second(64)
    ahead = lax.dot_general(
        (k * jnp.exp(closing - logs)).astype(BF16), v, TN, preferred_element_type=F32
    )
    back = lax.dot_general((k * jnp.exp(logs)).astype(BF16), v, TN, preferred_element_type=F32)
    parts = (
        (slice(0, 64), jnp.where(second, ahead[64:, :], ahead[:64, :]).astype(BF16)),
        (slice(64, 128), jnp.where(second, back[64:, :], back[:64, :]).astype(BF16)),
        (slice(128, 144), log_rows(closing)),
        (slice(144, 160), tail[...]),
    )
    for at, part in parts:
        for copy in range(16):
            message[copy, at, :] = part


def log_rows(log):
    high = log.astype(BF16)
    low = (log - high.astype(F32)).astype(BF16)
    first = lax.broadcasted_iota(jnp.int32, (16, 128), 0) < 8
    return jnp.where(first, high.astype(F32), low.astype(F32)).astype(BF16)


def scan_states(gathered, count, position):
    def log_of(m):
        return gathered[m, 128:129, :].astype(F32) + gathered[m, 136:137, :].astype(F32)

    def one_way(order, rows):
        state = jnp.zeros((64, 128), F32)
        log = jnp.zeros((1, 128), F32)
        held, held_log = state, log
        for m in order:
            here = position == m
            held = jnp.where(here, state, held)
            held_log = jnp.where(here, log, held_log)
            own = log_of(m)
            state = jnp.exp(own) * state + gathered[m, rows, :].astype(F32)
            log = log + own
        return held, held_log, state, log

    ahead = one_way(range(count), slice(0, 64))
    back = one_way(reversed(range(count)), slice(64, 128))
    return ahead, back


def level_kernel(position, gathered, inside, message):
    ahead, back = scan_states(gathered, 16, position[0])
    inside[0:64, :] = ahead[0]
    inside[64:128, :] = back[0]
    inside[128:136, :] = jnp.broadcast_to(ahead[1], (8, 128))
    inside[136:144, :] = jnp.broadcast_to(back[1], (8, 128))
    parts = [
        (slice(0, 64), ahead[2].astype(BF16)),
        (slice(64, 128), back[2].astype(BF16)),
        (slice(128, 144), log_rows(ahead[3])),
    ]
    group = lax.broadcasted_iota(jnp.int32, (16, 128), 1) // 32
    for y in range(4):
        made = gathered[y, 144:160, :].astype(F32)
        for zl in range(1, 4):
            moved = pltpu.roll(gathered[zl * 4 + y, 144:160, :].astype(F32), zl * 32, 1)
            made = jnp.where(group == zl, moved, made)
        parts.append((slice(144 + y * 16, 160 + y * 16), made.astype(BF16)))
    for at, part in parts:
        for copy in range(4):
            message[copy, at, :] = part


def column_block(position, shift):
    return pl.ds(pl.multiple_of(((position + 4 - shift) % 4) * 512, 512), 512)


def by_piece(y, rows, pieces, lanes):
    total = None
    for shift, piece in enumerate(pieces):
        part = jnp.dot(
            rows[:, column_block(y, shift)], piece[:, lanes], preferred_element_type=F32
        )
        total = part if total is None else total + part
    return total


def conv_kernel(core, y, own, other, p0, p1, p2, p3, taps, convolved, moments, padded):
    pieces = (p0, p1, p2, p3)

    def rows_of(rows):
        both = by_piece(y[0], rows, pieces, slice(0, 256))
        return (both[:, :128] * jax.nn.sigmoid(both[:, 128:])).astype(BF16).astype(F32)

    first, second = rows_of(own), rows_of(other)
    for k in range(4):
        mine = pl.ds(pl.multiple_of(16 + k * 192 + core[0] * 96, 16), 96)
        theirs = pl.ds(pl.multiple_of(16 + k * 192 + (1 - core[0]) * 96, 16), 96)
        padded[mine, :] = first[k * 112 : k * 112 + 96, :]
        padded[theirs, :] = second[k * 112 : k * 112 + 96, :]
    is_second = jnp.full((16, 128), core[0], jnp.int32) == 1
    padded[0:16, :] = jnp.where(is_second, first[432:448, :], second[432:448, :])
    padded[784:800, :] = jnp.where(is_second, second[96:112, :], first[96:112, :])
    ones = jnp.ones((8, 128), F32)
    rows = 128
    for i in range(6):
        total = None
        for j in range(31):
            start = i * rows + j + 1
            term = taps[j : j + 1, :] * padded[start : start + rows, :]
            total = term if total is None else total + term
        convolved[i * rows : (i + 1) * rows, :] = total
        highest = lax.Precision.HIGHEST
        s1 = lax.dot_general(ones, total, NT, precision=highest, preferred_element_type=F32)
        s2 = lax.dot_general(ones, total * total, NT, precision=highest, preferred_element_type=F32)
        for copy in range(8):
            moments[copy, 0:1, i * rows : (i + 1) * rows] = s1[0:1]
            moments[copy, 1:2, i * rows : (i + 1) * rows] = s2[0:1]


def within_kernel(
    core, y, own, other, p0, p1, p2, p3, keys, values, running, queries, gates, within
):
    pieces = (p0, p1, p2, p3)
    put_rows(
        core[0],
        by_piece(y[0], own, pieces, slice(0, 256)),
        by_piece(y[0], other, pieces, slice(0, 256)),
        (queries, gates),
    )
    logs = running[...]
    turned = jnp.transpose(logs)
    k = (keys[...].astype(F32) * 0.125).astype(BF16)
    v = values[...]
    rows = 128
    zero = jnp.zeros((), BF16)
    masks = [lane_is_second(768) == bool(h) for h in range(2)]
    head_values = [jnp.where(mask, v, zero) for mask in masks]
    for i in range(6):
        at = slice(i * rows, (i + 1) * rows)
        q = queries[at, :]
        diagonal = lax.broadcasted_iota(jnp.int32, (rows, 768), 1) == (
            lax.broadcasted_iota(jnp.int32, (rows, 768), 0) + i * rows
        )
        total = None
        for h in range(2):
            scores = lax.dot_general(
                jnp.where(masks[h][:rows], q, zero), k, NT, preferred_element_type=F32
            )
            distance = jnp.abs(turned[at, h : h + 1] - logs[h : h + 1, :])
            weights = jnp.exp(-distance) + jnp.where(diagonal, 1.0, 0.0)
            part = jnp.dot(
                (scores * weights).astype(BF16), head_values[h], preferred_element_type=F32
            )
            total = part if total is None else total + part
        within[at, :] = total


def out_part(y, rows, pieces, shifts, spare):
    parts = []
    for piece, shift in zip(pieces, shifts):
        part = lax.dot_general(rows[:, :240], piece[:, 256:496], NT, preferred_element_type=F32)
        left = spare[:, column_block(y, shift)]
        parts.append(part + jnp.dot(rows[:, 240:], left, preferred_element_type=F32))
    return jnp.concatenate(parts, axis=1)


def heads_kernel(
    position,
    queries,
    gates,
    within,
    running,
    gathered,
    inside,
    start,
    head_gain,
    heads,
    spare,
):
    ahead, back = scan_states(gathered, 4, position[0])
    forward = inside[0:64, :] + jnp.exp(inside[128:129, :]) * (
        ahead[0] + jnp.exp(ahead[1]) * start[0:64, :]
    )
    backward = inside[64:128, :] + jnp.exp(inside[136:137, :]) * (
        back[0] + jnp.exp(back[1]) * start[64:128, :]
    )
    second = lane_is_second(64)

    def diagonal_blocks(state):
        return jnp.concatenate(
            [jnp.where(second, 0.0, state), jnp.where(second, state, 0.0)], axis=0
        ).astype(BF16)

    forward, backward = diagonal_blocks(forward), diagonal_blocks(backward)
    logs = by_lane(running[...])
    closing = logs[767:768, :]
    rows = 128
    half = lane_is_second(rows)

    def head_mean(x):
        low = jnp.sum(jnp.where(half, 0.0, x), axis=1, keepdims=True)
        high = jnp.sum(jnp.where(half, x, 0.0), axis=1, keepdims=True)
        return jnp.where(half, high, low) / 64

    for i in range(6):
        at = slice(i * rows, (i + 1) * rows)
        q = queries[at, :]
        log = logs[at, :]
        retained = (
            within[at, :]
            + jnp.exp(log) * jnp.dot(q, forward, preferred_element_type=F32)
            + jnp.exp(closing - log) * jnp.dot(q, backward, preferred_element_type=F32)
        )
        centred = retained - head_mean(retained)
        normed = centred * lax.rsqrt(head_mean(centred * centred) + EPSILON)
        gate = jax.nn.silu(gates[at, :].astype(F32))
        heads[at, :] = (normed * head_gain[...] * gate).astype(BF16)
    for y in range(4):
        for zh in range(4):
            where = y * 512 + zh * 128
            spare[:, where : where + 128] = gathered[zh, 144 + y * 16 : 160 + y * 16, :]


def mixers_kernel(
    core,
    y,
    heads,
    convolved,
    moments,
    channel_gain,
    p0,
    p1,
    p2,
    p3,
    spare,
    mine,
    sent_a,
    sent_b,
    rows_in,
):
    sums = moments[0]
    for k in range(1, 8):
        sums = sums + moments[k]
    sums = jnp.transpose(jnp.concatenate([sums, jnp.zeros((6, 768), F32)], axis=0)) / DC
    rows = 128
    for i in range(6):
        at = slice(i * rows, (i + 1) * rows)
        average, squares = sums[at, 0:1], sums[at, 1:2]
        scaled = (convolved[at, :] - average) * lax.rsqrt(squares - average * average + EPSILON)
        rows_in[at, 0:128] = jax.nn.silu(scaled * channel_gain[...]).astype(BF16)
        rows_in[at, 128:256] = heads[at, :]

    def half_of(which):
        return jnp.concatenate(
            [
                rows_in[pl.ds(pl.multiple_of(k * 192 + which * 96, 32), 96), :]
                for k in range(4)
            ],
            axis=0,
        )

    mine[...] = half_of(core[0])
    other = half_of(1 - core[0])
    sent_a[...] = out_part(y[0], other, (p0, p1), (0, 1), spare).astype(BF16)
    sent_b[...] = out_part(y[0], other, (p2, p3), (2, 3), spare).astype(BF16)


def join_kernel(shifts, y, mine, arrived, p0, p1, spare, out):
    own = out_part(y[0], mine[...], (p0, p1), shifts, spare)
    out[...] = (own + arrived[...].astype(F32)).astype(BF16)


def ring(x, axis, shift):
    count = lax.axis_size(axis)
    return lax.ppermute(x, axis, [(i, (i + shift) % count) for i in range(count)])


def copies(x, axes, count):
    return lax.all_to_all(
        jnp.broadcast_to(x[None], (count, *x.shape)), axes, 0, 0, tiled=True
    )


def body(
    tokens,
    input_gain,
    branch_value,
    branch_gate,
    query_weight,
    key_weight,
    value_weight,
    swish_weight,
    kernel_taps,
    channel_gain,
    decay_logs,
    start_state,
    head_gain,
    output_conv,
    output_heads,
):
    core = lax.axis_index("c").astype(jnp.int32)[None]
    y = lax.axis_index("y").astype(jnp.int32)[None]
    high = lax.axis_index("zh").astype(jnp.int32)[None]
    low = lax.axis_index(("zl", "y")).astype(jnp.int32)[None]

    place = lax.axis_index(("x", "c"))
    count = lax.axis_size(SP)
    edge = lax.ppermute(
        jnp.where(place == 7, tokens[80:96], tokens[0:16]),
        ALL,
        [(i * 8 + 7, i * 8 + 15) for i in range(count - 1)]
        + [(i * 8 + 8, i * 8) for i in range(count - 1)],
    )
    shard = call(
        shard_kernel,
        shape((32, 1008), BF16),
        (),
        (
            key_weight,
            value_weight,
            branch_value,
            branch_gate,
            query_weight,
            swish_weight,
            output_conv.T,
            output_heads.T,
        ),
    )
    normed = call(
        norm_kernel, shape((4, 112, 2048), BF16), (), (tokens, edge, input_gain[None])
    )
    shard, normed = lax.optimization_barrier((shard, normed))
    own = lax.all_to_all(normed, "x", 0, 0, tiled=True).reshape(448, 2048)
    rows = lax.all_gather(shard, ("zh", "zl"), axis=0, tiled=True)
    own, rows = lax.optimization_barrier((own, rows))
    other = ring(own, "c", 1)
    state_weight = copies(rows[:, :256], "y", 4).reshape(2048, 256)
    gate_piece, rest_piece = rows[:, 256:512], rows[:, 512:]
    gate_pieces = (gate_piece,) + tuple(ring(gate_piece, "y", d) for d in (1, 2, 3))
    rest_pieces = (rest_piece,) + tuple(ring(rest_piece, "y", d) for d in (1, 2, 3))

    running = jnp.cumsum(decay_logs, axis=1)
    running = jnp.concatenate([running, jnp.zeros((6, 768), F32)], axis=0)
    start = start_state.transpose(0, 2, 1, 3).reshape(128, 128)

    half = shape((768, 128), BF16)
    full = shape((768, 128), F32)
    tail = jnp.pad(output_heads[112:], ((0, 0), (0, 96)))
    keys, values, sent = call(
        states_kernel,
        (half, half, shape((16, 160, 128), BF16)),
        (core,),
        (own, other, state_weight, running, tail),
    )
    gathered = lax.all_to_all(sent, ("zl", "y"), 0, 0, tiled=True)
    inside, sent = call(
        level_kernel,
        (shape((144, 128), F32), shape((4, 208, 128), BF16)),
        (low,),
        (gathered,),
    )
    gathered = lax.all_to_all(sent, "zh", 0, 0, tiled=True)
    convolved, moments = call(
        conv_kernel,
        (full, shape((8, 2, 768), F32)),
        (core, y),
        (own, other, *gate_pieces, kernel_taps),
        scratch=(pltpu.VMEM((800, 128), F32),),
    )
    moments = lax.all_to_all(moments, ("x", "c"), 0, 0, tiled=True)
    queries, gates, within = call(
        within_kernel,
        (half, half, full),
        (core, y),
        (own, other, *rest_pieces, keys, values, running),
    )
    heads, spare = call(
        heads_kernel,
        (half, shape((16, 2048), BF16)),
        (high,),
        (queries, gates, within, running, gathered, inside, start, head_gain[None]),
    )
    p0, p1, p2, p3 = rest_pieces
    mine, sent_a, sent_b = call(
        mixers_kernel,
        (shape((384, 256), BF16), shape((384, 1024), BF16), shape((384, 1024), BF16)),
        (core, y),
        (heads, convolved, moments, channel_gain[None], *rest_pieces, spare),
        scratch=(pltpu.VMEM((768, 256), BF16),),
    )
    arrived_a = ring(sent_a, "c", 1)
    arrived_b = ring(sent_b, "c", 1)

    def join(shifts, *arrays):
        made = call(
            functools.partial(join_kernel, shifts),
            shape((384, 1024), BF16),
            (y,),
            (mine, *arrays, spare),
        )
        return made.reshape(4, 96, 1024)

    joined_a = join((0, 1), arrived_a, p0, p1)
    parts_a = lax.all_to_all(joined_a, "x", 0, 0, tiled=True)
    joined_b = join((2, 3), arrived_b, p2, p3)
    parts_b = lax.all_to_all(joined_b, "x", 0, 0, tiled=True)
    return call(last_kernel, shape((96, 2048), BF16), (y,), (parts_a, parts_b))


def solution(mesh):
    split = Mesh(mesh.devices.reshape(4, 4, 4, 4, 2), ALL)
    in_specs = (
        P(ALL, None),
        P(),
        P(SP, ("x", "c")),
        P(SP, ("x", "c")),
        P(SP, ("x", "c")),
        P(SP, ("x", "c")),
        P(SP, ("x", "c")),
        P(SP, ("x", "c")),
        P(None, ("x", "c")),
        P(("x", "c")),
        P(("x", "c"), SP),
        P(None, ("x", "c"), None, None),
        P(("x", "c")),
        P(("x", "c"), SP),
        P(("x", "c"), SP),
    )

    return jax.shard_map(
        body, mesh=split, in_specs=in_specs, out_specs=P(ALL, None), check_vma=False
    )
```

```python
import jax
import jax.numpy as jnp
from jax import lax
from jax.experimental import pallas as pl
from jax.experimental.pallas import tpu as pltpu
from jax.sharding import Mesh
from jax.sharding import PartitionSpec as P

DC = 1024
EPSILON = 1e-06
F32 = jnp.float32
BF16 = jnp.bfloat16
SP = ("zh", "zl", "y")
ALL = ("zh", "zl", "y", "x", "c")
NT = (((1,), (1,)), ((), ()))
TN = (((0,), (0,)), ((), ()))
VMEM = pl.BlockSpec(memory_space=pltpu.VMEM)
SMEM = pl.BlockSpec(memory_space=pltpu.SMEM)


def call(kernel, out_shape, scalars, arrays, scratch=()):
    return pl.pallas_call(
        kernel,
        out_shape=out_shape,
        in_specs=[SMEM] * len(scalars) + [VMEM] * len(arrays),
        out_specs=[VMEM] * len(out_shape) if isinstance(out_shape, tuple) else VMEM,
        scratch_shapes=scratch,
        compiler_params=pltpu.CompilerParams(vmem_limit_bytes=20 * 1024 * 1024),
    )(*scalars, *arrays)


def shape(dims, dtype):
    return jax.ShapeDtypeStruct(dims, dtype)


def swap_groups(read, write, rows):
    group = lax.broadcasted_iota(jnp.int32, (rows, 128), 1) // 32
    for outer in range(4):
        for inner in range(4):
            made = None
            for k in range(4):
                moved = read(outer, k)
                turn = ((k - inner) * 32) % 128
                if turn:
                    moved = pltpu.roll(moved, turn, 1)
                made = moved if made is None else jnp.where(group == k, moved, made)
            write(outer, inner, made)


def shard_kernel(k, v, bv, bg, q, s, oc, oh, out):
    for i, part in enumerate((k, v, bv, bg, q, s, oc)):
        out[:, i * 128 : i * 128 + 128] = part[...]
    out[:, 896:1008] = oh[:, 0:112]


def norm_kernel(tokens, edge, gain, out):
    rows = 16

    def block(source, at, to):
        x = source[at, :].astype(F32)
        inverse = lax.rsqrt(jnp.mean(x * x, axis=1, keepdims=True) + EPSILON)
        normed = x * inverse * gain[...]

        def read(zh, zl):
            z = zh * 4 + zl
            return normed[:, z * 128 : z * 128 + 128]

        def write(zh, y, made):
            where = (y * 4 + zh) * 128
            made = made.astype(BF16)
            for copy in range(4):
                out[copy, to, where : where + 128] = made

        swap_groups(read, write, rows)

    def step(i, carry):
        at = pl.ds(pl.multiple_of(i * rows, rows), rows)
        block(tokens, at, at)
        return carry

    lax.fori_loop(0, 6, step, 0, unroll=2)
    block(edge, slice(0, 16), slice(96, 112))


def last_kernel(parts, out):
    rows = 16

    def step(i, carry):
        at = pl.ds(pl.multiple_of(i * rows, rows), rows)
        total = parts[0, at, :].astype(F32)
        for k in range(1, 4):
            total = total + parts[k, at, :].astype(F32)

        def read(zh, y):
            where = (y * 4 + zh) * 128
            return total[:, where : where + 128]

        def write(zh, zl, made):
            where = (zh * 4 + zl) * 128
            out[at, where : where + 128] = made.astype(BF16)

        swap_groups(read, write, rows)
        return carry

    lax.fori_loop(0, 6, step, 0, unroll=2)


def lane_is_second(rows):
    return lax.broadcasted_iota(jnp.int32, (rows, 128), 1) >= 64


def by_lane(running):
    turned = jnp.transpose(running)
    return jnp.where(lane_is_second(turned.shape[0]), turned[:, 1:2], turned[:, 0:1])


def put_rows(core, own, other, targets):
    for k in range(4):
        mine = pl.ds(pl.multiple_of(k * 192 + core * 96, 32), 96)
        theirs = pl.ds(pl.multiple_of(k * 192 + (1 - core) * 96, 32), 96)
        part = slice(k * 112, k * 112 + 96)
        for n, target in enumerate(targets):
            lanes = slice(n * 128, n * 128 + 128)
            target[mine, :] = own[part, lanes].astype(BF16)
            target[theirs, :] = other[part, lanes].astype(BF16)


def states_kernel(core, own, other, weight, running, tail, keys, values, message):
    w = weight[...]
    put_rows(
        core[0],
        jnp.dot(own[...], w, preferred_element_type=F32),
        jnp.dot(other[...], w, preferred_element_type=F32),
        (keys, values),
    )
    logs = by_lane(running[...])
    closing = logs[767:768, :]
    k = keys[...].astype(F32) * 0.125
    v = values[...]
    second = lane_is_second(64)
    ahead = lax.dot_general(
        (k * jnp.exp(closing - logs)).astype(BF16), v, TN, preferred_element_type=F32
    )
    back = lax.dot_general((k * jnp.exp(logs)).astype(BF16), v, TN, preferred_element_type=F32)
    parts = (
        (slice(0, 64), jnp.where(second, ahead[64:, :], ahead[:64, :]).astype(BF16)),
        (slice(64, 128), jnp.where(second, back[64:, :], back[:64, :]).astype(BF16)),
        (slice(128, 144), log_rows(closing)),
        (slice(144, 160), tail[...]),
    )
    for at, part in parts:
        for copy in range(16):
            message[copy, at, :] = part


def log_rows(log):
    high = log.astype(BF16)
    low = (log - high.astype(F32)).astype(BF16)
    first = lax.broadcasted_iota(jnp.int32, (16, 128), 0) < 8
    return jnp.where(first, high.astype(F32), low.astype(F32)).astype(BF16)


def scan_states(gathered, count, position):
    def log_of(m):
        return gathered[m, 128:129, :].astype(F32) + gathered[m, 136:137, :].astype(F32)

    def one_way(order, rows):
        state = jnp.zeros((64, 128), F32)
        log = jnp.zeros((1, 128), F32)
        held, held_log = state, log
        for m in order:
            here = position == m
            held = jnp.where(here, state, held)
            held_log = jnp.where(here, log, held_log)
            own = log_of(m)
            state = jnp.exp(own) * state + gathered[m, rows, :].astype(F32)
            log = log + own
        return held, held_log, state, log

    ahead = one_way(range(count), slice(0, 64))
    back = one_way(reversed(range(count)), slice(64, 128))
    return ahead, back


def level_kernel(position, gathered, inside, message):
    ahead, back = scan_states(gathered, 16, position[0])
    inside[0:64, :] = ahead[0]
    inside[64:128, :] = back[0]
    inside[128:136, :] = jnp.broadcast_to(ahead[1], (8, 128))
    inside[136:144, :] = jnp.broadcast_to(back[1], (8, 128))
    parts = [
        (slice(0, 64), ahead[2].astype(BF16)),
        (slice(64, 128), back[2].astype(BF16)),
        (slice(128, 144), log_rows(ahead[3])),
    ]
    group = lax.broadcasted_iota(jnp.int32, (16, 128), 1) // 32
    for y in range(4):
        made = gathered[y, 144:160, :].astype(F32)
        for zl in range(1, 4):
            moved = pltpu.roll(gathered[zl * 4 + y, 144:160, :].astype(F32), zl * 32, 1)
            made = jnp.where(group == zl, moved, made)
        parts.append((slice(144 + y * 16, 160 + y * 16), made.astype(BF16)))
    for at, part in parts:
        for copy in range(4):
            message[copy, at, :] = part


def column_block(position, shift):
    return pl.ds(pl.multiple_of(((position + 4 - shift) % 4) * 512, 512), 512)


def by_piece(y, rows, pieces, lanes):
    total = None
    for shift, piece in enumerate(pieces):
        part = jnp.dot(
            rows[:, column_block(y, shift)], piece[:, lanes], preferred_element_type=F32
        )
        total = part if total is None else total + part
    return total


def conv_kernel(core, y, own, other, p0, p1, p2, p3, taps, convolved, moments, padded):
    pieces = (p0, p1, p2, p3)

    def rows_of(rows):
        both = by_piece(y[0], rows, pieces, slice(0, 256))
        return (both[:, :128] * jax.nn.sigmoid(both[:, 128:])).astype(BF16).astype(F32)

    first, second = rows_of(own), rows_of(other)
    for k in range(4):
        mine = pl.ds(pl.multiple_of(16 + k * 192 + core[0] * 96, 16), 96)
        theirs = pl.ds(pl.multiple_of(16 + k * 192 + (1 - core[0]) * 96, 16), 96)
        padded[mine, :] = first[k * 112 : k * 112 + 96, :]
        padded[theirs, :] = second[k * 112 : k * 112 + 96, :]
    is_second = jnp.full((16, 128), core[0], jnp.int32) == 1
    padded[0:16, :] = jnp.where(is_second, first[432:448, :], second[432:448, :])
    padded[784:800, :] = jnp.where(is_second, second[96:112, :], first[96:112, :])
    ones = jnp.ones((8, 128), F32)
    rows = 128
    for i in range(6):
        total = None
        for j in range(31):
            start = i * rows + j + 1
            term = taps[j : j + 1, :] * padded[start : start + rows, :]
            total = term if total is None else total + term
        convolved[i * rows : (i + 1) * rows, :] = total
        highest = lax.Precision.HIGHEST
        s1 = lax.dot_general(ones, total, NT, precision=highest, preferred_element_type=F32)
        s2 = lax.dot_general(ones, total * total, NT, precision=highest, preferred_element_type=F32)
        moments[0:1, i * rows : (i + 1) * rows] = s1[0:1]
        moments[1:2, i * rows : (i + 1) * rows] = s2[0:1]


def within_kernel(
    core, y, own, other, p0, p1, p2, p3, keys, values, running, queries, gates, within
):
    pieces = (p0, p1, p2, p3)
    put_rows(
        core[0],
        by_piece(y[0], own, pieces, slice(0, 256)),
        by_piece(y[0], other, pieces, slice(0, 256)),
        (queries, gates),
    )
    logs = running[...]
    turned = jnp.transpose(logs)
    k = (keys[...].astype(F32) * 0.125).astype(BF16)
    v = values[...]
    rows = 128
    zero = jnp.zeros((), BF16)
    masks = [lane_is_second(768) == bool(h) for h in range(2)]
    head_values = [jnp.where(mask, v, zero) for mask in masks]
    for i in range(6):
        at = slice(i * rows, (i + 1) * rows)
        q = queries[at, :]
        diagonal = lax.broadcasted_iota(jnp.int32, (rows, 768), 1) == (
            lax.broadcasted_iota(jnp.int32, (rows, 768), 0) + i * rows
        )
        total = None
        for h in range(2):
            scores = lax.dot_general(
                jnp.where(masks[h][:rows], q, zero), k, NT, preferred_element_type=F32
            )
            distance = jnp.abs(turned[at, h : h + 1] - logs[h : h + 1, :])
            weights = jnp.exp(-distance) + jnp.where(diagonal, 1.0, 0.0)
            part = jnp.dot(
                (scores * weights).astype(BF16), head_values[h], preferred_element_type=F32
            )
            total = part if total is None else total + part
        within[at, :] = total


def out_rows(y, rows, pieces, spare, write):
    for shift, piece in enumerate(pieces):
        lanes = column_block(y, shift)
        part = lax.dot_general(rows[:, :240], piece[:, 256:496], NT, preferred_element_type=F32)
        part = part + jnp.dot(rows[:, 240:], spare[:, lanes], preferred_element_type=F32)
        write(lanes, part)


def heads_kernel(
    position,
    queries,
    gates,
    within,
    running,
    gathered,
    inside,
    start,
    head_gain,
    heads,
    spare,
):
    ahead, back = scan_states(gathered, 4, position[0])
    forward = inside[0:64, :] + jnp.exp(inside[128:129, :]) * (
        ahead[0] + jnp.exp(ahead[1]) * start[0:64, :]
    )
    backward = inside[64:128, :] + jnp.exp(inside[136:137, :]) * (
        back[0] + jnp.exp(back[1]) * start[64:128, :]
    )
    second = lane_is_second(64)

    def diagonal_blocks(state):
        return jnp.concatenate(
            [jnp.where(second, 0.0, state), jnp.where(second, state, 0.0)], axis=0
        ).astype(BF16)

    forward, backward = diagonal_blocks(forward), diagonal_blocks(backward)
    logs = by_lane(running[...])
    closing = logs[767:768, :]
    rows = 128
    half = lane_is_second(rows)

    def head_mean(x):
        low = jnp.sum(jnp.where(half, 0.0, x), axis=1, keepdims=True)
        high = jnp.sum(jnp.where(half, x, 0.0), axis=1, keepdims=True)
        return jnp.where(half, high, low) / 64

    for i in range(6):
        at = slice(i * rows, (i + 1) * rows)
        q = queries[at, :]
        log = logs[at, :]
        retained = (
            within[at, :]
            + jnp.exp(log) * jnp.dot(q, forward, preferred_element_type=F32)
            + jnp.exp(closing - log) * jnp.dot(q, backward, preferred_element_type=F32)
        )
        centred = retained - head_mean(retained)
        normed = centred * lax.rsqrt(head_mean(centred * centred) + EPSILON)
        gate = jax.nn.silu(gates[at, :].astype(F32))
        heads[at, :] = (normed * head_gain[...] * gate).astype(BF16)
    for y in range(4):
        for zh in range(4):
            where = y * 512 + zh * 128
            spare[:, where : where + 128] = gathered[zh, 144 + y * 16 : 160 + y * 16, :]


def mixers_kernel(
    core,
    y,
    heads,
    convolved,
    moments,
    channel_gain,
    p0,
    p1,
    p2,
    p3,
    spare,
    mine,
    sent,
    rows_in,
):
    sums = moments[0]
    for k in range(1, 8):
        sums = sums + moments[k]
    sums = jnp.transpose(jnp.concatenate([sums, jnp.zeros((6, 768), F32)], axis=0)) / DC
    rows = 128
    for i in range(6):
        at = slice(i * rows, (i + 1) * rows)
        average, squares = sums[at, 0:1], sums[at, 1:2]
        scaled = (convolved[at, :] - average) * lax.rsqrt(squares - average * average + EPSILON)
        rows_in[at, 0:128] = jax.nn.silu(scaled * channel_gain[...]).astype(BF16)
        rows_in[at, 128:256] = heads[at, :]

    def half_of(which):
        return jnp.concatenate(
            [
                rows_in[pl.ds(pl.multiple_of(k * 192 + which * 96, 32), 96), :]
                for k in range(4)
            ],
            axis=0,
        )

    mine[...] = half_of(core[0])

    def write(lanes, part):
        sent[:, lanes] = part.astype(BF16)

    out_rows(y[0], half_of(1 - core[0]), (p0, p1, p2, p3), spare, write)


def join_kernel(y, mine, arrived, p0, p1, p2, p3, spare, out):
    def write(lanes, part):
        out[:, lanes] = (part + arrived[:, lanes].astype(F32)).astype(BF16)

    out_rows(y[0], mine[...], (p0, p1, p2, p3), spare, write)


def ring(x, axis, shift):
    count = lax.axis_size(axis)
    return lax.ppermute(x, axis, [(i, (i + shift) % count) for i in range(count)])


def copies(x, axes, count):
    return lax.all_to_all(
        jnp.broadcast_to(x[None], (count, *x.shape)), axes, 0, 0, tiled=True
    )


def body(
    tokens,
    input_gain,
    branch_value,
    branch_gate,
    query_weight,
    key_weight,
    value_weight,
    swish_weight,
    kernel_taps,
    channel_gain,
    decay_logs,
    start_state,
    head_gain,
    output_conv,
    output_heads,
):
    core = lax.axis_index("c").astype(jnp.int32)[None]
    y = lax.axis_index("y").astype(jnp.int32)[None]
    high = lax.axis_index("zh").astype(jnp.int32)[None]
    low = lax.axis_index(("zl", "y")).astype(jnp.int32)[None]

    place = lax.axis_index(("x", "c"))
    count = lax.axis_size(SP)
    edge = lax.ppermute(
        jnp.where(place == 7, tokens[80:96], tokens[0:16]),
        ALL,
        [(i * 8 + 7, i * 8 + 15) for i in range(count - 1)]
        + [(i * 8 + 8, i * 8) for i in range(count - 1)],
    )
    shard = call(
        shard_kernel,
        shape((32, 1008), BF16),
        (),
        (
            key_weight,
            value_weight,
            branch_value,
            branch_gate,
            query_weight,
            swish_weight,
            output_conv.T,
            output_heads.T,
        ),
    )
    normed = call(
        norm_kernel, shape((4, 112, 2048), BF16), (), (tokens, edge, input_gain[None])
    )
    shard, normed = lax.optimization_barrier((shard, normed))
    own = lax.all_to_all(normed, "x", 0, 0, tiled=True).reshape(448, 2048)
    rows = lax.all_gather(shard, ("zh", "zl"), axis=0, tiled=True)
    own, rows = lax.optimization_barrier((own, rows))
    other = ring(own, "c", 1)
    state_weight = copies(rows[:, :256], "y", 4).reshape(2048, 256)
    gate_piece, rest_piece = rows[:, 256:512], rows[:, 512:]
    gate_pieces = (gate_piece,) + tuple(ring(gate_piece, "y", d) for d in (1, 2, 3))
    rest_pieces = (rest_piece,) + tuple(ring(rest_piece, "y", d) for d in (1, 2, 3))

    running = jnp.cumsum(decay_logs, axis=1)
    running = jnp.concatenate([running, jnp.zeros((6, 768), F32)], axis=0)
    start = start_state.transpose(0, 2, 1, 3).reshape(128, 128)

    half = shape((768, 128), BF16)
    full = shape((768, 128), F32)
    tail = jnp.pad(output_heads[112:], ((0, 0), (0, 96)))
    keys, values, sent = call(
        states_kernel,
        (half, half, shape((16, 160, 128), BF16)),
        (core,),
        (own, other, state_weight, running, tail),
    )
    gathered = lax.all_to_all(sent, ("zl", "y"), 0, 0, tiled=True)
    inside, sent = call(
        level_kernel,
        (shape((144, 128), F32), shape((4, 208, 128), BF16)),
        (low,),
        (gathered,),
    )
    gathered = lax.all_to_all(sent, "zh", 0, 0, tiled=True)
    convolved, moments = call(
        conv_kernel,
        (full, shape((2, 768), F32)),
        (core, y),
        (own, other, *gate_pieces, kernel_taps),
        scratch=(pltpu.VMEM((800, 128), F32),),
    )
    moments = lax.all_gather(moments, ("x", "c"))
    queries, gates, within = call(
        within_kernel,
        (half, half, full),
        (core, y),
        (own, other, *rest_pieces, keys, values, running),
    )
    heads, spare = call(
        heads_kernel,
        (half, shape((16, 2048), BF16)),
        (high,),
        (queries, gates, within, running, gathered, inside, start, head_gain[None]),
    )
    mine, sent = call(
        mixers_kernel,
        (shape((384, 256), BF16), shape((384, 2048), BF16)),
        (core, y),
        (heads, convolved, moments, channel_gain[None], *rest_pieces, spare),
        scratch=(pltpu.VMEM((768, 256), BF16),),
    )
    arrived = ring(sent, "c", 1)
    joined = call(
        join_kernel,
        shape((384, 2048), BF16),
        (y,),
        (mine, arrived, *rest_pieces, spare),
    )
    parts = lax.all_to_all(joined.reshape(4, 96, 2048), "x", 0, 0, tiled=True)
    return call(last_kernel, shape((96, 2048), BF16), (), (parts,))


def solution(mesh):
    split = Mesh(mesh.devices.reshape(4, 4, 4, 4, 2), ALL)
    in_specs = (
        P(ALL, None),
        P(),
        P(SP, ("x", "c")),
        P(SP, ("x", "c")),
        P(SP, ("x", "c")),
        P(SP, ("x", "c")),
        P(SP, ("x", "c")),
        P(SP, ("x", "c")),
        P(None, ("x", "c")),
        P(("x", "c")),
        P(("x", "c"), SP),
        P(None, ("x", "c"), None, None),
        P(("x", "c")),
        P(("x", "c"), SP),
        P(("x", "c"), SP),
    )

    return jax.shard_map(
        body, mesh=split, in_specs=in_specs, out_specs=P(ALL, None), check_vma=False
    )
```

```python
import jax
import jax.numpy as jnp
from jax import lax
from jax.experimental import pallas as pl
from jax.experimental.pallas import tpu as pltpu
from jax.sharding import Mesh
from jax.sharding import PartitionSpec as P

DC = 1024
EPSILON = 1e-06
F32 = jnp.float32
BF16 = jnp.bfloat16
SP = ("zh", "zl", "y")
ALL = ("zh", "zl", "y", "x", "c")
NT = (((1,), (1,)), ((), ()))
TN = (((0,), (0,)), ((), ()))
VMEM = pl.BlockSpec(memory_space=pltpu.VMEM)
SMEM = pl.BlockSpec(memory_space=pltpu.SMEM)
HBM = pl.BlockSpec(memory_space=pltpu.HBM)


def call(kernel, out_shape, scalars, arrays, scratch=(), grant=20, far=(), out_far=()):
    def specs(count, away):
        return [HBM if i in away else VMEM for i in range(count)]

    arrays = [
        pltpu.with_memory_space_constraint(a, pltpu.HBM) if i in far else a
        for i, a in enumerate(arrays)
    ]
    if isinstance(out_shape, tuple):
        out_shape = tuple(
            pltpu.HBM(s.shape, s.dtype) if i in out_far else s for i, s in enumerate(out_shape)
        )
    elif out_far:
        out_shape = pltpu.HBM(out_shape.shape, out_shape.dtype)
    outs = specs(len(out_shape), out_far) if isinstance(out_shape, tuple) else specs(1, out_far)[0]
    return pl.pallas_call(
        kernel,
        out_shape=out_shape,
        in_specs=[SMEM] * len(scalars) + specs(len(arrays), far),
        out_specs=outs,
        scratch_shapes=scratch,
        compiler_params=pltpu.CompilerParams(vmem_limit_bytes=grant * 1024 * 1024),
    )(*scalars, *arrays)


def start_copies(pairs, semaphores):
    copies = [
        pltpu.make_async_copy(source, target, semaphores.at[i])
        for i, (source, target) in enumerate(pairs)
    ]
    for copy in copies:
        copy.start()
    return copies


def shape(dims, dtype):
    return jax.ShapeDtypeStruct(dims, dtype)


def swap_groups(read, write, rows):
    group = lax.broadcasted_iota(jnp.int32, (rows, 128), 1) // 32
    for outer in range(4):
        for inner in range(4):
            made = None
            for k in range(4):
                moved = read(outer, k)
                turn = ((k - inner) * 32) % 128
                if turn:
                    moved = pltpu.roll(moved, turn, 1)
                made = moved if made is None else jnp.where(group == k, moved, made)
            write(outer, inner, made)


def shard_kernel(k, v, bv, bg, q, s, oc, oh, out):
    for i, part in enumerate((k, v, bv, bg, q, s, oc)):
        out[:, i * 128 : i * 128 + 128] = part[...]
    out[:, 896:1008] = oh[:, 0:112]


def norm_kernel(tokens_far, edge, gain_far, out_far, tokens, gain, out, semaphores):
    rows = 16
    for copy in start_copies(((tokens_far, tokens), (gain_far, gain)), semaphores):
        copy.wait()

    def block(source, at, to):
        x = source[at, :].astype(F32)
        inverse = lax.rsqrt(jnp.mean(x * x, axis=1, keepdims=True) + EPSILON)
        normed = x * inverse * gain[...]

        def read(zh, zl):
            z = zh * 4 + zl
            return normed[:, z * 128 : z * 128 + 128]

        def write(zh, y, made):
            where = (y * 4 + zh) * 128
            out[to, where : where + 128] = made.astype(BF16)

        swap_groups(read, write, rows)

    def step(i, carry):
        at = pl.ds(pl.multiple_of(i * rows, rows), rows)
        block(tokens, at, at)
        return carry

    lax.fori_loop(0, 6, step, 0, unroll=2)
    block(edge, slice(0, 16), slice(96, 112))
    for copy in start_copies([(out, out_far.at[k]) for k in range(4)], semaphores):
        copy.wait()


def last_kernel(parts, out):
    rows = 16

    def step(i, carry):
        at = pl.ds(pl.multiple_of(i * rows, rows), rows)
        total = parts[0, at, :].astype(F32)
        for k in range(1, 4):
            total = total + parts[k, at, :].astype(F32)

        def read(zh, y):
            where = (y * 4 + zh) * 128
            return total[:, where : where + 128]

        def write(zh, zl, made):
            where = (zh * 4 + zl) * 128
            out[at, where : where + 128] = made.astype(BF16)

        swap_groups(read, write, rows)
        return carry

    lax.fori_loop(0, 6, step, 0, unroll=2)


def lane_is_second(rows):
    return lax.broadcasted_iota(jnp.int32, (rows, 128), 1) >= 64


def by_lane(running):
    turned = jnp.transpose(running)
    return jnp.where(lane_is_second(turned.shape[0]), turned[:, 1:2], turned[:, 0:1])


def put_rows(core, own, other, target):
    for k in range(4):
        mine = pl.ds(pl.multiple_of(k * 192 + core * 96, 32), 96)
        theirs = pl.ds(pl.multiple_of(k * 192 + (1 - core) * 96, 32), 96)
        part = slice(k * 112, k * 112 + 96)
        target[mine, :] = own[part, :].astype(BF16)
        target[theirs, :] = other[part, :].astype(BF16)


def states_kernel(core, own, other, weight, running, tail, both_far, message, both, semaphores):
    w = weight[...]
    put_rows(
        core[0],
        jnp.dot(own[...], w, preferred_element_type=F32),
        jnp.dot(other[...], w, preferred_element_type=F32),
        both,
    )
    (kept,) = start_copies(((both, both_far),), semaphores)
    logs = by_lane(running[...])
    closing = logs[767:768, :]
    k = both[:, 0:128].astype(F32) * 0.125
    v = both[:, 128:256]
    second = lane_is_second(64)
    ahead = lax.dot_general(
        (k * jnp.exp(closing - logs)).astype(BF16), v, TN, preferred_element_type=F32
    )
    back = lax.dot_general((k * jnp.exp(logs)).astype(BF16), v, TN, preferred_element_type=F32)
    parts = (
        (slice(0, 64), jnp.where(second, ahead[64:, :], ahead[:64, :]).astype(BF16)),
        (slice(64, 128), jnp.where(second, back[64:, :], back[:64, :]).astype(BF16)),
        (slice(128, 144), log_rows(closing)),
        (slice(144, 160), tail[...]),
    )
    for at, part in parts:
        for copy in range(16):
            message[copy, at, :] = part
    kept.wait()


def log_rows(log):
    high = log.astype(BF16)
    low = (log - high.astype(F32)).astype(BF16)
    first = lax.broadcasted_iota(jnp.int32, (16, 128), 0) < 8
    return jnp.where(first, high.astype(F32), low.astype(F32)).astype(BF16)


def scan_states(gathered, count, position):
    def log_of(m):
        return gathered[m, 128:129, :].astype(F32) + gathered[m, 136:137, :].astype(F32)

    def one_way(order, rows):
        state = jnp.zeros((64, 128), F32)
        log = jnp.zeros((1, 128), F32)
        held, held_log = state, log
        for m in order:
            here = position == m
            held = jnp.where(here, state, held)
            held_log = jnp.where(here, log, held_log)
            own = log_of(m)
            state = jnp.exp(own) * state + gathered[m, rows, :].astype(F32)
            log = log + own
        return held, held_log, state, log

    ahead = one_way(range(count), slice(0, 64))
    back = one_way(reversed(range(count)), slice(64, 128))
    return ahead, back


def level_kernel(position, gathered, message_far, message, semaphores):
    ahead, back = scan_states(gathered, 16, position[0])
    parts = [
        (slice(0, 64), ahead[2].astype(BF16)),
        (slice(64, 128), back[2].astype(BF16)),
        (slice(128, 144), log_rows(ahead[3])),
    ]
    group = lax.broadcasted_iota(jnp.int32, (16, 128), 1) // 32
    for y in range(4):
        made = gathered[y, 144:160, :].astype(F32)
        for zl in range(1, 4):
            moved = pltpu.roll(gathered[zl * 4 + y, 144:160, :].astype(F32), zl * 32, 1)
            made = jnp.where(group == zl, moved, made)
        parts.append((slice(144 + y * 16, 160 + y * 16), made.astype(BF16)))
    for at, part in parts:
        message[at, :] = part
    for copy in start_copies([(message, message_far.at[k]) for k in range(4)], semaphores):
        copy.wait()


def column_block(position, shift):
    return pl.ds(pl.multiple_of(((position + 4 - shift) % 4) * 512, 512), 512)


def by_piece(y, rows, pieces, lanes):
    total = None
    for shift, piece in enumerate(pieces):
        part = jnp.dot(
            rows[:, column_block(y, shift)], piece[:, lanes], preferred_element_type=F32
        )
        total = part if total is None else total + part
    return total


def conv_kernel(core, y, own, other, p0, p1, p2, p3, taps, convolved_far, moments_far, padded, convolved, moments, semaphores):
    pieces = (p0, p1, p2, p3)

    def rows_of(rows):
        both = by_piece(y[0], rows, pieces, slice(0, 256))
        return (both[:, :128] * jax.nn.sigmoid(both[:, 128:])).astype(BF16).astype(F32)

    first, second = rows_of(own), rows_of(other)
    for k in range(4):
        mine = pl.ds(pl.multiple_of(16 + k * 192 + core[0] * 96, 16), 96)
        theirs = pl.ds(pl.multiple_of(16 + k * 192 + (1 - core[0]) * 96, 16), 96)
        padded[mine, :] = first[k * 112 : k * 112 + 96, :]
        padded[theirs, :] = second[k * 112 : k * 112 + 96, :]
    is_second = jnp.full((16, 128), core[0], jnp.int32) == 1
    padded[0:16, :] = jnp.where(is_second, first[432:448, :], second[432:448, :])
    padded[784:800, :] = jnp.where(is_second, second[96:112, :], first[96:112, :])
    ones = jnp.ones((8, 128), F32)
    rows = 128
    for i in range(6):
        total = None
        for j in range(31):
            start = i * rows + j + 1
            term = taps[j : j + 1, :] * padded[start : start + rows, :]
            total = term if total is None else total + term
        convolved[i * rows : (i + 1) * rows, :] = total
        highest = lax.Precision.HIGHEST
        s1 = lax.dot_general(ones, total, NT, precision=highest, preferred_element_type=F32)
        s2 = lax.dot_general(ones, total * total, NT, precision=highest, preferred_element_type=F32)
        moments[0:1, i * rows : (i + 1) * rows] = s1[0:1]
        moments[1:2, i * rows : (i + 1) * rows] = s2[0:1]
    pairs = ((convolved, convolved_far), (moments, moments_far))
    for copy in start_copies(pairs, semaphores):
        copy.wait()


def out_rows(y, rows, pieces, spare, write):
    for shift, piece in enumerate(pieces):
        lanes = column_block(y, shift)
        part = lax.dot_general(rows[:, :240], piece[:, 256:496], NT, preferred_element_type=F32)
        part = part + jnp.dot(rows[:, 240:], spare[:, lanes], preferred_element_type=F32)
        write(lanes, part)


def mixers_kernel(
    core,
    y,
    low,
    high,
    own,
    other,
    p0,
    p1,
    p2,
    p3,
    inner,
    outer,
    both_far,
    running_far,
    start_far,
    head_gain_far,
    convolved_far,
    moments_far,
    channel_gain_far,
    mine,
    sent,
    spare,
    pair,
    rows_in,
    both,
    running,
    start,
    head_gain,
    convolved,
    moments,
    channel_gain,
    semaphores,
):
    pieces = (p0, p1, p2, p3)
    loads = start_copies(
        (
            (both_far, both),
            (running_far, running),
            (start_far, start),
            (head_gain_far, head_gain),
            (convolved_far, convolved),
            (moments_far, moments),
            (channel_gain_far, channel_gain),
        ),
        semaphores,
    )
    put_rows(
        core[0],
        by_piece(y[0], own, pieces, slice(0, 256)),
        by_piece(y[0], other, pieces, slice(0, 256)),
        pair,
    )
    for load in loads:
        load.wait()
    near = scan_states(inner, 16, low[0])
    far = scan_states(outer, 4, high[0])
    second = lane_is_second(64)

    def entering(way):
        begun = jnp.concatenate([start[way, 0], start[way, 1]], axis=1)
        state = far[way][0] + jnp.exp(far[way][1]) * begun
        state = near[way][0] + jnp.exp(near[way][1]) * state
        return jnp.concatenate(
            [jnp.where(second, 0.0, state), jnp.where(second, state, 0.0)], axis=0
        ).astype(BF16)

    forward, backward = entering(0), entering(1)
    logs = running[...]
    turned = jnp.transpose(logs)
    sums = moments[0]
    for k in range(1, 8):
        sums = sums + moments[k]
    sums = jnp.transpose(jnp.concatenate([sums, jnp.zeros((6, 768), F32)], axis=0)) / DC
    for yy in range(4):
        for zh in range(4):
            where = yy * 512 + zh * 128
            spare[:, where : where + 128] = outer[zh, 144 + yy * 16 : 160 + yy * 16, :]

    k = (both[:, 0:128].astype(F32) * 0.125).astype(BF16)
    v = both[:, 128:256]
    rows = 128
    zero = jnp.zeros((), BF16)
    half = lane_is_second(rows)
    masks = [lane_is_second(768) == bool(h) for h in range(2)]
    head_values = [jnp.where(mask, v, zero) for mask in masks]

    def head_mean(x):
        first = jnp.sum(jnp.where(half, 0.0, x), axis=1, keepdims=True)
        last = jnp.sum(jnp.where(half, x, 0.0), axis=1, keepdims=True)
        return jnp.where(half, last, first) / 64

    for i in range(6):
        at = slice(i * rows, (i + 1) * rows)
        q = pair[at, 0:128]
        diagonal = lax.broadcasted_iota(jnp.int32, (rows, 768), 1) == (
            lax.broadcasted_iota(jnp.int32, (rows, 768), 0) + i * rows
        )
        log = jnp.where(half, turned[at, 1:2], turned[at, 0:1])
        closing = jnp.where(half[0:1], turned[767:768, 1:2], turned[767:768, 0:1])
        retained = jnp.exp(log) * jnp.dot(q, forward, preferred_element_type=F32)
        retained = retained + jnp.exp(closing - log) * jnp.dot(
            q, backward, preferred_element_type=F32
        )
        for h in range(2):
            scores = lax.dot_general(
                jnp.where(masks[h][:rows], q, zero), k, NT, preferred_element_type=F32
            )
            distance = jnp.abs(turned[at, h : h + 1] - logs[h : h + 1, :])
            weights = jnp.exp(-distance) + jnp.where(diagonal, 1.0, 0.0)
            retained = retained + jnp.dot(
                (scores * weights).astype(BF16), head_values[h], preferred_element_type=F32
            )
        centred = retained - head_mean(retained)
        normed = centred * lax.rsqrt(head_mean(centred * centred) + EPSILON)
        gate = jax.nn.silu(pair[at, 128:256].astype(F32))
        rows_in[at, 128:256] = (normed * head_gain[...] * gate).astype(BF16)
        average, squares = sums[at, 0:1], sums[at, 1:2]
        scaled = (convolved[at, :] - average) * lax.rsqrt(squares - average * average + EPSILON)
        rows_in[at, 0:128] = jax.nn.silu(scaled * channel_gain[...]).astype(BF16)

    def half_of(which):
        return jnp.concatenate(
            [
                rows_in[pl.ds(pl.multiple_of(k * 192 + which * 96, 32), 96), :]
                for k in range(4)
            ],
            axis=0,
        )

    mine[...] = half_of(core[0])

    def write(lanes, part):
        sent[:, lanes] = part.astype(BF16)

    out_rows(y[0], half_of(1 - core[0]), pieces, spare, write)


def join_kernel(y, mine, arrived, p0, p1, p2, p3, spare, out):
    def write(lanes, part):
        out[:, lanes] = (part + arrived[:, lanes].astype(F32)).astype(BF16)

    out_rows(y[0], mine[...], (p0, p1, p2, p3), spare, write)


def ring(x, axis, shift):
    count = lax.axis_size(axis)
    return lax.ppermute(x, axis, [(i, (i + shift) % count) for i in range(count)])


def copies(x, axes, count):
    return lax.all_to_all(
        jnp.broadcast_to(x[None], (count, *x.shape)), axes, 0, 0, tiled=True
    )


def body(
    tokens,
    input_gain,
    branch_value,
    branch_gate,
    query_weight,
    key_weight,
    value_weight,
    swish_weight,
    kernel_taps,
    channel_gain,
    decay_logs,
    start_state,
    head_gain,
    output_conv,
    output_heads,
):
    core = lax.axis_index("c").astype(jnp.int32)[None]
    y = lax.axis_index("y").astype(jnp.int32)[None]
    high = lax.axis_index("zh").astype(jnp.int32)[None]
    low = lax.axis_index(("zl", "y")).astype(jnp.int32)[None]

    place = lax.axis_index(("x", "c"))
    count = lax.axis_size(SP)
    edge = lax.ppermute(
        jnp.where(place == 7, tokens[80:96], tokens[0:16]),
        ALL,
        [(i * 8 + 7, i * 8 + 15) for i in range(count - 1)]
        + [(i * 8 + 8, i * 8) for i in range(count - 1)],
    )
    shard = call(
        shard_kernel,
        shape((32, 1008), BF16),
        (),
        (
            key_weight,
            value_weight,
            branch_value,
            branch_gate,
            query_weight,
            swish_weight,
            output_conv.T,
            output_heads.T,
        ),
        grant=56,
    )
    normed = call(
        norm_kernel,
        shape((4, 112, 2048), BF16),
        (),
        (tokens, edge, input_gain[None]),
        scratch=(
            pltpu.VMEM((96, 2048), BF16),
            pltpu.VMEM((1, 2048), F32),
            pltpu.VMEM((112, 2048), BF16),
            pltpu.SemaphoreType.DMA((4,)),
        ),
        far=(0, 2),
        out_far=(0,),
    )
    shard, normed = lax.optimization_barrier((shard, normed))
    own = lax.all_to_all(normed, "x", 0, 0, tiled=True).reshape(448, 2048)
    rows = lax.all_gather(shard, ("zh", "zl"), axis=0, tiled=True)
    own, rows = lax.optimization_barrier((own, rows))
    other = ring(own, "c", 1)
    state_weight = copies(rows[:, :256], "y", 4).reshape(2048, 256)
    gate_piece, rest_piece = rows[:, 256:512], rows[:, 512:]
    gate_pieces = (gate_piece,) + tuple(ring(gate_piece, "y", d) for d in (1, 2, 3))
    rest_pieces = (rest_piece,) + tuple(ring(rest_piece, "y", d) for d in (1, 2, 3))

    running = jnp.cumsum(decay_logs, axis=1)
    running = jnp.concatenate([running, jnp.zeros((6, 768), F32)], axis=0)

    full = shape((768, 128), F32)
    tail = jnp.pad(output_heads[112:], ((0, 0), (0, 96)))
    both, sent = call(
        states_kernel,
        (shape((768, 256), BF16), shape((16, 160, 128), BF16)),
        (core,),
        (own, other, state_weight, running, tail),
        scratch=(pltpu.VMEM((768, 256), BF16), pltpu.SemaphoreType.DMA((1,))),
        out_far=(0,),
    )
    inner = lax.all_to_all(sent, ("zl", "y"), 0, 0, tiled=True)
    sent = call(
        level_kernel,
        shape((4, 208, 128), BF16),
        (low,),
        (inner,),
        scratch=(pltpu.VMEM((208, 128), BF16), pltpu.SemaphoreType.DMA((4,))),
        out_far=(0,),
    )
    outer = lax.all_to_all(sent, "zh", 0, 0, tiled=True)
    convolved, moments = call(
        conv_kernel,
        (full, shape((2, 768), F32)),
        (core, y),
        (own, other, *gate_pieces, kernel_taps),
        scratch=(
            pltpu.VMEM((800, 128), F32),
            pltpu.VMEM((768, 128), F32),
            pltpu.VMEM((2, 768), F32),
            pltpu.SemaphoreType.DMA((2,)),
        ),
        out_far=(0, 1),
    )
    moments = lax.all_gather(moments, ("x", "c"))
    mine, sent, spare = call(
        mixers_kernel,
        (shape((384, 256), BF16), shape((384, 2048), BF16), shape((16, 2048), BF16)),
        (core, y, low, high),
        (
            own,
            other,
            *rest_pieces,
            inner,
            outer,
            both,
            running,
            start_state,
            head_gain[None],
            convolved,
            moments,
            channel_gain[None],
        ),
        scratch=(
            pltpu.VMEM((768, 256), BF16),
            pltpu.VMEM((768, 256), BF16),
            pltpu.VMEM((768, 256), BF16),
            pltpu.VMEM((8, 768), F32),
            pltpu.VMEM((2, 2, 64, 64), F32),
            pltpu.VMEM((1, 128), F32),
            pltpu.VMEM((768, 128), F32),
            pltpu.VMEM((8, 2, 768), F32),
            pltpu.VMEM((1, 128), F32),
            pltpu.SemaphoreType.DMA((7,)),
        ),
        far=(8, 9, 10, 11, 12, 13, 14),
    )
    arrived = ring(sent, "c", 1)
    joined = call(join_kernel, shape((384, 2048), BF16), (y,), (mine, arrived, *rest_pieces, spare))
    parts = lax.all_to_all(joined.reshape(4, 96, 2048), "x", 0, 0, tiled=True)
    return call(last_kernel, shape((96, 2048), BF16), (), (parts,))


def solution(mesh):
    split = Mesh(mesh.devices.reshape(4, 4, 4, 4, 2), ALL)
    in_specs = (
        P(ALL, None),
        P(),
        P(SP, ("x", "c")),
        P(SP, ("x", "c")),
        P(SP, ("x", "c")),
        P(SP, ("x", "c")),
        P(SP, ("x", "c")),
        P(SP, ("x", "c")),
        P(None, ("x", "c")),
        P(("x", "c")),
        P(("x", "c"), SP),
        P(None, ("x", "c"), None, None),
        P(("x", "c")),
        P(("x", "c"), SP),
        P(("x", "c"), SP),
    )

    return jax.shard_map(
        body, mesh=split, in_specs=in_specs, out_specs=P(ALL, None), check_vma=False
    )
```

```python
import jax
import jax.numpy as jnp
from jax import lax
from jax.experimental import pallas as pl
from jax.experimental.pallas import tpu as pltpu
from jax.sharding import Mesh
from jax.sharding import PartitionSpec as P

DC = 1024
EPSILON = 1e-06
F32 = jnp.float32
BF16 = jnp.bfloat16
SP = ("zh", "zl", "y")
ALL = ("zh", "zl", "y", "x", "c")
NT = (((1,), (1,)), ((), ()))
TN = (((0,), (0,)), ((), ()))
VMEM = pl.BlockSpec(memory_space=pltpu.VMEM)
SMEM = pl.BlockSpec(memory_space=pltpu.SMEM)
HBM = pl.BlockSpec(memory_space=pltpu.HBM)


def call(kernel, out_shape, scalars, arrays, scratch=(), grant=20, far=(), out_far=()):
    def specs(count, away):
        return [HBM if i in away else VMEM for i in range(count)]

    arrays = [
        pltpu.with_memory_space_constraint(a, pltpu.HBM) if i in far else a
        for i, a in enumerate(arrays)
    ]
    if isinstance(out_shape, tuple):
        out_shape = tuple(
            pltpu.HBM(s.shape, s.dtype) if i in out_far else s for i, s in enumerate(out_shape)
        )
    elif out_far:
        out_shape = pltpu.HBM(out_shape.shape, out_shape.dtype)
    outs = specs(len(out_shape), out_far) if isinstance(out_shape, tuple) else specs(1, out_far)[0]
    return pl.pallas_call(
        kernel,
        out_shape=out_shape,
        in_specs=[SMEM] * len(scalars) + specs(len(arrays), far),
        out_specs=outs,
        scratch_shapes=scratch,
        compiler_params=pltpu.CompilerParams(vmem_limit_bytes=grant * 1024 * 1024),
    )(*scalars, *arrays)


def start_copies(pairs, semaphores):
    copies = [
        pltpu.make_async_copy(source, target, semaphores.at[i])
        for i, (source, target) in enumerate(pairs)
    ]
    for copy in copies:
        copy.start()
    return copies


def shape(dims, dtype):
    return jax.ShapeDtypeStruct(dims, dtype)


def swap_groups(read, write, rows):
    group = lax.broadcasted_iota(jnp.int32, (rows, 128), 1) // 32
    for outer in range(4):
        for inner in range(4):
            made = None
            for k in range(4):
                moved = read(outer, k)
                turn = ((k - inner) * 32) % 128
                if turn:
                    moved = pltpu.roll(moved, turn, 1)
                made = moved if made is None else jnp.where(group == k, moved, made)
            write(outer, inner, made)


def shard_kernel(k, v, bv, bg, q, s, oc, oh, out):
    for i, part in enumerate((k, v, bv, bg, q, s, oc)):
        out[:, i * 128 : i * 128 + 128] = part[...]
    out[:, 896:1008] = oh[:, 0:112]


def norm_kernel(tokens_far, edge, gain_far, out_far, tokens, gain, out, semaphores):
    rows = 16
    for copy in start_copies(((tokens_far, tokens), (gain_far, gain)), semaphores):
        copy.wait()

    def block(source, at, to):
        x = source[at, :].astype(F32)
        inverse = lax.rsqrt(jnp.mean(x * x, axis=1, keepdims=True) + EPSILON)
        normed = x * inverse * gain[...]

        def read(zh, zl):
            z = zh * 4 + zl
            return normed[:, z * 128 : z * 128 + 128]

        def write(zh, y, made):
            where = (y * 4 + zh) * 128
            out[to, where : where + 128] = made.astype(BF16)

        swap_groups(read, write, rows)

    def step(i, carry):
        at = pl.ds(pl.multiple_of(i * rows, rows), rows)
        block(tokens, at, at)
        return carry

    lax.fori_loop(0, 6, step, 0, unroll=2)
    block(edge, slice(0, 16), slice(96, 112))
    for copy in start_copies([(out, out_far.at[k]) for k in range(4)], semaphores):
        copy.wait()


def last_kernel(parts, out):
    rows = 16

    def step(i, carry):
        at = pl.ds(pl.multiple_of(i * rows, rows), rows)
        total = parts[0, at, :].astype(F32)
        for k in range(1, 4):
            total = total + parts[k, at, :].astype(F32)

        def read(zh, y):
            where = (y * 4 + zh) * 128
            return total[:, where : where + 128]

        def write(zh, zl, made):
            where = (zh * 4 + zl) * 128
            out[at, where : where + 128] = made.astype(BF16)

        swap_groups(read, write, rows)
        return carry

    lax.fori_loop(0, 6, step, 0, unroll=2)


def lane_is_second(rows):
    return lax.broadcasted_iota(jnp.int32, (rows, 128), 1) >= 64


def by_lane(running):
    turned = jnp.transpose(running)
    return jnp.where(lane_is_second(turned.shape[0]), turned[:, 1:2], turned[:, 0:1])


def put_rows(core, own, other, target):
    for k in range(4):
        mine = pl.ds(pl.multiple_of(k * 192 + core * 96, 32), 96)
        theirs = pl.ds(pl.multiple_of(k * 192 + (1 - core) * 96, 32), 96)
        part = slice(k * 112, k * 112 + 96)
        target[mine, :] = own[part, :].astype(BF16)
        target[theirs, :] = other[part, :].astype(BF16)


def states_kernel(core, own, other, weight, running, tail, both_far, message_far, both, message, semaphores):
    w = weight[...]
    put_rows(
        core[0],
        jnp.dot(own[...], w, preferred_element_type=F32),
        jnp.dot(other[...], w, preferred_element_type=F32),
        both,
    )
    kept = pltpu.make_async_copy(both, both_far, semaphores.at[16])
    kept.start()
    logs = by_lane(running[...])
    closing = logs[767:768, :]
    k = both[:, 0:128].astype(F32) * 0.125
    v = both[:, 128:256]
    second = lane_is_second(64)
    ahead = lax.dot_general(
        (k * jnp.exp(closing - logs)).astype(BF16), v, TN, preferred_element_type=F32
    )
    back = lax.dot_general((k * jnp.exp(logs)).astype(BF16), v, TN, preferred_element_type=F32)
    parts = (
        (slice(0, 64), jnp.where(second, ahead[64:, :], ahead[:64, :]).astype(BF16)),
        (slice(64, 128), jnp.where(second, back[64:, :], back[:64, :]).astype(BF16)),
        (slice(128, 144), log_rows(closing)),
        (slice(144, 160), tail[...]),
    )
    for at, part in parts:
        message[at, :] = part
    for copy in start_copies([(message, message_far.at[k]) for k in range(16)], semaphores):
        copy.wait()
    kept.wait()


def log_rows(log):
    high = log.astype(BF16)
    low = (log - high.astype(F32)).astype(BF16)
    first = lax.broadcasted_iota(jnp.int32, (16, 128), 0) < 8
    return jnp.where(first, high.astype(F32), low.astype(F32)).astype(BF16)


def scan_states(gathered, count, position):
    def log_of(m):
        return gathered[m, 128:129, :].astype(F32) + gathered[m, 136:137, :].astype(F32)

    def one_way(order, rows):
        state = jnp.zeros((64, 128), F32)
        log = jnp.zeros((1, 128), F32)
        held, held_log = state, log
        for m in order:
            here = position == m
            held = jnp.where(here, state, held)
            held_log = jnp.where(here, log, held_log)
            own = log_of(m)
            state = jnp.exp(own) * state + gathered[m, rows, :].astype(F32)
            log = log + own
        return held, held_log, state, log

    ahead = one_way(range(count), slice(0, 64))
    back = one_way(reversed(range(count)), slice(64, 128))
    return ahead, back


def level_kernel(position, gathered, message_far, message, semaphores):
    ahead, back = scan_states(gathered, 16, position[0])
    parts = [
        (slice(0, 64), ahead[2].astype(BF16)),
        (slice(64, 128), back[2].astype(BF16)),
        (slice(128, 144), log_rows(ahead[3])),
    ]
    group = lax.broadcasted_iota(jnp.int32, (16, 128), 1) // 32
    for y in range(4):
        made = gathered[y, 144:160, :].astype(F32)
        for zl in range(1, 4):
            moved = pltpu.roll(gathered[zl * 4 + y, 144:160, :].astype(F32), zl * 32, 1)
            made = jnp.where(group == zl, moved, made)
        parts.append((slice(144 + y * 16, 160 + y * 16), made.astype(BF16)))
    for at, part in parts:
        message[at, :] = part
    for copy in start_copies([(message, message_far.at[k]) for k in range(4)], semaphores):
        copy.wait()


def column_block(position, shift):
    return pl.ds(pl.multiple_of(((position + 4 - shift) % 4) * 512, 512), 512)


def split_kernel(rows_far, states_far, gate, rest, semaphores):
    pairs = [(rows_far.at[:, 0:256], states_far.at[k]) for k in range(4)]
    pairs += [(rows_far.at[:, 256:512], gate), (rows_far.at[:, 512:1008], rest)]
    for copy in start_copies(pairs, semaphores):
        copy.wait()


def by_piece(y, rows, pieces, lanes):
    total = None
    for shift, piece in enumerate(pieces):
        part = jnp.dot(
            rows[:, column_block(y, shift)], piece[:, lanes], preferred_element_type=F32
        )
        total = part if total is None else total + part
    return total


def conv_kernel(core, y, own, other, p0, p1, p2, p3, taps, convolved_far, moments_far, padded, convolved, moments, semaphores):
    pieces = (p0, p1, p2, p3)

    def rows_of(rows):
        both = by_piece(y[0], rows, pieces, slice(0, 256))
        return (both[:, :128] * jax.nn.sigmoid(both[:, 128:])).astype(BF16).astype(F32)

    first, second = rows_of(own), rows_of(other)
    for k in range(4):
        mine = pl.ds(pl.multiple_of(16 + k * 192 + core[0] * 96, 16), 96)
        theirs = pl.ds(pl.multiple_of(16 + k * 192 + (1 - core[0]) * 96, 16), 96)
        padded[mine, :] = first[k * 112 : k * 112 + 96, :]
        padded[theirs, :] = second[k * 112 : k * 112 + 96, :]
    is_second = jnp.full((16, 128), core[0], jnp.int32) == 1
    padded[0:16, :] = jnp.where(is_second, first[432:448, :], second[432:448, :])
    padded[784:800, :] = jnp.where(is_second, second[96:112, :], first[96:112, :])
    ones = jnp.ones((8, 128), F32)
    rows = 128
    for i in range(6):
        total = None
        for j in range(31):
            start = i * rows + j + 1
            term = taps[j : j + 1, :] * padded[start : start + rows, :]
            total = term if total is None else total + term
        convolved[i * rows : (i + 1) * rows, :] = total
        highest = lax.Precision.HIGHEST
        s1 = lax.dot_general(ones, total, NT, precision=highest, preferred_element_type=F32)
        s2 = lax.dot_general(ones, total * total, NT, precision=highest, preferred_element_type=F32)
        moments[0:1, i * rows : (i + 1) * rows] = s1[0:1]
        moments[1:2, i * rows : (i + 1) * rows] = s2[0:1]
    pairs = ((convolved, convolved_far), (moments, moments_far))
    for copy in start_copies(pairs, semaphores):
        copy.wait()


def within_kernel(
    core,
    y,
    own,
    other,
    p0,
    p1,
    p2,
    p3,
    both_far,
    running_far,
    pair_far,
    within_far,
    pair,
    within,
    both,
    running,
    semaphores,
):
    loads = start_copies(((both_far, both), (running_far, running)), semaphores)
    pieces = (p0, p1, p2, p3)
    put_rows(
        core[0],
        by_piece(y[0], own, pieces, slice(0, 256)),
        by_piece(y[0], other, pieces, slice(0, 256)),
        pair,
    )
    for load in loads:
        load.wait()
    (kept,) = start_copies(((pair, pair_far),), semaphores)
    logs = running[...]
    turned = jnp.transpose(logs)
    k = (both[:, 0:128].astype(F32) * 0.125).astype(BF16)
    v = both[:, 128:256]
    rows = 128
    zero = jnp.zeros((), BF16)
    masks = [lane_is_second(768) == bool(h) for h in range(2)]
    head_values = [jnp.where(mask, v, zero) for mask in masks]
    for i in range(6):
        at = slice(i * rows, (i + 1) * rows)
        q = pair[at, 0:128]
        diagonal = lax.broadcasted_iota(jnp.int32, (rows, 768), 1) == (
            lax.broadcasted_iota(jnp.int32, (rows, 768), 0) + i * rows
        )
        total = None
        for h in range(2):
            scores = lax.dot_general(
                jnp.where(masks[h][:rows], q, zero), k, NT, preferred_element_type=F32
            )
            distance = jnp.abs(turned[at, h : h + 1] - logs[h : h + 1, :])
            weights = jnp.exp(-distance) + jnp.where(diagonal, 1.0, 0.0)
            part = jnp.dot(
                (scores * weights).astype(BF16), head_values[h], preferred_element_type=F32
            )
            total = part if total is None else total + part
        within[at, :] = total
    kept.wait()
    (kept,) = start_copies(((within, within_far),), semaphores)
    kept.wait()


def out_rows(y, rows, pieces, spare, write):
    for shift, piece in enumerate(pieces):
        lanes = column_block(y, shift)
        part = lax.dot_general(rows[:, :240], piece[:, 256:496], NT, preferred_element_type=F32)
        part = part + jnp.dot(rows[:, 240:], spare[:, lanes], preferred_element_type=F32)
        write(lanes, part)


def mixers_kernel(
    core,
    y,
    low,
    high,
    p0,
    p1,
    p2,
    p3,
    inner,
    outer,
    pair_far,
    within_far,
    running_far,
    start_far,
    head_gain_far,
    convolved_far,
    moments_0,
    moments_1,
    moments_2,
    moments_3,
    channel_gain_far,
    mine,
    sent,
    spare,
    rows_in,
    pair,
    within,
    running,
    start,
    head_gain,
    convolved,
    moments,
    channel_gain,
    semaphores,
):
    pieces = (p0, p1, p2, p3)
    loads = start_copies(
        (
            (start_far, start),
            (running_far, running),
            (moments_0, moments.at[0]),
            (moments_1, moments.at[1]),
            (moments_2, moments.at[2]),
            (moments_3, moments.at[3]),
            (pair_far, pair),
            (head_gain_far, head_gain),
            (within_far, within),
            (convolved_far, convolved),
            (channel_gain_far, channel_gain),
        ),
        semaphores,
    )
    near = scan_states(inner, 16, low[0])
    far = scan_states(outer, 4, high[0])
    second = lane_is_second(64)
    for yy in range(4):
        for zh in range(4):
            where = yy * 512 + zh * 128
            spare[:, where : where + 128] = outer[zh, 144 + yy * 16 : 160 + yy * 16, :]
    for load in loads:
        load.wait()

    def entering(way):
        begun = jnp.concatenate([start[way, 0], start[way, 1]], axis=1)
        state = far[way][0] + jnp.exp(far[way][1]) * begun
        state = near[way][0] + jnp.exp(near[way][1]) * state
        return jnp.concatenate(
            [jnp.where(second, 0.0, state), jnp.where(second, state, 0.0)], axis=0
        ).astype(BF16)

    forward, backward = entering(0), entering(1)
    turned = jnp.transpose(running[...])
    sums = moments[0] + moments[1] + (moments[2] + moments[3])
    sums = jnp.transpose(jnp.concatenate([sums, jnp.zeros((6, 768), F32)], axis=0)) / DC
    rows = 128
    half = lane_is_second(rows)

    def head_mean(x):
        first = jnp.sum(jnp.where(half, 0.0, x), axis=1, keepdims=True)
        last = jnp.sum(jnp.where(half, x, 0.0), axis=1, keepdims=True)
        return jnp.where(half, last, first) / 64

    for i in range(6):
        at = slice(i * rows, (i + 1) * rows)
        q = pair[at, 0:128]
        log = jnp.where(half, turned[at, 1:2], turned[at, 0:1])
        closing = jnp.where(half[0:1], turned[767:768, 1:2], turned[767:768, 0:1])
        retained = within[at, :] + jnp.exp(log) * jnp.dot(
            q, forward, preferred_element_type=F32
        )
        retained = retained + jnp.exp(closing - log) * jnp.dot(
            q, backward, preferred_element_type=F32
        )
        centred = retained - head_mean(retained)
        normed = centred * lax.rsqrt(head_mean(centred * centred) + EPSILON)
        gate = jax.nn.silu(pair[at, 128:256].astype(F32))
        rows_in[at, 128:256] = (normed * head_gain[...] * gate).astype(BF16)
        average, squares = sums[at, 0:1], sums[at, 1:2]
        scaled = (convolved[at, :] - average) * lax.rsqrt(squares - average * average + EPSILON)
        rows_in[at, 0:128] = jax.nn.silu(scaled * channel_gain[...]).astype(BF16)

    def half_of(which):
        return jnp.concatenate(
            [
                rows_in[pl.ds(pl.multiple_of(k * 192 + which * 96, 32), 96), :]
                for k in range(4)
            ],
            axis=0,
        )

    mine[...] = half_of(core[0])

    def write(lanes, part):
        sent[:, lanes] = part.astype(BF16)

    out_rows(y[0], half_of(1 - core[0]), pieces, spare, write)


def join_kernel(y, mine, arrived, p0, p1, p2, p3, spare, out):
    def write(lanes, part):
        out[:, lanes] = (part + arrived[:, lanes].astype(F32)).astype(BF16)

    out_rows(y[0], mine[...], (p0, p1, p2, p3), spare, write)


def ring(x, axis, shift):
    count = lax.axis_size(axis)
    return lax.ppermute(x, axis, [(i, (i + shift) % count) for i in range(count)])


def body(
    tokens,
    input_gain,
    branch_value,
    branch_gate,
    query_weight,
    key_weight,
    value_weight,
    swish_weight,
    kernel_taps,
    channel_gain,
    decay_logs,
    start_state,
    head_gain,
    output_conv,
    output_heads,
):
    core = lax.axis_index("c").astype(jnp.int32)[None]
    y = lax.axis_index("y").astype(jnp.int32)[None]
    high = lax.axis_index("zh").astype(jnp.int32)[None]
    low = lax.axis_index(("zl", "y")).astype(jnp.int32)[None]

    place = lax.axis_index(("x", "c"))
    count = lax.axis_size(SP)
    edge = lax.ppermute(
        jnp.where(place == 7, tokens[80:96], tokens[0:16]),
        ALL,
        [(i * 8 + 7, i * 8 + 15) for i in range(count - 1)]
        + [(i * 8 + 8, i * 8) for i in range(count - 1)],
    )
    shard = call(
        shard_kernel,
        shape((32, 1008), BF16),
        (),
        (
            key_weight,
            value_weight,
            branch_value,
            branch_gate,
            query_weight,
            swish_weight,
            output_conv.T,
            output_heads.T,
        ),
        grant=56,
    )
    normed = call(
        norm_kernel,
        shape((4, 112, 2048), BF16),
        (),
        (tokens, edge, input_gain[None]),
        scratch=(
            pltpu.VMEM((96, 2048), BF16),
            pltpu.VMEM((1, 2048), F32),
            pltpu.VMEM((112, 2048), BF16),
            pltpu.SemaphoreType.DMA((4,)),
        ),
        far=(0, 2),
        out_far=(0,),
    )
    shard, normed = lax.optimization_barrier((shard, normed))
    own = lax.all_to_all(normed, "x", 0, 0, tiled=True).reshape(448, 2048)
    rows = lax.all_gather(shard, ("zh", "zl"), axis=0, tiled=True)
    own, rows = lax.optimization_barrier((own, rows))
    other = ring(own, "c", 1)
    state_piece, gate_piece, rest_piece = call(
        split_kernel,
        (
            shape((4, 512, 256), BF16),
            shape((512, 256), BF16),
            shape((512, 496), BF16),
        ),
        (),
        (rows,),
        scratch=(pltpu.SemaphoreType.DMA((6,)),),
        far=(0,),
        out_far=(0,),
    )
    state_weight = lax.all_to_all(state_piece, "y", 0, 0, tiled=True).reshape(2048, 256)
    gate_pieces = (gate_piece,) + tuple(ring(gate_piece, "y", d) for d in (1, 2, 3))
    rest_pieces = (rest_piece,) + tuple(ring(rest_piece, "y", d) for d in (1, 2, 3))

    running = jnp.cumsum(decay_logs, axis=1)
    running = jnp.concatenate([running, jnp.zeros((6, 768), F32)], axis=0)

    full = shape((768, 128), F32)
    tail = jnp.pad(output_heads[112:], ((0, 0), (0, 96)))
    both, sent = call(
        states_kernel,
        (shape((768, 256), BF16), shape((16, 160, 128), BF16)),
        (core,),
        (own, other, state_weight, running, tail),
        scratch=(
            pltpu.VMEM((768, 256), BF16),
            pltpu.VMEM((160, 128), BF16),
            pltpu.SemaphoreType.DMA((17,)),
        ),
        out_far=(0, 1),
    )
    inner = lax.all_to_all(sent, ("zl", "y"), 0, 0, tiled=True)
    sent = call(
        level_kernel,
        shape((4, 208, 128), BF16),
        (low,),
        (inner,),
        scratch=(pltpu.VMEM((208, 128), BF16), pltpu.SemaphoreType.DMA((4,))),
        out_far=(0,),
    )
    outer = lax.all_to_all(sent, "zh", 0, 0, tiled=True)
    convolved, moments = call(
        conv_kernel,
        (full, shape((2, 768), F32)),
        (core, y),
        (own, other, *gate_pieces, kernel_taps),
        scratch=(
            pltpu.VMEM((800, 128), F32),
            pltpu.VMEM((768, 128), F32),
            pltpu.VMEM((2, 768), F32),
            pltpu.SemaphoreType.DMA((2,)),
        ),
        out_far=(0, 1),
    )
    partner = ring(moments, "c", 1)
    moments = moments + partner
    moments = (moments,) + tuple(ring(moments, "x", d) for d in (1, 2, 3))
    pair, within = call(
        within_kernel,
        (shape((768, 256), BF16), full),
        (core, y),
        (own, other, *rest_pieces, both, running),
        scratch=(
            pltpu.VMEM((768, 256), BF16),
            pltpu.VMEM((768, 128), F32),
            pltpu.VMEM((768, 256), BF16),
            pltpu.VMEM((8, 768), F32),
            pltpu.SemaphoreType.DMA((2,)),
        ),
        far=(6, 7),
        out_far=(0, 1),
    )
    mine, sent, spare = call(
        mixers_kernel,
        (shape((384, 256), BF16), shape((384, 2048), BF16), shape((16, 2048), BF16)),
        (core, y, low, high),
        (
            *rest_pieces,
            inner,
            outer,
            pair,
            within,
            running,
            start_state,
            head_gain[None],
            convolved,
            *moments,
            channel_gain[None],
        ),
        scratch=(
            pltpu.VMEM((768, 256), BF16),
            pltpu.VMEM((768, 256), BF16),
            pltpu.VMEM((768, 128), F32),
            pltpu.VMEM((8, 768), F32),
            pltpu.VMEM((2, 2, 64, 64), F32),
            pltpu.VMEM((1, 128), F32),
            pltpu.VMEM((768, 128), F32),
            pltpu.VMEM((4, 2, 768), F32),
            pltpu.VMEM((1, 128), F32),
            pltpu.SemaphoreType.DMA((11,)),
        ),
        far=tuple(range(6, 17)),
    )
    arrived = ring(sent, "c", 1)
    joined = call(join_kernel, shape((384, 2048), BF16), (y,), (mine, arrived, *rest_pieces, spare))
    parts = lax.all_to_all(joined.reshape(4, 96, 2048), "x", 0, 0, tiled=True)
    return call(last_kernel, shape((96, 2048), BF16), (), (parts,))


def solution(mesh):
    split = Mesh(mesh.devices.reshape(4, 4, 4, 4, 2), ALL)
    in_specs = (
        P(ALL, None),
        P(),
        P(SP, ("x", "c")),
        P(SP, ("x", "c")),
        P(SP, ("x", "c")),
        P(SP, ("x", "c")),
        P(SP, ("x", "c")),
        P(SP, ("x", "c")),
        P(None, ("x", "c")),
        P(("x", "c")),
        P(("x", "c"), SP),
        P(None, ("x", "c"), None, None),
        P(("x", "c")),
        P(("x", "c"), SP),
        P(("x", "c"), SP),
    )

    return jax.shard_map(
        body, mesh=split, in_specs=in_specs, out_specs=P(ALL, None), check_vma=False
    )
```

```python
import jax
import jax.numpy as jnp
from jax import lax
from jax.experimental import pallas as pl
from jax.experimental.pallas import tpu as pltpu
from jax.sharding import Mesh
from jax.sharding import PartitionSpec as P

DC = 1024
EPSILON = 1e-06
F32 = jnp.float32
BF16 = jnp.bfloat16
SP = ("zh", "zl", "y")
ALL = ("zh", "zl", "y", "x", "c")
NT = (((1,), (1,)), ((), ()))
TN = (((0,), (0,)), ((), ()))
VMEM = pl.BlockSpec(memory_space=pltpu.VMEM)
SMEM = pl.BlockSpec(memory_space=pltpu.SMEM)
HBM = pl.BlockSpec(memory_space=pltpu.HBM)


def call(kernel, out_shape, scalars, arrays, scratch=(), grant=20, far=(), out_far=(), aliases={}):
    def specs(count, away):
        return [HBM if i in away else VMEM for i in range(count)]

    arrays = [
        pltpu.with_memory_space_constraint(a, pltpu.HBM) if i in far else a
        for i, a in enumerate(arrays)
    ]
    if isinstance(out_shape, tuple):
        out_shape = tuple(
            pltpu.HBM(s.shape, s.dtype) if i in out_far else s for i, s in enumerate(out_shape)
        )
    elif out_far:
        out_shape = pltpu.HBM(out_shape.shape, out_shape.dtype)
    outs = specs(len(out_shape), out_far) if isinstance(out_shape, tuple) else specs(1, out_far)[0]
    return pl.pallas_call(
        kernel,
        out_shape=out_shape,
        in_specs=[SMEM] * len(scalars) + specs(len(arrays), far),
        out_specs=outs,
        scratch_shapes=scratch,
        compiler_params=pltpu.CompilerParams(vmem_limit_bytes=grant * 1024 * 1024),
        input_output_aliases=aliases,
    )(*scalars, *arrays)


def start_copies(pairs, semaphores):
    copies = [
        pltpu.make_async_copy(source, target, semaphores.at[i])
        for i, (source, target) in enumerate(pairs)
    ]
    for copy in copies:
        copy.start()
    return copies


def shape(dims, dtype):
    return jax.ShapeDtypeStruct(dims, dtype)


def swap_groups(read, write, rows):
    group = lax.broadcasted_iota(jnp.int32, (rows, 128), 1) // 32
    for outer in range(4):
        for inner in range(4):
            made = None
            for k in range(4):
                moved = read(outer, k)
                turn = ((k - inner) * 32) % 128
                if turn:
                    moved = pltpu.roll(moved, turn, 1)
                made = moved if made is None else jnp.where(group == k, moved, made)
            write(outer, inner, made)


def shard_kernel(k, v, bv, bg, q, s, oc, oh, out):
    for i, part in enumerate((k, v, bv, bg, q, s, oc)):
        out[:, i * 128 : i * 128 + 128] = part[...]
    out[:, 896:1008] = oh[:, 0:112]


def normed_rows(source, at, gain, out, to):
    rows = 16
    x = source[at, :].astype(F32)
    inverse = lax.rsqrt(jnp.mean(x * x, axis=1, keepdims=True) + EPSILON)
    normed = x * inverse * gain[...]

    def read(zh, zl):
        z = zh * 4 + zl
        return normed[:, z * 128 : z * 128 + 128]

    def write(zh, y, made):
        where = (y * 4 + zh) * 128
        out[to, where : where + 128] = made.astype(BF16)

    swap_groups(read, write, rows)


def norm_kernel(tokens_far, gain_far, out_far, tokens, gain, out, semaphores):
    for copy in start_copies(((tokens_far, tokens), (gain_far, gain)), semaphores):
        copy.wait()

    def step(i, carry):
        at = pl.ds(pl.multiple_of(i * 16, 16), 16)
        normed_rows(tokens, at, gain, out, at)
        return carry

    lax.fori_loop(0, 6, step, 0, unroll=2)
    pairs = [(out, out_far.at[k, 0:96, :]) for k in range(4)]
    for copy in start_copies(pairs, semaphores):
        copy.wait()


def edge_kernel(edge, gain, given_far, out_far, out, semaphores):
    normed_rows(edge, slice(0, 16), gain, out, slice(0, 16))
    pairs = [(out, out_far.at[k, 96:112, :]) for k in range(4)]
    for copy in start_copies(pairs, semaphores):
        copy.wait()


def last_kernel(parts, out):
    rows = 16

    def step(i, carry):
        at = pl.ds(pl.multiple_of(i * rows, rows), rows)
        total = parts[0, at, :].astype(F32)
        for k in range(1, 4):
            total = total + parts[k, at, :].astype(F32)

        def read(zh, y):
            where = (y * 4 + zh) * 128
            return total[:, where : where + 128]

        def write(zh, zl, made):
            where = (zh * 4 + zl) * 128
            out[at, where : where + 128] = made.astype(BF16)

        swap_groups(read, write, rows)
        return carry

    lax.fori_loop(0, 6, step, 0, unroll=2)


def lane_is_second(rows):
    return lax.broadcasted_iota(jnp.int32, (rows, 128), 1) >= 64


def by_lane(running):
    turned = jnp.transpose(running)
    return jnp.where(lane_is_second(turned.shape[0]), turned[:, 1:2], turned[:, 0:1])


def put_rows(core, own, other, target):
    for k in range(4):
        mine = pl.ds(pl.multiple_of(k * 192 + core * 96, 32), 96)
        theirs = pl.ds(pl.multiple_of(k * 192 + (1 - core) * 96, 32), 96)
        part = slice(k * 112, k * 112 + 96)
        target[mine, :] = own[part, :].astype(BF16)
        target[theirs, :] = other[part, :].astype(BF16)


def states_kernel(core, own, other, weight, running, tail, both_far, message, both, semaphores):
    w = weight[...]
    put_rows(
        core[0],
        jnp.dot(own[...], w, preferred_element_type=F32),
        jnp.dot(other[...], w, preferred_element_type=F32),
        both,
    )
    (kept,) = start_copies(((both, both_far),), semaphores)
    logs = by_lane(running[...])
    closing = logs[767:768, :]
    k = both[:, 0:128].astype(F32) * 0.125
    v = both[:, 128:256]
    second = lane_is_second(64)
    ahead = lax.dot_general(
        (k * jnp.exp(closing - logs)).astype(BF16), v, TN, preferred_element_type=F32
    )
    back = lax.dot_general((k * jnp.exp(logs)).astype(BF16), v, TN, preferred_element_type=F32)
    parts = (
        (slice(0, 64), jnp.where(second, ahead[64:, :], ahead[:64, :]).astype(BF16)),
        (slice(64, 128), jnp.where(second, back[64:, :], back[:64, :]).astype(BF16)),
        (slice(128, 144), log_rows(closing)),
        (slice(144, 160), tail[...]),
    )
    for at, part in parts:
        for copy in range(16):
            message[copy, at, :] = part
    kept.wait()


def log_rows(log):
    high = log.astype(BF16)
    low = (log - high.astype(F32)).astype(BF16)
    first = lax.broadcasted_iota(jnp.int32, (16, 128), 0) < 8
    return jnp.where(first, high.astype(F32), low.astype(F32)).astype(BF16)


def scan_states(gathered, count, position):
    def log_of(m):
        return gathered[m, 128:129, :].astype(F32) + gathered[m, 136:137, :].astype(F32)

    def one_way(order, rows):
        state = jnp.zeros((64, 128), F32)
        log = jnp.zeros((1, 128), F32)
        held, held_log = state, log
        for m in order:
            here = position == m
            held = jnp.where(here, state, held)
            held_log = jnp.where(here, log, held_log)
            own = log_of(m)
            state = jnp.exp(own) * state + gathered[m, rows, :].astype(F32)
            log = log + own
        return held, held_log, state, log

    ahead = one_way(range(count), slice(0, 64))
    back = one_way(reversed(range(count)), slice(64, 128))
    return ahead, back


def level_kernel(position, gathered, message_far, message, semaphores):
    ahead, back = scan_states(gathered, 16, position[0])
    parts = [
        (slice(0, 64), ahead[2].astype(BF16)),
        (slice(64, 128), back[2].astype(BF16)),
        (slice(128, 144), log_rows(ahead[3])),
    ]
    group = lax.broadcasted_iota(jnp.int32, (16, 128), 1) // 32
    for y in range(4):
        made = gathered[y, 144:160, :].astype(F32)
        for zl in range(1, 4):
            moved = pltpu.roll(gathered[zl * 4 + y, 144:160, :].astype(F32), zl * 32, 1)
            made = jnp.where(group == zl, moved, made)
        parts.append((slice(144 + y * 16, 160 + y * 16), made.astype(BF16)))
    for at, part in parts:
        message[at, :] = part
    for copy in start_copies([(message, message_far.at[k]) for k in range(4)], semaphores):
        copy.wait()


def column_block(position, shift):
    return pl.ds(pl.multiple_of(((position + 4 - shift) % 4) * 512, 512), 512)


def by_piece(y, rows, pieces, lanes):
    total = None
    for shift, piece in enumerate(pieces):
        part = jnp.dot(
            rows[:, column_block(y, shift)], piece[:, lanes], preferred_element_type=F32
        )
        total = part if total is None else total + part
    return total


def conv_kernel(core, y, own, other, p0, p1, p2, p3, taps, convolved_far, moments_far, padded, convolved, moments, semaphores):
    pieces = (p0, p1, p2, p3)

    def rows_of(rows):
        both = by_piece(y[0], rows, pieces, slice(0, 256))
        return (both[:, :128] * jax.nn.sigmoid(both[:, 128:])).astype(BF16).astype(F32)

    first, second = rows_of(own), rows_of(other)
    for k in range(4):
        mine = pl.ds(pl.multiple_of(16 + k * 192 + core[0] * 96, 16), 96)
        theirs = pl.ds(pl.multiple_of(16 + k * 192 + (1 - core[0]) * 96, 16), 96)
        padded[mine, :] = first[k * 112 : k * 112 + 96, :]
        padded[theirs, :] = second[k * 112 : k * 112 + 96, :]
    is_second = jnp.full((16, 128), core[0], jnp.int32) == 1
    padded[0:16, :] = jnp.where(is_second, first[432:448, :], second[432:448, :])
    padded[784:800, :] = jnp.where(is_second, second[96:112, :], first[96:112, :])
    ones = jnp.ones((8, 128), F32)
    rows = 128
    for i in range(6):
        total = None
        for j in range(31):
            start = i * rows + j + 1
            term = taps[j : j + 1, :] * padded[start : start + rows, :]
            total = term if total is None else total + term
        convolved[i * rows : (i + 1) * rows, :] = total
        highest = lax.Precision.HIGHEST
        s1 = lax.dot_general(ones, total, NT, precision=highest, preferred_element_type=F32)
        s2 = lax.dot_general(ones, total * total, NT, precision=highest, preferred_element_type=F32)
        moments[0:1, i * rows : (i + 1) * rows] = s1[0:1]
        moments[1:2, i * rows : (i + 1) * rows] = s2[0:1]
    pairs = ((convolved, convolved_far), (moments, moments_far))
    for copy in start_copies(pairs, semaphores):
        copy.wait()


def out_rows(y, rows, pieces, spare, write):
    for shift, piece in enumerate(pieces):
        lanes = column_block(y, shift)
        part = lax.dot_general(rows[:, :240], piece[:, 256:496], NT, preferred_element_type=F32)
        part = part + jnp.dot(rows[:, 240:], spare[:, lanes], preferred_element_type=F32)
        write(lanes, part)


def mixers_kernel(
    core,
    y,
    low,
    high,
    own,
    other,
    p0,
    p1,
    p2,
    p3,
    inner,
    outer,
    both_far,
    running_far,
    start_far,
    head_gain_far,
    convolved_far,
    moments_far,
    channel_gain_far,
    mine,
    sent,
    spare,
    pair,
    rows_in,
    both,
    running,
    start,
    head_gain,
    convolved,
    moments,
    channel_gain,
    semaphores,
):
    pieces = (p0, p1, p2, p3)
    loads = start_copies(
        (
            (both_far, both),
            (running_far, running),
            (start_far, start),
            (head_gain_far, head_gain),
            (convolved_far, convolved),
            (moments_far, moments),
            (channel_gain_far, channel_gain),
        ),
        semaphores,
    )
    put_rows(
        core[0],
        by_piece(y[0], own, pieces, slice(0, 256)),
        by_piece(y[0], other, pieces, slice(0, 256)),
        pair,
    )
    for load in loads:
        load.wait()
    near = scan_states(inner, 16, low[0])
    far = scan_states(outer, 4, high[0])
    second = lane_is_second(64)

    def entering(way):
        begun = jnp.concatenate([start[way, 0], start[way, 1]], axis=1)
        state = far[way][0] + jnp.exp(far[way][1]) * begun
        state = near[way][0] + jnp.exp(near[way][1]) * state
        return jnp.concatenate(
            [jnp.where(second, 0.0, state), jnp.where(second, state, 0.0)], axis=0
        ).astype(BF16)

    forward, backward = entering(0), entering(1)
    logs = running[...]
    turned = jnp.transpose(logs)
    sums = moments[0]
    for k in range(1, 8):
        sums = sums + moments[k]
    sums = jnp.transpose(jnp.concatenate([sums, jnp.zeros((6, 768), F32)], axis=0)) / DC
    for yy in range(4):
        for zh in range(4):
            where = yy * 512 + zh * 128
            spare[:, where : where + 128] = outer[zh, 144 + yy * 16 : 160 + yy * 16, :]

    k = (both[:, 0:128].astype(F32) * 0.125).astype(BF16)
    v = both[:, 128:256]
    rows = 128
    zero = jnp.zeros((), BF16)
    half = lane_is_second(rows)
    masks = [lane_is_second(768) == bool(h) for h in range(2)]
    head_values = [jnp.where(mask, v, zero) for mask in masks]

    def head_mean(x):
        first = jnp.sum(jnp.where(half, 0.0, x), axis=1, keepdims=True)
        last = jnp.sum(jnp.where(half, x, 0.0), axis=1, keepdims=True)
        return jnp.where(half, last, first) / 64

    for i in range(6):
        at = slice(i * rows, (i + 1) * rows)
        q = pair[at, 0:128]
        log = jnp.where(half, turned[at, 1:2], turned[at, 0:1])
        closing = jnp.where(half[0:1], turned[767:768, 1:2], turned[767:768, 0:1])
        retained = jnp.exp(log) * jnp.dot(q, forward, preferred_element_type=F32)
        retained = retained + jnp.exp(closing - log) * jnp.dot(
            q, backward, preferred_element_type=F32
        )
        for h in range(2):
            scores = lax.dot_general(
                jnp.where(masks[h][:rows], q, zero), k, NT, preferred_element_type=F32
            )
            distance = jnp.abs(turned[at, h : h + 1] - logs[h : h + 1, :])
            weights = jnp.exp(-distance)
            retained = retained + jnp.dot(
                (scores * weights).astype(BF16), head_values[h], preferred_element_type=F32
            )
        same = q.astype(F32) * k[at, :].astype(F32)
        retained = retained + 64 * head_mean(same) * v[at, :].astype(F32)
        centred = retained - head_mean(retained)
        normed = centred * lax.rsqrt(head_mean(centred * centred) + EPSILON)
        gate = jax.nn.silu(pair[at, 128:256].astype(F32))
        rows_in[at, 128:256] = (normed * head_gain[...] * gate).astype(BF16)
        average, squares = sums[at, 0:1], sums[at, 1:2]
        scaled = (convolved[at, :] - average) * lax.rsqrt(squares - average * average + EPSILON)
        rows_in[at, 0:128] = jax.nn.silu(scaled * channel_gain[...]).astype(BF16)

    def half_of(which):
        return jnp.concatenate(
            [
                rows_in[pl.ds(pl.multiple_of(k * 192 + which * 96, 32), 96), :]
                for k in range(4)
            ],
            axis=0,
        )

    mine[...] = half_of(core[0])

    def write(lanes, part):
        sent[:, lanes] = part.astype(BF16)

    out_rows(y[0], half_of(1 - core[0]), pieces, spare, write)


def join_kernel(y, mine, arrived, p0, p1, p2, p3, spare, out):
    def write(lanes, part):
        out[:, lanes] = (part + arrived[:, lanes].astype(F32)).astype(BF16)

    out_rows(y[0], mine[...], (p0, p1, p2, p3), spare, write)


def ring(x, axis, shift):
    count = lax.axis_size(axis)
    return lax.ppermute(x, axis, [(i, (i + shift) % count) for i in range(count)])


def copies(x, axes, count):
    return lax.all_to_all(
        jnp.broadcast_to(x[None], (count, *x.shape)), axes, 0, 0, tiled=True
    )


def body(
    tokens,
    input_gain,
    branch_value,
    branch_gate,
    query_weight,
    key_weight,
    value_weight,
    swish_weight,
    kernel_taps,
    channel_gain,
    decay_logs,
    start_state,
    head_gain,
    output_conv,
    output_heads,
):
    core = lax.axis_index("c").astype(jnp.int32)[None]
    y = lax.axis_index("y").astype(jnp.int32)[None]
    high = lax.axis_index("zh").astype(jnp.int32)[None]
    low = lax.axis_index(("zl", "y")).astype(jnp.int32)[None]

    place = lax.axis_index(("x", "c"))
    count = lax.axis_size(SP)
    edge = lax.ppermute(
        jnp.where(place == 7, tokens[80:96], tokens[0:16]),
        ALL,
        [(i * 8 + 7, i * 8 + 15) for i in range(count - 1)]
        + [(i * 8 + 8, i * 8) for i in range(count - 1)],
    )
    shard = call(
        shard_kernel,
        shape((32, 1008), BF16),
        (),
        (
            key_weight,
            value_weight,
            branch_value,
            branch_gate,
            query_weight,
            swish_weight,
            output_conv.T,
            output_heads.T,
        ),
        grant=56,
    )
    running = jnp.cumsum(decay_logs, axis=1)
    running = jnp.concatenate([running, jnp.zeros((6, 768), F32)], axis=0)
    tail = jnp.pad(output_heads[112:], ((0, 0), (0, 96)))
    normed = call(
        norm_kernel,
        shape((4, 112, 2048), BF16),
        (),
        (tokens, input_gain[None]),
        scratch=(
            pltpu.VMEM((96, 2048), BF16),
            pltpu.VMEM((1, 2048), F32),
            pltpu.VMEM((96, 2048), BF16),
            pltpu.SemaphoreType.DMA((4,)),
        ),
        far=(0, 1),
        out_far=(0,),
    )
    edge, normed, running, tail = lax.optimization_barrier((edge, normed, running, tail))
    normed = call(
        edge_kernel,
        shape((4, 112, 2048), BF16),
        (),
        (edge, input_gain[None], normed),
        scratch=(pltpu.VMEM((16, 2048), BF16), pltpu.SemaphoreType.DMA((4,))),
        far=(2,),
        out_far=(0,),
        aliases={2: 0},
    )
    shard, normed = lax.optimization_barrier((shard, normed))
    own = lax.all_to_all(normed, "x", 0, 0, tiled=True).reshape(448, 2048)
    rows = lax.all_gather(shard, ("zh", "zl"), axis=0, tiled=True)
    own, rows = lax.optimization_barrier((own, rows))
    other = ring(own, "c", 1)
    state_weight = copies(rows[:, :256], "y", 4).reshape(2048, 256)
    gate_piece, rest_piece = rows[:, 256:512], rows[:, 512:]
    gate_pieces = (gate_piece,) + tuple(ring(gate_piece, "y", d) for d in (1, 2, 3))
    rest_pieces = (rest_piece,) + tuple(ring(rest_piece, "y", d) for d in (1, 2, 3))

    full = shape((768, 128), F32)
    both, sent = call(
        states_kernel,
        (shape((768, 256), BF16), shape((16, 160, 128), BF16)),
        (core,),
        (own, other, state_weight, running, tail),
        scratch=(pltpu.VMEM((768, 256), BF16), pltpu.SemaphoreType.DMA((1,))),
        out_far=(0,),
    )
    inner = lax.all_to_all(sent, ("zl", "y"), 0, 0, tiled=True)
    sent = call(
        level_kernel,
        shape((4, 208, 128), BF16),
        (low,),
        (inner,),
        scratch=(pltpu.VMEM((208, 128), BF16), pltpu.SemaphoreType.DMA((4,))),
        out_far=(0,),
    )
    outer = lax.all_to_all(sent, "zh", 0, 0, tiled=True)
    convolved, moments = call(
        conv_kernel,
        (full, shape((2, 768), F32)),
        (core, y),
        (own, other, *gate_pieces, kernel_taps),
        scratch=(
            pltpu.VMEM((800, 128), F32),
            pltpu.VMEM((768, 128), F32),
            pltpu.VMEM((2, 768), F32),
            pltpu.SemaphoreType.DMA((2,)),
        ),
        out_far=(0, 1),
    )
    moments = lax.all_gather(moments, ("x", "c"))
    mine, sent, spare = call(
        mixers_kernel,
        (shape((384, 256), BF16), shape((384, 2048), BF16), shape((16, 2048), BF16)),
        (core, y, low, high),
        (
            own,
            other,
            *rest_pieces,
            inner,
            outer,
            both,
            running,
            start_state,
            head_gain[None],
            convolved,
            moments,
            channel_gain[None],
        ),
        scratch=(
            pltpu.VMEM((768, 256), BF16),
            pltpu.VMEM((768, 256), BF16),
            pltpu.VMEM((768, 256), BF16),
            pltpu.VMEM((8, 768), F32),
            pltpu.VMEM((2, 2, 64, 64), F32),
            pltpu.VMEM((1, 128), F32),
            pltpu.VMEM((768, 128), F32),
            pltpu.VMEM((8, 2, 768), F32),
            pltpu.VMEM((1, 128), F32),
            pltpu.SemaphoreType.DMA((7,)),
        ),
        far=(8, 9, 10, 11, 12, 13, 14),
    )
    arrived = ring(sent, "c", 1)
    joined = call(join_kernel, shape((384, 2048), BF16), (y,), (mine, arrived, *rest_pieces, spare))
    parts = lax.all_to_all(joined.reshape(4, 96, 2048), "x", 0, 0, tiled=True)
    return call(last_kernel, shape((96, 2048), BF16), (), (parts,))


def solution(mesh):
    split = Mesh(mesh.devices.reshape(4, 4, 4, 4, 2), ALL)
    in_specs = (
        P(ALL, None),
        P(),
        P(SP, ("x", "c")),
        P(SP, ("x", "c")),
        P(SP, ("x", "c")),
        P(SP, ("x", "c")),
        P(SP, ("x", "c")),
        P(SP, ("x", "c")),
        P(None, ("x", "c")),
        P(("x", "c")),
        P(("x", "c"), SP),
        P(None, ("x", "c"), None, None),
        P(("x", "c")),
        P(("x", "c"), SP),
        P(("x", "c"), SP),
    )

    return jax.shard_map(
        body, mesh=split, in_specs=in_specs, out_specs=P(ALL, None), check_vma=False
    )
```

```python
import jax
import jax.numpy as jnp
from jax import lax
from jax.experimental import pallas as pl
from jax.experimental.pallas import tpu as pltpu
from jax.sharding import Mesh
from jax.sharding import PartitionSpec as P

DC = 1024
EPSILON = 1e-06
F32 = jnp.float32
BF16 = jnp.bfloat16
SP = ("zh", "zl", "y")
ALL = ("zh", "zl", "y", "x", "c")
NT = (((1,), (1,)), ((), ()))
TN = (((0,), (0,)), ((), ()))
VMEM = pl.BlockSpec(memory_space=pltpu.VMEM)
SMEM = pl.BlockSpec(memory_space=pltpu.SMEM)
HBM = pl.BlockSpec(memory_space=pltpu.HBM)


def call(kernel, out_shape, scalars, arrays, scratch=(), grant=20, far=(), out_far=(), aliases={}):
    def specs(count, away):
        return [HBM if i in away else VMEM for i in range(count)]

    arrays = [
        pltpu.with_memory_space_constraint(a, pltpu.HBM) if i in far else a
        for i, a in enumerate(arrays)
    ]
    if isinstance(out_shape, tuple):
        out_shape = tuple(
            pltpu.HBM(s.shape, s.dtype) if i in out_far else s for i, s in enumerate(out_shape)
        )
    elif out_far:
        out_shape = pltpu.HBM(out_shape.shape, out_shape.dtype)
    outs = specs(len(out_shape), out_far) if isinstance(out_shape, tuple) else specs(1, out_far)[0]
    return pl.pallas_call(
        kernel,
        out_shape=out_shape,
        in_specs=[SMEM] * len(scalars) + specs(len(arrays), far),
        out_specs=outs,
        scratch_shapes=scratch,
        compiler_params=pltpu.CompilerParams(vmem_limit_bytes=grant * 1024 * 1024),
        input_output_aliases=aliases,
    )(*scalars, *arrays)


def start_copies(pairs, semaphores):
    copies = [
        pltpu.make_async_copy(source, target, semaphores.at[i])
        for i, (source, target) in enumerate(pairs)
    ]
    for copy in copies:
        copy.start()
    return copies


def shape(dims, dtype):
    return jax.ShapeDtypeStruct(dims, dtype)


def swap_groups(read, write, rows):
    group = lax.broadcasted_iota(jnp.int32, (rows, 128), 1) // 32
    for outer in range(4):
        for inner in range(4):
            made = None
            for k in range(4):
                moved = read(outer, k)
                turn = ((k - inner) * 32) % 128
                if turn:
                    moved = pltpu.roll(moved, turn, 1)
                made = moved if made is None else jnp.where(group == k, moved, made)
            write(outer, inner, made)


def shard_kernel(k, v, bv, bg, q, s, oc, oh, out):
    for i, part in enumerate((k, v, bv, bg, q, s, oc)):
        out[:, i * 128 : i * 128 + 128] = part[...]
    out[:, 896:1008] = oh[:, 0:112]


def normed_rows(source, at, gain, out, to):
    rows = 16
    x = source[at, :].astype(F32)
    inverse = lax.rsqrt(jnp.mean(x * x, axis=1, keepdims=True) + EPSILON)
    normed = x * inverse * gain[...]

    def read(zh, zl):
        z = zh * 4 + zl
        return normed[:, z * 128 : z * 128 + 128]

    def write(zh, y, made):
        where = (y * 4 + zh) * 128
        out[to, where : where + 128] = made.astype(BF16)

    swap_groups(read, write, rows)


def norm_kernel(tokens_far, gain_far, out_far, tokens, gain, out, semaphores):
    for copy in start_copies(((tokens_far, tokens), (gain_far, gain)), semaphores):
        copy.wait()

    def step(i, carry):
        at = pl.ds(pl.multiple_of(i * 16, 16), 16)
        normed_rows(tokens, at, gain, out, at)
        return carry

    lax.fori_loop(0, 6, step, 0, unroll=2)
    pairs = [(out, out_far.at[k, 0:96, :]) for k in range(4)]
    for copy in start_copies(pairs, semaphores):
        copy.wait()


def edge_kernel(edge, gain, given_far, out_far, out, semaphores):
    normed_rows(edge, slice(0, 16), gain, out, slice(0, 16))
    pairs = [(out, out_far.at[k, 96:112, :]) for k in range(4)]
    for copy in start_copies(pairs, semaphores):
        copy.wait()


def last_kernel(parts, out):
    rows = 16

    def step(i, carry):
        at = pl.ds(pl.multiple_of(i * rows, rows), rows)
        total = parts[0, at, :].astype(F32)
        for k in range(1, 4):
            total = total + parts[k, at, :].astype(F32)

        def read(zh, y):
            where = (y * 4 + zh) * 128
            return total[:, where : where + 128]

        def write(zh, zl, made):
            where = (zh * 4 + zl) * 128
            out[at, where : where + 128] = made.astype(BF16)

        swap_groups(read, write, rows)
        return carry

    lax.fori_loop(0, 6, step, 0, unroll=2)


def lane_is_second(rows):
    return lax.broadcasted_iota(jnp.int32, (rows, 128), 1) >= 64


def by_lane(running):
    turned = jnp.transpose(running)
    return jnp.where(lane_is_second(turned.shape[0]), turned[:, 1:2], turned[:, 0:1])


def put_rows(core, own, other, target):
    for k in range(4):
        mine = pl.ds(pl.multiple_of(k * 192 + core * 96, 32), 96)
        theirs = pl.ds(pl.multiple_of(k * 192 + (1 - core) * 96, 32), 96)
        part = slice(k * 112, k * 112 + 96)
        target[mine, :] = own[part, :].astype(BF16)
        target[theirs, :] = other[part, :].astype(BF16)


def states_kernel(
    core, own, other_far, weight, running, tail, both_far, message, both, other, semaphores
):
    (load,) = start_copies(((other_far, other),), semaphores)
    w = weight[...]
    first = jnp.dot(own[...], w, preferred_element_type=F32)
    load.wait()
    put_rows(core[0], first, jnp.dot(other[...], w, preferred_element_type=F32), both)
    (kept,) = start_copies(((both, both_far),), semaphores)
    logs = by_lane(running[...])
    closing = logs[767:768, :]
    k = both[:, 0:128].astype(F32) * 0.125
    v = both[:, 128:256]
    second = lane_is_second(64)
    ahead = lax.dot_general(
        (k * jnp.exp(closing - logs)).astype(BF16), v, TN, preferred_element_type=F32
    )
    back = lax.dot_general((k * jnp.exp(logs)).astype(BF16), v, TN, preferred_element_type=F32)
    parts = (
        (slice(0, 64), jnp.where(second, ahead[64:, :], ahead[:64, :]).astype(BF16)),
        (slice(64, 128), jnp.where(second, back[64:, :], back[:64, :]).astype(BF16)),
        (slice(128, 144), log_rows(closing)),
        (slice(144, 160), tail[...]),
    )
    for at, part in parts:
        for copy in range(16):
            message[copy, at, :] = part
    kept.wait()


def log_rows(log):
    high = log.astype(BF16)
    low = (log - high.astype(F32)).astype(BF16)
    first = lax.broadcasted_iota(jnp.int32, (16, 128), 0) < 8
    return jnp.where(first, high.astype(F32), low.astype(F32)).astype(BF16)


def scan_states(gathered, count, position):
    def log_of(m):
        return gathered[m, 128:129, :].astype(F32) + gathered[m, 136:137, :].astype(F32)

    def one_way(order, rows):
        state = jnp.zeros((64, 128), F32)
        log = jnp.zeros((1, 128), F32)
        held, held_log = state, log
        for m in order:
            here = position == m
            held = jnp.where(here, state, held)
            held_log = jnp.where(here, log, held_log)
            own = log_of(m)
            state = jnp.exp(own) * state + gathered[m, rows, :].astype(F32)
            log = log + own
        return held, held_log, state, log

    ahead = one_way(range(count), slice(0, 64))
    back = one_way(reversed(range(count)), slice(64, 128))
    return ahead, back


def level_kernel(position, gathered, message_far, message, semaphores):
    ahead, back = scan_states(gathered, 16, position[0])
    parts = [
        (slice(0, 64), ahead[2].astype(BF16)),
        (slice(64, 128), back[2].astype(BF16)),
        (slice(128, 144), log_rows(ahead[3])),
    ]
    group = lax.broadcasted_iota(jnp.int32, (16, 128), 1) // 32
    for y in range(4):
        made = gathered[y, 144:160, :].astype(F32)
        for zl in range(1, 4):
            moved = pltpu.roll(gathered[zl * 4 + y, 144:160, :].astype(F32), zl * 32, 1)
            made = jnp.where(group == zl, moved, made)
        parts.append((slice(144 + y * 16, 160 + y * 16), made.astype(BF16)))
    for at, part in parts:
        message[at, :] = part
    for copy in start_copies([(message, message_far.at[k]) for k in range(4)], semaphores):
        copy.wait()


def column_block(position, shift):
    return pl.ds(pl.multiple_of(((position + 4 - shift) % 4) * 512, 512), 512)


def by_piece(y, rows, pieces, lanes):
    total = None
    for shift, piece in enumerate(pieces):
        part = jnp.dot(
            rows[:, column_block(y, shift)], piece[:, lanes], preferred_element_type=F32
        )
        total = part if total is None else total + part
    return total


def conv_kernel(
    core,
    y,
    own,
    other_far,
    p0,
    p1,
    p2,
    p3,
    taps,
    convolved_far,
    moments_far,
    padded,
    convolved,
    moments,
    other,
    semaphores,
):
    (load,) = start_copies(((other_far, other),), semaphores)
    pieces = (p0, p1, p2, p3)

    def rows_of(rows):
        both = by_piece(y[0], rows, pieces, slice(0, 256))
        return (both[:, :128] * jax.nn.sigmoid(both[:, 128:])).astype(BF16).astype(F32)

    first = rows_of(own)
    load.wait()
    second = rows_of(other)
    for k in range(4):
        mine = pl.ds(pl.multiple_of(16 + k * 192 + core[0] * 96, 16), 96)
        theirs = pl.ds(pl.multiple_of(16 + k * 192 + (1 - core[0]) * 96, 16), 96)
        padded[mine, :] = first[k * 112 : k * 112 + 96, :]
        padded[theirs, :] = second[k * 112 : k * 112 + 96, :]
    is_second = jnp.full((16, 128), core[0], jnp.int32) == 1
    padded[0:16, :] = jnp.where(is_second, first[432:448, :], second[432:448, :])
    padded[784:800, :] = jnp.where(is_second, second[96:112, :], first[96:112, :])
    ones = jnp.ones((8, 128), F32)
    rows = 128
    for i in range(6):
        total = None
        for j in range(31):
            start = i * rows + j + 1
            term = taps[j : j + 1, :] * padded[start : start + rows, :]
            total = term if total is None else total + term
        convolved[i * rows : (i + 1) * rows, :] = total
        highest = lax.Precision.HIGHEST
        s1 = lax.dot_general(ones, total, NT, precision=highest, preferred_element_type=F32)
        s2 = lax.dot_general(ones, total * total, NT, precision=highest, preferred_element_type=F32)
        moments[0:1, i * rows : (i + 1) * rows] = s1[0:1]
        moments[1:2, i * rows : (i + 1) * rows] = s2[0:1]
    pairs = ((convolved, convolved_far), (moments, moments_far))
    for copy in start_copies(pairs, semaphores):
        copy.wait()


def out_rows(y, rows, pieces, spare, write):
    for shift, piece in enumerate(pieces):
        lanes = column_block(y, shift)
        part = lax.dot_general(rows[:, :240], piece[:, 256:496], NT, preferred_element_type=F32)
        part = part + jnp.dot(rows[:, 240:], spare[:, lanes], preferred_element_type=F32)
        write(lanes, part)


def mixers_kernel(
    core,
    y,
    low,
    high,
    own,
    other_far,
    p0,
    p1,
    p2,
    p3,
    inner,
    outer,
    both_far,
    running_far,
    start_far,
    head_gain_far,
    convolved_far,
    moments_far,
    channel_gain_far,
    mine,
    sent,
    spare,
    pair,
    rows_in,
    both,
    running,
    start,
    head_gain,
    convolved,
    moments,
    channel_gain,
    other,
    semaphores,
):
    pieces = (p0, p1, p2, p3)
    loads = start_copies(
        (
            (other_far, other),
            (both_far, both),
            (running_far, running),
            (start_far, start),
            (head_gain_far, head_gain),
            (convolved_far, convolved),
            (moments_far, moments),
            (channel_gain_far, channel_gain),
        ),
        semaphores,
    )
    first = by_piece(y[0], own, pieces, slice(0, 256))
    for load in loads:
        load.wait()
    put_rows(core[0], first, by_piece(y[0], other, pieces, slice(0, 256)), pair)
    near = scan_states(inner, 16, low[0])
    far = scan_states(outer, 4, high[0])
    second = lane_is_second(64)

    def entering(way):
        begun = jnp.concatenate([start[way, 0], start[way, 1]], axis=1)
        state = far[way][0] + jnp.exp(far[way][1]) * begun
        state = near[way][0] + jnp.exp(near[way][1]) * state
        return jnp.concatenate(
            [jnp.where(second, 0.0, state), jnp.where(second, state, 0.0)], axis=0
        ).astype(BF16)

    forward, backward = entering(0), entering(1)
    logs = running[...]
    turned = jnp.transpose(logs)
    sums = moments[0]
    for k in range(1, 8):
        sums = sums + moments[k]
    sums = jnp.transpose(jnp.concatenate([sums, jnp.zeros((6, 768), F32)], axis=0)) / DC
    for yy in range(4):
        for zh in range(4):
            where = yy * 512 + zh * 128
            spare[:, where : where + 128] = outer[zh, 144 + yy * 16 : 160 + yy * 16, :]

    k = (both[:, 0:128].astype(F32) * 0.125).astype(BF16)
    v = both[:, 128:256]
    rows = 128
    zero = jnp.zeros((), BF16)
    half = lane_is_second(rows)
    masks = [lane_is_second(768) == bool(h) for h in range(2)]
    head_values = [jnp.where(mask, v, zero) for mask in masks]

    def head_mean(x):
        first = jnp.sum(jnp.where(half, 0.0, x), axis=1, keepdims=True)
        last = jnp.sum(jnp.where(half, x, 0.0), axis=1, keepdims=True)
        return jnp.where(half, last, first) / 64

    for i in range(6):
        at = slice(i * rows, (i + 1) * rows)
        q = pair[at, 0:128]
        log = jnp.where(half, turned[at, 1:2], turned[at, 0:1])
        closing = jnp.where(half[0:1], turned[767:768, 1:2], turned[767:768, 0:1])
        retained = jnp.exp(log) * jnp.dot(q, forward, preferred_element_type=F32)
        retained = retained + jnp.exp(closing - log) * jnp.dot(
            q, backward, preferred_element_type=F32
        )
        for h in range(2):
            scores = lax.dot_general(
                jnp.where(masks[h][:rows], q, zero), k, NT, preferred_element_type=F32
            )
            distance = jnp.abs(turned[at, h : h + 1] - logs[h : h + 1, :])
            weights = jnp.exp(-distance)
            retained = retained + jnp.dot(
                (scores * weights).astype(BF16), head_values[h], preferred_element_type=F32
            )
        same = q.astype(F32) * k[at, :].astype(F32)
        retained = retained + 64 * head_mean(same) * v[at, :].astype(F32)
        centred = retained - head_mean(retained)
        normed = centred * lax.rsqrt(head_mean(centred * centred) + EPSILON)
        gate = jax.nn.silu(pair[at, 128:256].astype(F32))
        rows_in[at, 128:256] = (normed * head_gain[...] * gate).astype(BF16)
        average, squares = sums[at, 0:1], sums[at, 1:2]
        scaled = (convolved[at, :] - average) * lax.rsqrt(squares - average * average + EPSILON)
        rows_in[at, 0:128] = jax.nn.silu(scaled * channel_gain[...]).astype(BF16)

    def half_of(which):
        return jnp.concatenate(
            [
                rows_in[pl.ds(pl.multiple_of(k * 192 + which * 96, 32), 96), :]
                for k in range(4)
            ],
            axis=0,
        )

    mine[...] = half_of(core[0])

    def write(lanes, part):
        sent[:, lanes] = part.astype(BF16)

    out_rows(y[0], half_of(1 - core[0]), pieces, spare, write)


def join_kernel(y, mine, arrived, p0, p1, p2, p3, spare, out):
    def write(lanes, part):
        out[:, lanes] = (part + arrived[:, lanes].astype(F32)).astype(BF16)

    out_rows(y[0], mine[...], (p0, p1, p2, p3), spare, write)


def ring(x, axis, shift):
    count = lax.axis_size(axis)
    return lax.ppermute(x, axis, [(i, (i + shift) % count) for i in range(count)])


def copies(x, axes, count):
    return lax.all_to_all(
        jnp.broadcast_to(x[None], (count, *x.shape)), axes, 0, 0, tiled=True
    )


def body(
    tokens,
    input_gain,
    branch_value,
    branch_gate,
    query_weight,
    key_weight,
    value_weight,
    swish_weight,
    kernel_taps,
    channel_gain,
    decay_logs,
    start_state,
    head_gain,
    output_conv,
    output_heads,
):
    core = lax.axis_index("c").astype(jnp.int32)[None]
    y = lax.axis_index("y").astype(jnp.int32)[None]
    high = lax.axis_index("zh").astype(jnp.int32)[None]
    low = lax.axis_index(("zl", "y")).astype(jnp.int32)[None]

    place = lax.axis_index(("x", "c"))
    count = lax.axis_size(SP)
    edge = lax.ppermute(
        jnp.where(place == 7, tokens[80:96], tokens[0:16]),
        ALL,
        [(i * 8 + 7, i * 8 + 15) for i in range(count - 1)]
        + [(i * 8 + 8, i * 8) for i in range(count - 1)],
    )
    shard = call(
        shard_kernel,
        shape((32, 1008), BF16),
        (),
        (
            key_weight,
            value_weight,
            branch_value,
            branch_gate,
            query_weight,
            swish_weight,
            output_conv.T,
            output_heads.T,
        ),
        grant=56,
    )
    running = jnp.cumsum(decay_logs, axis=1)
    running = jnp.concatenate([running, jnp.zeros((6, 768), F32)], axis=0)
    tail = jnp.pad(output_heads[112:], ((0, 0), (0, 96)))
    normed = call(
        norm_kernel,
        shape((4, 112, 2048), BF16),
        (),
        (tokens, input_gain[None]),
        scratch=(
            pltpu.VMEM((96, 2048), BF16),
            pltpu.VMEM((1, 2048), F32),
            pltpu.VMEM((96, 2048), BF16),
            pltpu.SemaphoreType.DMA((4,)),
        ),
        far=(0, 1),
        out_far=(0,),
    )
    edge, normed, running, tail = lax.optimization_barrier((edge, normed, running, tail))
    normed = call(
        edge_kernel,
        shape((4, 112, 2048), BF16),
        (),
        (edge, input_gain[None], normed),
        scratch=(pltpu.VMEM((16, 2048), BF16), pltpu.SemaphoreType.DMA((4,))),
        far=(2,),
        out_far=(0,),
        aliases={2: 0},
    )
    shard, normed = lax.optimization_barrier((shard, normed))
    own = lax.all_to_all(normed, "x", 0, 0, tiled=True).reshape(448, 2048)
    rows = lax.all_gather(shard, ("zh", "zl"), axis=0, tiled=True)
    own, rows = lax.optimization_barrier((own, rows))
    other = ring(own, "c", 1)
    state_weight = copies(rows[:, :256], "y", 4).reshape(2048, 256)
    gate_piece, rest_piece = rows[:, 256:512], rows[:, 512:]
    gate_pieces = (gate_piece,) + tuple(ring(gate_piece, "y", d) for d in (1, 2, 3))
    rest_pieces = (rest_piece,) + tuple(ring(rest_piece, "y", d) for d in (1, 2, 3))

    full = shape((768, 128), F32)
    both, sent = call(
        states_kernel,
        (shape((768, 256), BF16), shape((16, 160, 128), BF16)),
        (core,),
        (own, other, state_weight, running, tail),
        scratch=(
            pltpu.VMEM((768, 256), BF16),
            pltpu.VMEM((448, 2048), BF16),
            pltpu.SemaphoreType.DMA((1,)),
        ),
        far=(1,),
        out_far=(0,),
    )
    inner = lax.all_to_all(sent, ("zl", "y"), 0, 0, tiled=True)
    sent = call(
        level_kernel,
        shape((4, 208, 128), BF16),
        (low,),
        (inner,),
        scratch=(pltpu.VMEM((208, 128), BF16), pltpu.SemaphoreType.DMA((4,))),
        out_far=(0,),
    )
    outer = lax.all_to_all(sent, "zh", 0, 0, tiled=True)
    convolved, moments = call(
        conv_kernel,
        (full, shape((2, 768), F32)),
        (core, y),
        (own, other, *gate_pieces, kernel_taps),
        scratch=(
            pltpu.VMEM((800, 128), F32),
            pltpu.VMEM((768, 128), F32),
            pltpu.VMEM((2, 768), F32),
            pltpu.VMEM((448, 2048), BF16),
            pltpu.SemaphoreType.DMA((2,)),
        ),
        far=(1,),
        out_far=(0, 1),
    )
    moments = lax.all_gather(moments, ("x", "c"))
    mine, sent, spare = call(
        mixers_kernel,
        (shape((384, 256), BF16), shape((384, 2048), BF16), shape((16, 2048), BF16)),
        (core, y, low, high),
        (
            own,
            other,
            *rest_pieces,
            inner,
            outer,
            both,
            running,
            start_state,
            head_gain[None],
            convolved,
            moments,
            channel_gain[None],
        ),
        scratch=(
            pltpu.VMEM((768, 256), BF16),
            pltpu.VMEM((768, 256), BF16),
            pltpu.VMEM((768, 256), BF16),
            pltpu.VMEM((8, 768), F32),
            pltpu.VMEM((2, 2, 64, 64), F32),
            pltpu.VMEM((1, 128), F32),
            pltpu.VMEM((768, 128), F32),
            pltpu.VMEM((8, 2, 768), F32),
            pltpu.VMEM((1, 128), F32),
            pltpu.VMEM((448, 2048), BF16),
            pltpu.SemaphoreType.DMA((8,)),
        ),
        far=(1, 8, 9, 10, 11, 12, 13, 14),
    )
    arrived = ring(sent, "c", 1)
    joined = call(join_kernel, shape((384, 2048), BF16), (y,), (mine, arrived, *rest_pieces, spare))
    parts = lax.all_to_all(joined.reshape(4, 96, 2048), "x", 0, 0, tiled=True)
    return call(last_kernel, shape((96, 2048), BF16), (), (parts,))


def solution(mesh):
    split = Mesh(mesh.devices.reshape(4, 4, 4, 4, 2), ALL)
    in_specs = (
        P(ALL, None),
        P(),
        P(SP, ("x", "c")),
        P(SP, ("x", "c")),
        P(SP, ("x", "c")),
        P(SP, ("x", "c")),
        P(SP, ("x", "c")),
        P(SP, ("x", "c")),
        P(None, ("x", "c")),
        P(("x", "c")),
        P(("x", "c"), SP),
        P(None, ("x", "c"), None, None),
        P(("x", "c")),
        P(("x", "c"), SP),
        P(("x", "c"), SP),
    )

    return jax.shard_map(
        body, mesh=split, in_specs=in_specs, out_specs=P(ALL, None), check_vma=False
    )
```

```python
import jax
import jax.numpy as jnp
from jax import lax
from jax.experimental import pallas as pl
from jax.experimental.pallas import tpu as pltpu
from jax.sharding import Mesh
from jax.sharding import PartitionSpec as P

DC = 1024
EPSILON = 1e-06
F32 = jnp.float32
BF16 = jnp.bfloat16
SP = ("zh", "zl", "y")
ALL = ("zh", "zl", "y", "x", "c")
NT = (((1,), (1,)), ((), ()))
TN = (((0,), (0,)), ((), ()))
VMEM = pl.BlockSpec(memory_space=pltpu.VMEM)
SMEM = pl.BlockSpec(memory_space=pltpu.SMEM)
HBM = pl.BlockSpec(memory_space=pltpu.HBM)


def call(kernel, out_shape, scalars, arrays, scratch=(), grant=20, far=(), out_far=(), aliases={}):
    def specs(count, away):
        return [HBM if i in away else VMEM for i in range(count)]

    arrays = [
        pltpu.with_memory_space_constraint(a, pltpu.HBM) if i in far else a
        for i, a in enumerate(arrays)
    ]
    if isinstance(out_shape, tuple):
        out_shape = tuple(
            pltpu.HBM(s.shape, s.dtype) if i in out_far else s for i, s in enumerate(out_shape)
        )
    elif out_far:
        out_shape = pltpu.HBM(out_shape.shape, out_shape.dtype)
    outs = specs(len(out_shape), out_far) if isinstance(out_shape, tuple) else specs(1, out_far)[0]
    return pl.pallas_call(
        kernel,
        out_shape=out_shape,
        in_specs=[SMEM] * len(scalars) + specs(len(arrays), far),
        out_specs=outs,
        scratch_shapes=scratch,
        compiler_params=pltpu.CompilerParams(vmem_limit_bytes=grant * 1024 * 1024),
        input_output_aliases=aliases,
    )(*scalars, *arrays)


def start_copies(pairs, semaphores):
    copies = [
        pltpu.make_async_copy(source, target, semaphores.at[i])
        for i, (source, target) in enumerate(pairs)
    ]
    for copy in copies:
        copy.start()
    return copies


def shape(dims, dtype):
    return jax.ShapeDtypeStruct(dims, dtype)


def swap_groups(read, write, rows):
    group = lax.broadcasted_iota(jnp.int32, (rows, 128), 1) // 32
    for outer in range(4):
        for inner in range(4):
            made = None
            for k in range(4):
                moved = read(outer, k)
                turn = ((k - inner) * 32) % 128
                if turn:
                    moved = pltpu.roll(moved, turn, 1)
                made = moved if made is None else jnp.where(group == k, moved, made)
            write(outer, inner, made)


def shard_kernel(k, v, bv, bg, q, s, oc, oh, out):
    for i, part in enumerate((k, v, bv, bg, q, s, oc)):
        out[:, i * 128 : i * 128 + 128] = part[...]
    out[:, 896:1008] = oh[:, 0:112]


def normed_rows(source, at, gain, out, to):
    rows = 16
    x = source[at, :].astype(F32)
    inverse = lax.rsqrt(jnp.mean(x * x, axis=1, keepdims=True) + EPSILON)
    normed = x * inverse * gain[...]

    def read(zh, zl):
        z = zh * 4 + zl
        return normed[:, z * 128 : z * 128 + 128]

    def write(zh, y, made):
        where = (y * 4 + zh) * 128
        out[to, where : where + 128] = made.astype(BF16)

    swap_groups(read, write, rows)


def norm_kernel(tokens_far, gain_far, out_far, tokens, gain, out, semaphores):
    for copy in start_copies(((tokens_far, tokens), (gain_far, gain)), semaphores):
        copy.wait()

    def step(i, carry):
        at = pl.ds(pl.multiple_of(i * 16, 16), 16)
        normed_rows(tokens, at, gain, out, at)
        return carry

    lax.fori_loop(0, 6, step, 0, unroll=2)
    pairs = [(out, out_far.at[k, 0:96, :]) for k in range(4)]
    for copy in start_copies(pairs, semaphores):
        copy.wait()


def edge_kernel(edge, gain, given_far, out_far, out, semaphores):
    normed_rows(edge, slice(0, 16), gain, out, slice(0, 16))
    pairs = [(out, out_far.at[k, 96:112, :]) for k in range(4)]
    for copy in start_copies(pairs, semaphores):
        copy.wait()


def last_kernel(parts, out):
    rows = 16

    def step(i, carry):
        at = pl.ds(pl.multiple_of(i * rows, rows), rows)
        total = parts[0, at, :].astype(F32)
        for k in range(1, 4):
            total = total + parts[k, at, :].astype(F32)

        def read(zh, y):
            where = (y * 4 + zh) * 128
            return total[:, where : where + 128]

        def write(zh, zl, made):
            where = (zh * 4 + zl) * 128
            out[at, where : where + 128] = made.astype(BF16)

        swap_groups(read, write, rows)
        return carry

    lax.fori_loop(0, 6, step, 0, unroll=2)


def lane_is_second(rows):
    return lax.broadcasted_iota(jnp.int32, (rows, 128), 1) >= 64


def by_lane(running):
    turned = jnp.transpose(running)
    return jnp.where(lane_is_second(turned.shape[0]), turned[:, 1:2], turned[:, 0:1])


def put_rows(core, own, other, target):
    for k in range(4):
        mine = pl.ds(pl.multiple_of(k * 192 + core * 96, 32), 96)
        theirs = pl.ds(pl.multiple_of(k * 192 + (1 - core) * 96, 32), 96)
        part = slice(k * 112, k * 112 + 96)
        target[mine, :] = own[part, :].astype(BF16)
        target[theirs, :] = other[part, :].astype(BF16)


def summed(x):
    lane = lax.broadcasted_iota(jnp.int32, x.shape, 1)
    shift = 1
    while shift < x.shape[1]:
        x = x + jnp.where(lane >= shift, pltpu.roll(x, shift, 1), 0.0)
        shift *= 2
    return x


def states_kernel(
    core,
    own,
    other,
    weight,
    decay,
    tail,
    both_far,
    message_far,
    running_far,
    both,
    running,
    message,
    semaphores,
):
    running[...] = summed(jnp.concatenate([decay[...], jnp.zeros((6, 768), F32)], axis=0))
    w = weight[...]
    put_rows(
        core[0],
        jnp.dot(own[...], w, preferred_element_type=F32),
        jnp.dot(other[...], w, preferred_element_type=F32),
        both,
    )
    kept = start_copies(
        ((both, both_far), (running, running_far)), semaphores.at[pl.ds(16, 2)]
    )
    logs = by_lane(running[...])
    closing = logs[767:768, :]
    k = both[:, 0:128].astype(F32) * 0.125
    v = both[:, 128:256]
    second = lane_is_second(64)
    ahead = lax.dot_general(
        (k * jnp.exp(closing - logs)).astype(BF16), v, TN, preferred_element_type=F32
    )
    back = lax.dot_general((k * jnp.exp(logs)).astype(BF16), v, TN, preferred_element_type=F32)
    parts = (
        (slice(0, 64), jnp.where(second, ahead[64:, :], ahead[:64, :]).astype(BF16)),
        (slice(64, 128), jnp.where(second, back[64:, :], back[:64, :]).astype(BF16)),
        (slice(128, 144), log_rows(closing)),
        (slice(144, 160), tail[...]),
    )
    for at, part in parts:
        message[at, :] = part
    kept += start_copies([(message, message_far.at[k]) for k in range(16)], semaphores)
    for copy in kept:
        copy.wait()


def log_rows(log):
    high = log.astype(BF16)
    low = (log - high.astype(F32)).astype(BF16)
    first = lax.broadcasted_iota(jnp.int32, (16, 128), 0) < 8
    return jnp.where(first, high.astype(F32), low.astype(F32)).astype(BF16)


def scan_states(gathered, count, position):
    def log_of(m):
        return gathered[m, 128:129, :].astype(F32) + gathered[m, 136:137, :].astype(F32)

    def one_way(order, rows):
        state = jnp.zeros((64, 128), F32)
        log = jnp.zeros((1, 128), F32)
        held, held_log = state, log
        for m in order:
            here = position == m
            held = jnp.where(here, state, held)
            held_log = jnp.where(here, log, held_log)
            own = log_of(m)
            state = jnp.exp(own) * state + gathered[m, rows, :].astype(F32)
            log = log + own
        return held, held_log, state, log

    ahead = one_way(range(count), slice(0, 64))
    back = one_way(reversed(range(count)), slice(64, 128))
    return ahead, back


def level_kernel(position, gathered, message_far, message, semaphores):
    ahead, back = scan_states(gathered, 16, position[0])
    parts = [
        (slice(0, 64), ahead[2].astype(BF16)),
        (slice(64, 128), back[2].astype(BF16)),
        (slice(128, 144), log_rows(ahead[3])),
    ]
    group = lax.broadcasted_iota(jnp.int32, (16, 128), 1) // 32
    for y in range(4):
        made = gathered[y, 144:160, :].astype(F32)
        for zl in range(1, 4):
            moved = pltpu.roll(gathered[zl * 4 + y, 144:160, :].astype(F32), zl * 32, 1)
            made = jnp.where(group == zl, moved, made)
        parts.append((slice(144 + y * 16, 160 + y * 16), made.astype(BF16)))
    for at, part in parts:
        message[at, :] = part
    for copy in start_copies([(message, message_far.at[k]) for k in range(4)], semaphores):
        copy.wait()


def column_block(position, shift):
    return pl.ds(pl.multiple_of(((position + 4 - shift) % 4) * 512, 512), 512)


def by_piece(y, rows, pieces, lanes):
    total = None
    for shift, piece in enumerate(pieces):
        part = jnp.dot(
            rows[:, column_block(y, shift)], piece[:, lanes], preferred_element_type=F32
        )
        total = part if total is None else total + part
    return total


def conv_kernel(core, y, own, other, p0, p1, p2, p3, taps, convolved_far, moments_far, padded, convolved, moments, semaphores):
    pieces = (p0, p1, p2, p3)

    def rows_of(rows):
        both = by_piece(y[0], rows, pieces, slice(0, 256))
        return (both[:, :128] * jax.nn.sigmoid(both[:, 128:])).astype(BF16).astype(F32)

    first, second = rows_of(own), rows_of(other)
    for k in range(4):
        mine = pl.ds(pl.multiple_of(16 + k * 192 + core[0] * 96, 16), 96)
        theirs = pl.ds(pl.multiple_of(16 + k * 192 + (1 - core[0]) * 96, 16), 96)
        padded[mine, :] = first[k * 112 : k * 112 + 96, :]
        padded[theirs, :] = second[k * 112 : k * 112 + 96, :]
    is_second = jnp.full((16, 128), core[0], jnp.int32) == 1
    padded[0:16, :] = jnp.where(is_second, first[432:448, :], second[432:448, :])
    padded[784:800, :] = jnp.where(is_second, second[96:112, :], first[96:112, :])
    ones = jnp.ones((8, 128), F32)
    rows = 128
    for i in range(6):
        total = None
        for j in range(31):
            start = i * rows + j + 1
            term = taps[j : j + 1, :] * padded[start : start + rows, :]
            total = term if total is None else total + term
        convolved[i * rows : (i + 1) * rows, :] = total
        highest = lax.Precision.HIGHEST
        s1 = lax.dot_general(ones, total, NT, precision=highest, preferred_element_type=F32)
        s2 = lax.dot_general(ones, total * total, NT, precision=highest, preferred_element_type=F32)
        moments[0:1, i * rows : (i + 1) * rows] = s1[0:1]
        moments[1:2, i * rows : (i + 1) * rows] = s2[0:1]
    pairs = ((convolved, convolved_far), (moments, moments_far))
    for copy in start_copies(pairs, semaphores):
        copy.wait()


def out_rows(y, rows, weight, write):
    for shift in range(4):
        part = lax.dot_general(rows, weight[shift], NT, preferred_element_type=F32)
        write(column_block(y, shift), part)


def mixers_kernel(
    core,
    y,
    low,
    high,
    own,
    other,
    p0,
    p1,
    p2,
    p3,
    inner,
    outer,
    both_far,
    running_far,
    start_far,
    head_gain_far,
    convolved_far,
    moments_far,
    channel_gain_far,
    mine,
    sent,
    weight,
    spare,
    pair,
    rows_in,
    both,
    running,
    start,
    head_gain,
    convolved,
    moments,
    channel_gain,
    semaphores,
):
    pieces = (p0, p1, p2, p3)
    loads = start_copies(
        (
            (both_far, both),
            (running_far, running),
            (start_far, start),
            (head_gain_far, head_gain),
            (convolved_far, convolved),
            (moments_far, moments),
            (channel_gain_far, channel_gain),
        ),
        semaphores,
    )
    put_rows(
        core[0],
        by_piece(y[0], own, pieces, slice(0, 256)),
        by_piece(y[0], other, pieces, slice(0, 256)),
        pair,
    )
    for load in loads:
        load.wait()
    near = scan_states(inner, 16, low[0])
    far = scan_states(outer, 4, high[0])
    second = lane_is_second(64)

    def entering(way):
        begun = jnp.concatenate([start[way, 0], start[way, 1]], axis=1)
        state = far[way][0] + jnp.exp(far[way][1]) * begun
        state = near[way][0] + jnp.exp(near[way][1]) * state
        return jnp.concatenate(
            [jnp.where(second, 0.0, state), jnp.where(second, state, 0.0)], axis=0
        ).astype(BF16)

    forward, backward = entering(0), entering(1)
    logs = running[...]
    turned = jnp.transpose(logs)
    sums = moments[0]
    for k in range(1, 8):
        sums = sums + moments[k]
    sums = jnp.transpose(jnp.concatenate([sums, jnp.zeros((6, 768), F32)], axis=0)) / DC
    for yy in range(4):
        for zh in range(4):
            where = yy * 512 + zh * 128
            spare[:, where : where + 128] = outer[zh, 144 + yy * 16 : 160 + yy * 16, :]
    for shift, piece in enumerate(pieces):
        last = jnp.transpose(spare[:, column_block(y[0], shift)].astype(F32)).astype(BF16)
        weight[shift, :, 0:240] = piece[:, 256:496]
        weight[shift, :, 240:256] = last

    k = (both[:, 0:128].astype(F32) * 0.125).astype(BF16)
    v = both[:, 128:256]
    rows = 128
    zero = jnp.zeros((), BF16)
    half = lane_is_second(rows)

    def head_mean(x):
        first = jnp.sum(jnp.where(half, 0.0, x), axis=1, keepdims=True)
        last = jnp.sum(jnp.where(half, x, 0.0), axis=1, keepdims=True)
        return jnp.where(half, last, first) / 64

    for i in range(6):
        at = slice(i * rows, (i + 1) * rows)
        q = pair[at, 0:128]
        log = jnp.where(half, turned[at, 1:2], turned[at, 0:1])
        closing = jnp.where(half[0:1], turned[767:768, 1:2], turned[767:768, 0:1])
        retained = jnp.exp(log) * jnp.dot(q, forward, preferred_element_type=F32)
        retained = retained + jnp.exp(closing - log) * jnp.dot(
            q, backward, preferred_element_type=F32
        )
        stacked = jnp.concatenate(
            [jnp.where(half, zero, q), jnp.where(half, q, zero)], axis=0
        )
        scores = lax.dot_general(stacked, k, NT, preferred_element_type=F32)
        parts = []
        for h in range(2):
            distance = jnp.abs(turned[at, h : h + 1] - logs[h : h + 1, :])
            part = scores[h * rows : (h + 1) * rows, :] * jnp.exp(-distance)
            parts.append(part.astype(BF16))
        mixed = jnp.dot(jnp.concatenate(parts, axis=0), v, preferred_element_type=F32)
        retained = retained + jnp.where(half, mixed[rows:, :], mixed[:rows, :])
        same = q.astype(F32) * k[at, :].astype(F32)
        retained = retained + 64 * head_mean(same) * v[at, :].astype(F32)
        centred = retained - head_mean(retained)
        normed = centred * lax.rsqrt(head_mean(centred * centred) + EPSILON)
        gate = jax.nn.silu(pair[at, 128:256].astype(F32))
        rows_in[at, 128:256] = (normed * head_gain[...] * gate).astype(BF16)
        average, squares = sums[at, 0:1], sums[at, 1:2]
        scaled = (convolved[at, :] - average) * lax.rsqrt(squares - average * average + EPSILON)
        rows_in[at, 0:128] = jax.nn.silu(scaled * channel_gain[...]).astype(BF16)

    def half_of(which):
        return jnp.concatenate(
            [
                rows_in[pl.ds(pl.multiple_of(k * 192 + which * 96, 32), 96), :]
                for k in range(4)
            ],
            axis=0,
        )

    mine[...] = half_of(core[0])

    def write(lanes, part):
        sent[:, lanes] = part.astype(BF16)

    out_rows(y[0], half_of(1 - core[0]), weight, write)


def join_kernel(y, mine, arrived, weight, out):
    def write(lanes, part):
        out[:, lanes] = (part + arrived[:, lanes].astype(F32)).astype(BF16)

    out_rows(y[0], mine[...], weight, write)


def ring(x, axis, shift):
    count = lax.axis_size(axis)
    return lax.ppermute(x, axis, [(i, (i + shift) % count) for i in range(count)])


def copies(x, axes, count):
    return lax.all_to_all(
        jnp.broadcast_to(x[None], (count, *x.shape)), axes, 0, 0, tiled=True
    )


def body(
    tokens,
    input_gain,
    branch_value,
    branch_gate,
    query_weight,
    key_weight,
    value_weight,
    swish_weight,
    kernel_taps,
    channel_gain,
    decay_logs,
    start_state,
    head_gain,
    output_conv,
    output_heads,
):
    core = lax.axis_index("c").astype(jnp.int32)[None]
    y = lax.axis_index("y").astype(jnp.int32)[None]
    high = lax.axis_index("zh").astype(jnp.int32)[None]
    low = lax.axis_index(("zl", "y")).astype(jnp.int32)[None]

    place = lax.axis_index(("x", "c"))
    count = lax.axis_size(SP)
    edge = lax.ppermute(
        jnp.where(place == 7, tokens[80:96], tokens[0:16]),
        ALL,
        [(i * 8 + 7, i * 8 + 15) for i in range(count - 1)]
        + [(i * 8 + 8, i * 8) for i in range(count - 1)],
    )
    shard = call(
        shard_kernel,
        shape((32, 1008), BF16),
        (),
        (
            key_weight,
            value_weight,
            branch_value,
            branch_gate,
            query_weight,
            swish_weight,
            output_conv.T,
            output_heads.T,
        ),
        grant=56,
    )
    tail = jnp.pad(output_heads[112:], ((0, 0), (0, 96)))
    normed = call(
        norm_kernel,
        shape((4, 112, 2048), BF16),
        (),
        (tokens, input_gain[None]),
        scratch=(
            pltpu.VMEM((96, 2048), BF16),
            pltpu.VMEM((1, 2048), F32),
            pltpu.VMEM((96, 2048), BF16),
            pltpu.SemaphoreType.DMA((4,)),
        ),
        far=(0, 1),
        out_far=(0,),
    )
    edge, normed = lax.optimization_barrier((edge, normed))
    normed = call(
        edge_kernel,
        shape((4, 112, 2048), BF16),
        (),
        (edge, input_gain[None], normed),
        scratch=(pltpu.VMEM((16, 2048), BF16), pltpu.SemaphoreType.DMA((4,))),
        far=(2,),
        out_far=(0,),
        aliases={2: 0},
    )
    shard, normed = lax.optimization_barrier((shard, normed))
    own = lax.all_to_all(normed, "x", 0, 0, tiled=True).reshape(448, 2048)
    rows = lax.all_gather(shard, ("zh", "zl"), axis=0, tiled=True)
    own, rows = lax.optimization_barrier((own, rows))
    other = ring(own, "c", 1)
    state_weight = copies(rows[:, :256], "y", 4).reshape(2048, 256)
    gate_piece, rest_piece = rows[:, 256:512], rows[:, 512:]
    gate_pieces = (gate_piece,) + tuple(ring(gate_piece, "y", d) for d in (1, 2, 3))
    rest_pieces = (rest_piece,) + tuple(ring(rest_piece, "y", d) for d in (1, 2, 3))

    full = shape((768, 128), F32)
    both, sent, running = call(
        states_kernel,
        (shape((768, 256), BF16), shape((16, 160, 128), BF16), shape((8, 768), F32)),
        (core,),
        (own, other, state_weight, decay_logs, tail),
        scratch=(
            pltpu.VMEM((768, 256), BF16),
            pltpu.VMEM((8, 768), F32),
            pltpu.VMEM((160, 128), BF16),
            pltpu.SemaphoreType.DMA((18,)),
        ),
        out_far=(0, 1, 2),
    )
    inner = lax.all_to_all(sent, ("zl", "y"), 0, 0, tiled=True)
    sent = call(
        level_kernel,
        shape((4, 208, 128), BF16),
        (low,),
        (inner,),
        scratch=(pltpu.VMEM((208, 128), BF16), pltpu.SemaphoreType.DMA((4,))),
        out_far=(0,),
    )
    outer = lax.all_to_all(sent, "zh", 0, 0, tiled=True)
    convolved, moments = call(
        conv_kernel,
        (full, shape((2, 768), F32)),
        (core, y),
        (own, other, *gate_pieces, kernel_taps),
        scratch=(
            pltpu.VMEM((800, 128), F32),
            pltpu.VMEM((768, 128), F32),
            pltpu.VMEM((2, 768), F32),
            pltpu.SemaphoreType.DMA((2,)),
        ),
        out_far=(0, 1),
    )
    moments = lax.all_gather(moments, ("x", "c"))
    mine, sent, weight = call(
        mixers_kernel,
        (shape((384, 256), BF16), shape((384, 2048), BF16), shape((4, 512, 256), BF16)),
        (core, y, low, high),
        (
            own,
            other,
            *rest_pieces,
            inner,
            outer,
            both,
            running,
            start_state,
            head_gain[None],
            convolved,
            moments,
            channel_gain[None],
        ),
        scratch=(
            pltpu.VMEM((16, 2048), BF16),
            pltpu.VMEM((768, 256), BF16),
            pltpu.VMEM((768, 256), BF16),
            pltpu.VMEM((768, 256), BF16),
            pltpu.VMEM((8, 768), F32),
            pltpu.VMEM((2, 2, 64, 64), F32),
            pltpu.VMEM((1, 128), F32),
            pltpu.VMEM((768, 128), F32),
            pltpu.VMEM((8, 2, 768), F32),
            pltpu.VMEM((1, 128), F32),
            pltpu.SemaphoreType.DMA((7,)),
        ),
        far=(8, 9, 10, 11, 12, 13, 14),
    )
    arrived = ring(sent, "c", 1)
    joined = call(join_kernel, shape((384, 2048), BF16), (y,), (mine, arrived, weight))
    parts = lax.all_to_all(joined.reshape(4, 96, 2048), "x", 0, 0, tiled=True)
    return call(last_kernel, shape((96, 2048), BF16), (), (parts,))


def solution(mesh):
    split = Mesh(mesh.devices.reshape(4, 4, 4, 4, 2), ALL)
    in_specs = (
        P(ALL, None),
        P(),
        P(SP, ("x", "c")),
        P(SP, ("x", "c")),
        P(SP, ("x", "c")),
        P(SP, ("x", "c")),
        P(SP, ("x", "c")),
        P(SP, ("x", "c")),
        P(None, ("x", "c")),
        P(("x", "c")),
        P(("x", "c"), SP),
        P(None, ("x", "c"), None, None),
        P(("x", "c")),
        P(("x", "c"), SP),
        P(("x", "c"), SP),
    )

    return jax.shard_map(
        body, mesh=split, in_specs=in_specs, out_specs=P(ALL, None), check_vma=False
    )
```

```python
import jax
import jax.numpy as jnp
from jax import lax
from jax.experimental import pallas as pl
from jax.experimental.pallas import tpu as pltpu
from jax.sharding import Mesh
from jax.sharding import PartitionSpec as P

DC = 1024
EPSILON = 1e-06
F32 = jnp.float32
BF16 = jnp.bfloat16
SP = ("zh", "zl", "y")
ALL = ("zh", "zl", "y", "x", "c")
NT = (((1,), (1,)), ((), ()))
TN = (((0,), (0,)), ((), ()))
VMEM = pl.BlockSpec(memory_space=pltpu.VMEM)
SMEM = pl.BlockSpec(memory_space=pltpu.SMEM)
HBM = pl.BlockSpec(memory_space=pltpu.HBM)


def call(kernel, out_shape, scalars, arrays, scratch=(), grant=20, far=(), out_far=(), aliases={}):
    def specs(count, away):
        return [HBM if i in away else VMEM for i in range(count)]

    arrays = [
        pltpu.with_memory_space_constraint(a, pltpu.HBM) if i in far else a
        for i, a in enumerate(arrays)
    ]
    if isinstance(out_shape, tuple):
        out_shape = tuple(
            pltpu.HBM(s.shape, s.dtype) if i in out_far else s for i, s in enumerate(out_shape)
        )
    elif out_far:
        out_shape = pltpu.HBM(out_shape.shape, out_shape.dtype)
    outs = specs(len(out_shape), out_far) if isinstance(out_shape, tuple) else specs(1, out_far)[0]
    return pl.pallas_call(
        kernel,
        out_shape=out_shape,
        in_specs=[SMEM] * len(scalars) + specs(len(arrays), far),
        out_specs=outs,
        scratch_shapes=scratch,
        compiler_params=pltpu.CompilerParams(vmem_limit_bytes=grant * 1024 * 1024),
        input_output_aliases=aliases,
    )(*scalars, *arrays)


def start_copies(pairs, semaphores):
    copies = [
        pltpu.make_async_copy(source, target, semaphores.at[i])
        for i, (source, target) in enumerate(pairs)
    ]
    for copy in copies:
        copy.start()
    return copies


def shape(dims, dtype):
    return jax.ShapeDtypeStruct(dims, dtype)


def swap_groups(read, write, rows):
    group = lax.broadcasted_iota(jnp.int32, (rows, 128), 1) // 32
    for outer in range(4):
        for inner in range(4):
            made = None
            for k in range(4):
                moved = read(outer, k)
                turn = ((k - inner) * 32) % 128
                if turn:
                    moved = pltpu.roll(moved, turn, 1)
                made = moved if made is None else jnp.where(group == k, moved, made)
            write(outer, inner, made)


def normed_rows(source, at, gain, out, to):
    rows = 16
    x = source[at, :].astype(F32)
    inverse = lax.rsqrt(jnp.mean(x * x, axis=1, keepdims=True) + EPSILON)
    normed = x * inverse * gain[...]

    def read(zh, zl):
        z = zh * 4 + zl
        return normed[:, z * 128 : z * 128 + 128]

    def write(zh, y, made):
        where = (y * 4 + zh) * 128
        out[to, where : where + 128] = made.astype(BF16)

    swap_groups(read, write, rows)


def norm_kernel(*refs):
    tokens_far, gain_far, *weights_far = refs[:10]
    out_far, shard, tokens, gain, out, weights, semaphores = refs[10:]

    def piece(ref, i):
        return ref.at[pl.ds(i * 32, 32), :]

    pairs = [(gain_far, gain)] + [(piece(tokens_far, i), piece(tokens, i)) for i in range(3)]
    pairs += [(part, weights.at[i]) for i, part in enumerate(weights_far)]
    loads = start_copies(pairs, semaphores)
    loads[0].wait()
    stores = []
    for i in range(3):
        loads[1 + i].wait()
        for part in range(2):
            at = slice(i * 32 + part * 16, i * 32 + part * 16 + 16)
            normed_rows(tokens, at, gain, out, at)
        pairs = [(piece(out, i), out_far.at[k, pl.ds(i * 32, 32), :]) for k in range(4)]
        stores += start_copies(pairs, semaphores.at[pl.ds(12 + 4 * i, 4)])
    for load in loads[4:]:
        load.wait()
    for i in range(7):
        shard[:, i * 128 : i * 128 + 128] = weights[i]
    shard[:, 896:1008] = weights[7, :, 0:112]
    for store in stores:
        store.wait()


def edge_kernel(edge, gain_far, given_far, out_far, gain, out, semaphores):
    (load,) = start_copies(((gain_far, gain),), semaphores)
    load.wait()
    normed_rows(edge, slice(0, 16), gain, out, slice(0, 16))
    pairs = [(out, out_far.at[k, 96:112, :]) for k in range(4)]
    for copy in start_copies(pairs, semaphores):
        copy.wait()


def last_kernel(parts, out):
    rows = 16

    def step(i, carry):
        at = pl.ds(pl.multiple_of(i * rows, rows), rows)
        total = parts[0, at, :].astype(F32)
        for k in range(1, 4):
            total = total + parts[k, at, :].astype(F32)

        def read(zh, y):
            where = (y * 4 + zh) * 128
            return total[:, where : where + 128]

        def write(zh, zl, made):
            where = (zh * 4 + zl) * 128
            out[at, where : where + 128] = made.astype(BF16)

        swap_groups(read, write, rows)
        return carry

    lax.fori_loop(0, 6, step, 0, unroll=2)


def lane_is_second(rows):
    return lax.broadcasted_iota(jnp.int32, (rows, 128), 1) >= 64


def by_lane(running):
    turned = jnp.transpose(running)
    return jnp.where(lane_is_second(turned.shape[0]), turned[:, 1:2], turned[:, 0:1])


def put_rows(core, own, other, target):
    for k in range(4):
        mine = pl.ds(pl.multiple_of(k * 192 + core * 96, 32), 96)
        theirs = pl.ds(pl.multiple_of(k * 192 + (1 - core) * 96, 32), 96)
        part = slice(k * 112, k * 112 + 96)
        target[mine, :] = own[part, :].astype(BF16)
        target[theirs, :] = other[part, :].astype(BF16)


def summed(x):
    lane = lax.broadcasted_iota(jnp.int32, x.shape, 1)
    shift = 1
    while shift < x.shape[1]:
        x = x + jnp.where(lane >= shift, pltpu.roll(x, shift, 1), 0.0)
        shift *= 2
    return x


def states_kernel(
    core,
    own,
    other,
    weight,
    decay,
    tail,
    both_far,
    message_far,
    running_far,
    both,
    running,
    message,
    semaphores,
):
    running[...] = summed(jnp.concatenate([decay[...], jnp.zeros((6, 768), F32)], axis=0))
    w = weight[...]
    put_rows(
        core[0],
        jnp.dot(own[...], w, preferred_element_type=F32),
        jnp.dot(other[...], w, preferred_element_type=F32),
        both,
    )
    kept = start_copies(
        ((both, both_far), (running, running_far)), semaphores.at[pl.ds(16, 2)]
    )
    logs = by_lane(running[...])
    closing = logs[767:768, :]
    k = both[:, 0:128].astype(F32) * 0.125
    v = both[:, 128:256]
    second = lane_is_second(64)
    ahead = lax.dot_general(
        (k * jnp.exp(closing - logs)).astype(BF16), v, TN, preferred_element_type=F32
    )
    back = lax.dot_general((k * jnp.exp(logs)).astype(BF16), v, TN, preferred_element_type=F32)
    parts = (
        (slice(0, 64), jnp.where(second, ahead[64:, :], ahead[:64, :]).astype(BF16)),
        (slice(64, 128), jnp.where(second, back[64:, :], back[:64, :]).astype(BF16)),
        (slice(128, 144), log_rows(closing)),
        (slice(144, 160), tail[...]),
    )
    for at, part in parts:
        message[at, :] = part
    kept += start_copies([(message, message_far.at[k]) for k in range(16)], semaphores)
    for copy in kept:
        copy.wait()


def log_rows(log):
    high = log.astype(BF16)
    low = (log - high.astype(F32)).astype(BF16)
    first = lax.broadcasted_iota(jnp.int32, (16, 128), 0) < 8
    return jnp.where(first, high.astype(F32), low.astype(F32)).astype(BF16)


def scan_states(gathered, count, position):
    def log_of(m):
        return gathered[m, 128:129, :].astype(F32) + gathered[m, 136:137, :].astype(F32)

    def one_way(order, rows):
        state = jnp.zeros((64, 128), F32)
        log = jnp.zeros((1, 128), F32)
        held, held_log = state, log
        for m in order:
            here = position == m
            held = jnp.where(here, state, held)
            held_log = jnp.where(here, log, held_log)
            own = log_of(m)
            state = jnp.exp(own) * state + gathered[m, rows, :].astype(F32)
            log = log + own
        return held, held_log, state, log

    ahead = one_way(range(count), slice(0, 64))
    back = one_way(reversed(range(count)), slice(64, 128))
    return ahead, back


def level_kernel(position, gathered, message_far, message, semaphores):
    ahead, back = scan_states(gathered, 16, position[0])
    parts = [
        (slice(0, 64), ahead[2].astype(BF16)),
        (slice(64, 128), back[2].astype(BF16)),
        (slice(128, 144), log_rows(ahead[3])),
    ]
    group = lax.broadcasted_iota(jnp.int32, (16, 128), 1) // 32
    for y in range(4):
        made = gathered[y, 144:160, :].astype(F32)
        for zl in range(1, 4):
            moved = pltpu.roll(gathered[zl * 4 + y, 144:160, :].astype(F32), zl * 32, 1)
            made = jnp.where(group == zl, moved, made)
        parts.append((slice(144 + y * 16, 160 + y * 16), made.astype(BF16)))
    for at, part in parts:
        message[at, :] = part
    for copy in start_copies([(message, message_far.at[k]) for k in range(4)], semaphores):
        copy.wait()


def column_block(position, shift):
    return pl.ds(pl.multiple_of(((position + 4 - shift) % 4) * 512, 512), 512)


def by_piece(y, rows, pieces, lanes):
    total = None
    for shift, piece in enumerate(pieces):
        part = jnp.dot(
            rows[:, column_block(y, shift)], piece[:, lanes], preferred_element_type=F32
        )
        total = part if total is None else total + part
    return total


def conv_kernel(core, y, own, other, p0, p1, p2, p3, taps, convolved_far, moments_far, padded, convolved, moments, semaphores):
    pieces = (p0, p1, p2, p3)

    def rows_of(rows):
        both = by_piece(y[0], rows, pieces, slice(0, 256))
        return (both[:, :128] * jax.nn.sigmoid(both[:, 128:])).astype(BF16).astype(F32)

    first, second = rows_of(own), rows_of(other)
    for k in range(4):
        mine = pl.ds(pl.multiple_of(16 + k * 192 + core[0] * 96, 16), 96)
        theirs = pl.ds(pl.multiple_of(16 + k * 192 + (1 - core[0]) * 96, 16), 96)
        padded[mine, :] = first[k * 112 : k * 112 + 96, :]
        padded[theirs, :] = second[k * 112 : k * 112 + 96, :]
    is_second = jnp.full((16, 128), core[0], jnp.int32) == 1
    padded[0:16, :] = jnp.where(is_second, first[432:448, :], second[432:448, :])
    padded[784:800, :] = jnp.where(is_second, second[96:112, :], first[96:112, :])
    ones = jnp.ones((8, 128), F32)
    rows = 128
    for i in range(6):
        total = None
        for j in range(31):
            start = i * rows + j + 1
            term = taps[j : j + 1, :] * padded[start : start + rows, :]
            total = term if total is None else total + term
        convolved[i * rows : (i + 1) * rows, :] = total
        highest = lax.Precision.HIGHEST
        s1 = lax.dot_general(ones, total, NT, precision=highest, preferred_element_type=F32)
        s2 = lax.dot_general(ones, total * total, NT, precision=highest, preferred_element_type=F32)
        moments[0:1, i * rows : (i + 1) * rows] = s1[0:1]
        moments[1:2, i * rows : (i + 1) * rows] = s2[0:1]
    pairs = ((convolved, convolved_far), (moments, moments_far))
    for copy in start_copies(pairs, semaphores):
        copy.wait()


def out_rows(y, rows, weight, write):
    for shift in range(4):
        part = lax.dot_general(rows, weight[shift], NT, preferred_element_type=F32)
        write(column_block(y, shift), part)


def mixers_kernel(
    core,
    y,
    low,
    high,
    own,
    other,
    p0,
    p1,
    p2,
    p3,
    inner,
    outer,
    both_far,
    running_far,
    start_far,
    head_gain_far,
    convolved_far,
    moments_far,
    channel_gain_far,
    mine,
    sent,
    weight,
    spare,
    pair,
    rows_in,
    both,
    running,
    start,
    head_gain,
    convolved,
    moments,
    channel_gain,
    semaphores,
):
    pieces = (p0, p1, p2, p3)
    loads = start_copies(
        (
            (both_far, both),
            (running_far, running),
            (start_far, start),
            (head_gain_far, head_gain),
            (convolved_far, convolved),
            (moments_far, moments),
            (channel_gain_far, channel_gain),
        ),
        semaphores,
    )
    put_rows(
        core[0],
        by_piece(y[0], own, pieces, slice(0, 256)),
        by_piece(y[0], other, pieces, slice(0, 256)),
        pair,
    )
    for load in loads:
        load.wait()
    near = scan_states(inner, 16, low[0])
    far = scan_states(outer, 4, high[0])
    second = lane_is_second(64)

    def entering(way):
        begun = jnp.concatenate([start[way, 0], start[way, 1]], axis=1)
        state = far[way][0] + jnp.exp(far[way][1]) * begun
        state = near[way][0] + jnp.exp(near[way][1]) * state
        return jnp.concatenate(
            [jnp.where(second, 0.0, state), jnp.where(second, state, 0.0)], axis=0
        ).astype(BF16)

    forward, backward = entering(0), entering(1)
    logs = running[...]
    turned = jnp.transpose(logs)
    sums = moments[0]
    for k in range(1, 8):
        sums = sums + moments[k]
    sums = jnp.transpose(jnp.concatenate([sums, jnp.zeros((6, 768), F32)], axis=0)) / DC
    for yy in range(4):
        for zh in range(4):
            where = yy * 512 + zh * 128
            spare[:, where : where + 128] = outer[zh, 144 + yy * 16 : 160 + yy * 16, :]
    for shift, piece in enumerate(pieces):
        last = jnp.transpose(spare[:, column_block(y[0], shift)].astype(F32)).astype(BF16)
        weight[shift, :, 0:240] = piece[:, 256:496]
        weight[shift, :, 240:256] = last

    k = (both[:, 0:128].astype(F32) * 0.125).astype(BF16)
    v = both[:, 128:256]
    rows = 128
    zero = jnp.zeros((), BF16)
    half = lane_is_second(rows)
    diagonal = lax.broadcasted_iota(jnp.int32, (rows, rows), 0) == (
        lax.broadcasted_iota(jnp.int32, (rows, rows), 1)
    )

    def head_mean(x):
        first = jnp.sum(jnp.where(half, 0.0, x), axis=1, keepdims=True)
        last = jnp.sum(jnp.where(half, x, 0.0), axis=1, keepdims=True)
        return jnp.where(half, last, first) / 64

    for i in range(6):
        at = slice(i * rows, (i + 1) * rows)
        q = pair[at, 0:128]
        log = jnp.where(half, turned[at, 1:2], turned[at, 0:1])
        closing = jnp.where(half[0:1], turned[767:768, 1:2], turned[767:768, 0:1])
        retained = jnp.exp(log) * jnp.dot(q, forward, preferred_element_type=F32)
        retained = retained + jnp.exp(closing - log) * jnp.dot(
            q, backward, preferred_element_type=F32
        )
        stacked = jnp.concatenate(
            [jnp.where(half, zero, q), jnp.where(half, q, zero)], axis=0
        )
        scores = lax.dot_general(stacked, k, NT, preferred_element_type=F32)
        parts = []
        for h in range(2):
            distance = jnp.abs(turned[at, h : h + 1] - logs[h : h + 1, :])
            head_scores = scores[h * rows : (h + 1) * rows, :]
            part = head_scores * jnp.exp(-distance)
            twice = part[:, at] + jnp.where(diagonal, head_scores[:, at], 0.0)
            sides = [part[:, : at.start], twice, part[:, at.stop :]]
            part = jnp.concatenate([side for side in sides if side.shape[1]], axis=1)
            parts.append(part.astype(BF16))
        mixed = jnp.dot(jnp.concatenate(parts, axis=0), v, preferred_element_type=F32)
        retained = retained + jnp.where(half, mixed[rows:, :], mixed[:rows, :])
        centred = retained - head_mean(retained)
        normed = centred * lax.rsqrt(head_mean(centred * centred) + EPSILON)
        gate = jax.nn.silu(pair[at, 128:256].astype(F32))
        rows_in[at, 128:256] = (normed * head_gain[...] * gate).astype(BF16)
        average, squares = sums[at, 0:1], sums[at, 1:2]
        scaled = (convolved[at, :] - average) * lax.rsqrt(squares - average * average + EPSILON)
        rows_in[at, 0:128] = jax.nn.silu(scaled * channel_gain[...]).astype(BF16)

    def half_of(which):
        return jnp.concatenate(
            [
                rows_in[pl.ds(pl.multiple_of(k * 192 + which * 96, 32), 96), :]
                for k in range(4)
            ],
            axis=0,
        )

    mine[...] = half_of(core[0])

    def write(lanes, part):
        sent[:, lanes] = part.astype(BF16)

    out_rows(y[0], half_of(1 - core[0]), weight, write)


def join_kernel(y, mine, arrived, weight, out):
    def write(lanes, part):
        out[:, lanes] = (part + arrived[:, lanes].astype(F32)).astype(BF16)

    out_rows(y[0], mine[...], weight, write)


def ring(x, axis, shift):
    count = lax.axis_size(axis)
    return lax.ppermute(x, axis, [(i, (i + shift) % count) for i in range(count)])


def copies(x, axes, count):
    return lax.all_to_all(
        jnp.broadcast_to(x[None], (count, *x.shape)), axes, 0, 0, tiled=True
    )


def body(
    tokens,
    input_gain,
    branch_value,
    branch_gate,
    query_weight,
    key_weight,
    value_weight,
    swish_weight,
    kernel_taps,
    channel_gain,
    decay_logs,
    start_state,
    head_gain,
    output_conv,
    output_heads,
):
    core = lax.axis_index("c").astype(jnp.int32)[None]
    y = lax.axis_index("y").astype(jnp.int32)[None]
    high = lax.axis_index("zh").astype(jnp.int32)[None]
    low = lax.axis_index(("zl", "y")).astype(jnp.int32)[None]

    place = lax.axis_index(("x", "c"))
    count = lax.axis_size(SP)
    edge = lax.ppermute(
        jnp.where(place == 7, tokens[80:96], tokens[0:16]),
        ALL,
        [(i * 8 + 7, i * 8 + 15) for i in range(count - 1)]
        + [(i * 8 + 8, i * 8) for i in range(count - 1)],
    )
    tail = jnp.pad(output_heads[112:], ((0, 0), (0, 96)))
    weights = (
        key_weight,
        value_weight,
        branch_value,
        branch_gate,
        query_weight,
        swish_weight,
        output_conv.T,
        output_heads.T,
    )
    normed, shard = call(
        norm_kernel,
        (shape((4, 112, 2048), BF16), shape((32, 1008), BF16)),
        (),
        (tokens, input_gain[None], *weights),
        scratch=(
            pltpu.VMEM((96, 2048), BF16),
            pltpu.VMEM((1, 2048), F32),
            pltpu.VMEM((96, 2048), BF16),
            pltpu.VMEM((8, 32, 128), BF16),
            pltpu.SemaphoreType.DMA((24,)),
        ),
        far=tuple(range(10)),
        out_far=(0,),
    )
    edge, normed = lax.optimization_barrier((edge, normed))
    normed = call(
        edge_kernel,
        shape((4, 112, 2048), BF16),
        (),
        (edge, input_gain[None], normed),
        scratch=(
            pltpu.VMEM((1, 2048), F32),
            pltpu.VMEM((16, 2048), BF16),
            pltpu.SemaphoreType.DMA((4,)),
        ),
        far=(1, 2),
        out_far=(0,),
        aliases={2: 0},
    )
    shard, normed = lax.optimization_barrier((shard, normed))
    own = lax.all_to_all(normed, "x", 0, 0, tiled=True).reshape(448, 2048)
    rows = lax.all_gather(shard, ("zh", "zl"), axis=0, tiled=True)
    own, rows = lax.optimization_barrier((own, rows))
    other = ring(own, "c", 1)
    state_weight = copies(rows[:, :256], "y", 4).reshape(2048, 256)
    gate_piece, rest_piece = rows[:, 256:512], rows[:, 512:]
    gate_pieces = (gate_piece,) + tuple(ring(gate_piece, "y", d) for d in (1, 2, 3))
    rest_pieces = (rest_piece,) + tuple(ring(rest_piece, "y", d) for d in (1, 2, 3))

    full = shape((768, 128), F32)
    both, sent, running = call(
        states_kernel,
        (shape((768, 256), BF16), shape((16, 160, 128), BF16), shape((8, 768), F32)),
        (core,),
        (own, other, state_weight, decay_logs, tail),
        scratch=(
            pltpu.VMEM((768, 256), BF16),
            pltpu.VMEM((8, 768), F32),
            pltpu.VMEM((160, 128), BF16),
            pltpu.SemaphoreType.DMA((18,)),
        ),
        out_far=(0, 1, 2),
    )
    inner = lax.all_to_all(sent, ("zl", "y"), 0, 0, tiled=True)
    sent = call(
        level_kernel,
        shape((4, 208, 128), BF16),
        (low,),
        (inner,),
        scratch=(pltpu.VMEM((208, 128), BF16), pltpu.SemaphoreType.DMA((4,))),
        out_far=(0,),
    )
    outer = lax.all_to_all(sent, "zh", 0, 0, tiled=True)
    convolved, moments = call(
        conv_kernel,
        (full, shape((2, 768), F32)),
        (core, y),
        (own, other, *gate_pieces, kernel_taps),
        scratch=(
            pltpu.VMEM((800, 128), F32),
            pltpu.VMEM((768, 128), F32),
            pltpu.VMEM((2, 768), F32),
            pltpu.SemaphoreType.DMA((2,)),
        ),
        out_far=(0, 1),
    )
    moments = lax.all_gather(moments, ("x", "c"))
    mine, sent, weight = call(
        mixers_kernel,
        (shape((384, 256), BF16), shape((384, 2048), BF16), shape((4, 512, 256), BF16)),
        (core, y, low, high),
        (
            own,
            other,
            *rest_pieces,
            inner,
            outer,
            both,
            running,
            start_state,
            head_gain[None],
            convolved,
            moments,
            channel_gain[None],
        ),
        scratch=(
            pltpu.VMEM((16, 2048), BF16),
            pltpu.VMEM((768, 256), BF16),
            pltpu.VMEM((768, 256), BF16),
            pltpu.VMEM((768, 256), BF16),
            pltpu.VMEM((8, 768), F32),
            pltpu.VMEM((2, 2, 64, 64), F32),
            pltpu.VMEM((1, 128), F32),
            pltpu.VMEM((768, 128), F32),
            pltpu.VMEM((8, 2, 768), F32),
            pltpu.VMEM((1, 128), F32),
            pltpu.SemaphoreType.DMA((7,)),
        ),
        far=(8, 9, 10, 11, 12, 13, 14),
    )
    arrived = ring(sent, "c", 1)
    joined = call(join_kernel, shape((384, 2048), BF16), (y,), (mine, arrived, weight))
    parts = lax.all_to_all(joined.reshape(4, 96, 2048), "x", 0, 0, tiled=True)
    return call(last_kernel, shape((96, 2048), BF16), (), (parts,))


def solution(mesh):
    split = Mesh(mesh.devices.reshape(4, 4, 4, 4, 2), ALL)
    in_specs = (
        P(ALL, None),
        P(),
        P(SP, ("x", "c")),
        P(SP, ("x", "c")),
        P(SP, ("x", "c")),
        P(SP, ("x", "c")),
        P(SP, ("x", "c")),
        P(SP, ("x", "c")),
        P(None, ("x", "c")),
        P(("x", "c")),
        P(("x", "c"), SP),
        P(None, ("x", "c"), None, None),
        P(("x", "c")),
        P(("x", "c"), SP),
        P(("x", "c"), SP),
    )

    return jax.shard_map(
        body, mesh=split, in_specs=in_specs, out_specs=P(ALL, None), check_vma=False
    )
```

```python
import jax
import jax.numpy as jnp
from jax import lax
from jax.experimental import pallas as pl
from jax.experimental.pallas import tpu as pltpu
from jax.sharding import Mesh
from jax.sharding import PartitionSpec as P

DC = 1024
EPSILON = 1e-06
F32 = jnp.float32
BF16 = jnp.bfloat16
SP = ("zh", "zl", "y")
ALL = ("zh", "zl", "y", "x", "c")
NT = (((1,), (1,)), ((), ()))
TN = (((0,), (0,)), ((), ()))
VMEM = pl.BlockSpec(memory_space=pltpu.VMEM)
SMEM = pl.BlockSpec(memory_space=pltpu.SMEM)
HBM = pl.BlockSpec(memory_space=pltpu.HBM)


def call(kernel, out_shape, scalars, arrays, scratch=(), grant=20, far=(), out_far=(), aliases={}):
    def specs(count, away):
        return [HBM if i in away else VMEM for i in range(count)]

    arrays = [
        pltpu.with_memory_space_constraint(a, pltpu.HBM) if i in far else a
        for i, a in enumerate(arrays)
    ]
    if isinstance(out_shape, tuple):
        out_shape = tuple(
            pltpu.HBM(s.shape, s.dtype) if i in out_far else s for i, s in enumerate(out_shape)
        )
    elif out_far:
        out_shape = pltpu.HBM(out_shape.shape, out_shape.dtype)
    outs = specs(len(out_shape), out_far) if isinstance(out_shape, tuple) else specs(1, out_far)[0]
    return pl.pallas_call(
        kernel,
        out_shape=out_shape,
        in_specs=[SMEM] * len(scalars) + specs(len(arrays), far),
        out_specs=outs,
        scratch_shapes=scratch,
        compiler_params=pltpu.CompilerParams(vmem_limit_bytes=grant * 1024 * 1024),
        input_output_aliases=aliases,
    )(*scalars, *arrays)


def start_copies(pairs, semaphores):
    copies = [
        pltpu.make_async_copy(source, target, semaphores.at[i])
        for i, (source, target) in enumerate(pairs)
    ]
    for copy in copies:
        copy.start()
    return copies


def shape(dims, dtype):
    return jax.ShapeDtypeStruct(dims, dtype)


def swap_groups(read, write, rows):
    group = lax.broadcasted_iota(jnp.int32, (rows, 128), 1) // 32
    for outer in range(4):
        for inner in range(4):
            made = None
            for k in range(4):
                moved = read(outer, k)
                turn = ((k - inner) * 32) % 128
                if turn:
                    moved = pltpu.roll(moved, turn, 1)
                made = moved if made is None else jnp.where(group == k, moved, made)
            write(outer, inner, made)


def shard_kernel(k, v, bv, bg, q, s, oc, oh, out):
    for i, part in enumerate((k, v, bv, bg, q, s, oc)):
        out[:, i * 128 : i * 128 + 128] = part[...]
    out[:, 896:1008] = oh[:, 0:112]


def normed_rows(source, at, gain, out, to):
    rows = 16
    x = source[at, :].astype(F32)
    inverse = lax.rsqrt(jnp.mean(x * x, axis=1, keepdims=True) + EPSILON)
    normed = x * inverse * gain[...]

    def read(zh, zl):
        z = zh * 4 + zl
        return normed[:, z * 128 : z * 128 + 128]

    def write(zh, y, made):
        where = (y * 4 + zh) * 128
        out[to, where : where + 128] = made.astype(BF16)

    swap_groups(read, write, rows)


def norm_kernel(tokens_far, gain_far, out_far, tokens, gain, out, semaphores):
    for copy in start_copies(((tokens_far, tokens), (gain_far, gain)), semaphores):
        copy.wait()

    def step(i, carry):
        at = pl.ds(pl.multiple_of(i * 16, 16), 16)
        normed_rows(tokens, at, gain, out, at)
        return carry

    lax.fori_loop(0, 6, step, 0, unroll=2)
    pairs = [(out, out_far.at[k, 0:96, :]) for k in range(4)]
    for copy in start_copies(pairs, semaphores):
        copy.wait()


def edge_kernel(edge, gain, given_far, out_far, out, semaphores):
    normed_rows(edge, slice(0, 16), gain, out, slice(0, 16))
    pairs = [(out, out_far.at[k, 96:112, :]) for k in range(4)]
    for copy in start_copies(pairs, semaphores):
        copy.wait()


def last_kernel(parts, out):
    rows = 16

    def step(i, carry):
        at = pl.ds(pl.multiple_of(i * rows, rows), rows)
        total = parts[0, at, :].astype(F32)
        for k in range(1, 4):
            total = total + parts[k, at, :].astype(F32)

        def read(zh, y):
            where = (y * 4 + zh) * 128
            return total[:, where : where + 128]

        def write(zh, zl, made):
            where = (zh * 4 + zl) * 128
            out[at, where : where + 128] = made.astype(BF16)

        swap_groups(read, write, rows)
        return carry

    lax.fori_loop(0, 6, step, 0, unroll=2)


def lane_is_second(rows):
    return lax.broadcasted_iota(jnp.int32, (rows, 128), 1) >= 64


def by_lane(running):
    turned = jnp.transpose(running)
    return jnp.where(lane_is_second(turned.shape[0]), turned[:, 1:2], turned[:, 0:1])


def put_rows(core, own, other, target):
    for k in range(4):
        mine = pl.ds(pl.multiple_of(k * 192 + core * 96, 32), 96)
        theirs = pl.ds(pl.multiple_of(k * 192 + (1 - core) * 96, 32), 96)
        part = slice(k * 112, k * 112 + 96)
        target[mine, :] = own[part, :].astype(BF16)
        target[theirs, :] = other[part, :].astype(BF16)


def summed(x):
    lane = lax.broadcasted_iota(jnp.int32, x.shape, 1)
    shift = 1
    while shift < x.shape[1]:
        x = x + jnp.where(lane >= shift, pltpu.roll(x, shift, 1), 0.0)
        shift *= 2
    return x


def states_kernel(
    core,
    own,
    other,
    weight,
    decay,
    tail,
    both_far,
    message_far,
    running_far,
    both,
    running,
    message,
    semaphores,
):
    running[...] = summed(jnp.concatenate([decay[...], jnp.zeros((6, 768), F32)], axis=0))
    w = weight[...]
    put_rows(
        core[0],
        jnp.dot(own[...], w, preferred_element_type=F32),
        jnp.dot(other[...], w, preferred_element_type=F32),
        both,
    )
    kept = start_copies(
        ((both, both_far), (running, running_far)), semaphores.at[pl.ds(16, 2)]
    )
    logs = by_lane(running[...])
    closing = logs[767:768, :]
    k = both[:, 0:128].astype(F32) * 0.125
    v = both[:, 128:256]
    second = lane_is_second(64)
    ahead = lax.dot_general(
        (k * jnp.exp(closing - logs)).astype(BF16), v, TN, preferred_element_type=F32
    )
    back = lax.dot_general((k * jnp.exp(logs)).astype(BF16), v, TN, preferred_element_type=F32)
    parts = (
        (slice(0, 64), jnp.where(second, ahead[64:, :], ahead[:64, :]).astype(BF16)),
        (slice(64, 128), jnp.where(second, back[64:, :], back[:64, :]).astype(BF16)),
        (slice(128, 144), log_rows(closing)),
        (slice(144, 160), tail[...]),
    )
    for at, part in parts:
        message[at, :] = part
    kept += start_copies([(message, message_far.at[k]) for k in range(16)], semaphores)
    for copy in kept:
        copy.wait()


def log_rows(log):
    high = log.astype(BF16)
    low = (log - high.astype(F32)).astype(BF16)
    first = lax.broadcasted_iota(jnp.int32, (16, 128), 0) < 8
    return jnp.where(first, high.astype(F32), low.astype(F32)).astype(BF16)


def scan_states(gathered, count, position):
    def log_of(m):
        return gathered[m, 128:129, :].astype(F32) + gathered[m, 136:137, :].astype(F32)

    def one_way(order, rows):
        state = jnp.zeros((64, 128), F32)
        log = jnp.zeros((1, 128), F32)
        held, held_log = state, log
        for m in order:
            here = position == m
            held = jnp.where(here, state, held)
            held_log = jnp.where(here, log, held_log)
            own = log_of(m)
            state = jnp.exp(own) * state + gathered[m, rows, :].astype(F32)
            log = log + own
        return held, held_log, state, log

    ahead = one_way(range(count), slice(0, 64))
    back = one_way(reversed(range(count)), slice(64, 128))
    return ahead, back


def level_kernel(position, gathered, message_far, message, semaphores):
    ahead, back = scan_states(gathered, 16, position[0])
    parts = [
        (slice(0, 64), ahead[2].astype(BF16)),
        (slice(64, 128), back[2].astype(BF16)),
        (slice(128, 144), log_rows(ahead[3])),
    ]
    group = lax.broadcasted_iota(jnp.int32, (16, 128), 1) // 32
    for y in range(4):
        made = gathered[y, 144:160, :].astype(F32)
        for zl in range(1, 4):
            moved = pltpu.roll(gathered[zl * 4 + y, 144:160, :].astype(F32), zl * 32, 1)
            made = jnp.where(group == zl, moved, made)
        parts.append((slice(144 + y * 16, 160 + y * 16), made.astype(BF16)))
    for at, part in parts:
        message[at, :] = part
    for copy in start_copies([(message, message_far.at[k]) for k in range(4)], semaphores):
        copy.wait()


def column_block(position, shift):
    return pl.ds(pl.multiple_of(((position + 4 - shift) % 4) * 512, 512), 512)


def by_piece(y, rows, pieces, lanes):
    total = None
    for shift, piece in enumerate(pieces):
        part = jnp.dot(
            rows[:, column_block(y, shift)], piece[:, lanes], preferred_element_type=F32
        )
        total = part if total is None else total + part
    return total


def conv_kernel(core, y, own, other, p0, p1, p2, p3, taps, convolved_far, moments_far, padded, convolved, moments, semaphores):
    pieces = (p0, p1, p2, p3)

    def rows_of(rows):
        both = by_piece(y[0], rows, pieces, slice(0, 256))
        return (both[:, :128] * jax.nn.sigmoid(both[:, 128:])).astype(BF16).astype(F32)

    first, second = rows_of(own), rows_of(other)
    for k in range(4):
        mine = pl.ds(pl.multiple_of(16 + k * 192 + core[0] * 96, 16), 96)
        theirs = pl.ds(pl.multiple_of(16 + k * 192 + (1 - core[0]) * 96, 16), 96)
        padded[mine, :] = first[k * 112 : k * 112 + 96, :]
        padded[theirs, :] = second[k * 112 : k * 112 + 96, :]
    is_second = jnp.full((16, 128), core[0], jnp.int32) == 1
    padded[0:16, :] = jnp.where(is_second, first[432:448, :], second[432:448, :])
    padded[784:800, :] = jnp.where(is_second, second[96:112, :], first[96:112, :])
    ones = jnp.ones((8, 128), F32)
    rows = 128
    for i in range(6):
        total = None
        for j in range(31):
            start = i * rows + j + 1
            term = taps[j : j + 1, :] * padded[start : start + rows, :]
            total = term if total is None else total + term
        convolved[i * rows : (i + 1) * rows, :] = total
        highest = lax.Precision.HIGHEST
        s1 = lax.dot_general(ones, total, NT, precision=highest, preferred_element_type=F32)
        s2 = lax.dot_general(ones, total * total, NT, precision=highest, preferred_element_type=F32)
        moments[0:1, i * rows : (i + 1) * rows] = s1[0:1]
        moments[1:2, i * rows : (i + 1) * rows] = s2[0:1]
    pairs = ((convolved, convolved_far), (moments, moments_far))
    for copy in start_copies(pairs, semaphores):
        copy.wait()


def out_rows(y, rows, weight, write):
    for shift in range(4):
        part = lax.dot_general(rows, weight[shift], NT, preferred_element_type=F32)
        write(column_block(y, shift), part)


def mixers_kernel(
    core,
    y,
    low,
    high,
    own,
    other,
    p0,
    p1,
    p2,
    p3,
    inner,
    outer,
    both_far,
    running_far,
    start_far,
    head_gain_far,
    convolved_far,
    moments_far,
    channel_gain_far,
    mine,
    sent,
    weight,
    spare,
    pair,
    rows_in,
    both,
    running,
    start,
    head_gain,
    convolved,
    moments,
    channel_gain,
    semaphores,
):
    pieces = (p0, p1, p2, p3)
    loads = start_copies(
        (
            (both_far, both),
            (running_far, running),
            (start_far, start),
            (head_gain_far, head_gain),
            (convolved_far, convolved),
            (moments_far, moments),
            (channel_gain_far, channel_gain),
        ),
        semaphores,
    )
    put_rows(
        core[0],
        by_piece(y[0], own, pieces, slice(0, 256)),
        by_piece(y[0], other, pieces, slice(0, 256)),
        pair,
    )
    for load in loads:
        load.wait()
    near = scan_states(inner, 16, low[0])
    far = scan_states(outer, 4, high[0])
    second = lane_is_second(64)

    def entering(way):
        begun = jnp.concatenate([start[way, 0], start[way, 1]], axis=1)
        state = far[way][0] + jnp.exp(far[way][1]) * begun
        state = near[way][0] + jnp.exp(near[way][1]) * state
        return jnp.concatenate(
            [jnp.where(second, 0.0, state), jnp.where(second, state, 0.0)], axis=0
        ).astype(BF16)

    forward, backward = entering(0), entering(1)
    logs = running[...]
    turned = jnp.transpose(logs)
    sums = moments[0]
    for k in range(1, 8):
        sums = sums + moments[k]
    sums = jnp.transpose(jnp.concatenate([sums, jnp.zeros((6, 768), F32)], axis=0)) / DC
    for yy in range(4):
        for zh in range(4):
            where = yy * 512 + zh * 128
            spare[:, where : where + 128] = outer[zh, 144 + yy * 16 : 160 + yy * 16, :]
    for shift, piece in enumerate(pieces):
        last = jnp.transpose(spare[:, column_block(y[0], shift)].astype(F32)).astype(BF16)
        weight[shift, :, 0:240] = piece[:, 256:496]
        weight[shift, :, 240:256] = last

    k = (both[:, 0:128].astype(F32) * 0.125).astype(BF16)
    v = both[:, 128:256]
    rows = 128
    zero = jnp.zeros((), BF16)
    half = lane_is_second(rows)
    diagonal = lax.broadcasted_iota(jnp.int32, (rows, rows), 0) == (
        lax.broadcasted_iota(jnp.int32, (rows, rows), 1)
    )

    def head_mean(x):
        first = jnp.sum(jnp.where(half, 0.0, x), axis=1, keepdims=True)
        last = jnp.sum(jnp.where(half, x, 0.0), axis=1, keepdims=True)
        return jnp.where(half, last, first) / 64

    for i in range(6):
        at = slice(i * rows, (i + 1) * rows)
        q = pair[at, 0:128]
        log = jnp.where(half, turned[at, 1:2], turned[at, 0:1])
        closing = jnp.where(half[0:1], turned[767:768, 1:2], turned[767:768, 0:1])
        retained = jnp.exp(log) * jnp.dot(q, forward, preferred_element_type=F32)
        retained = retained + jnp.exp(closing - log) * jnp.dot(
            q, backward, preferred_element_type=F32
        )
        stacked = jnp.concatenate(
            [jnp.where(half, zero, q), jnp.where(half, q, zero)], axis=0
        )
        scores = lax.dot_general(stacked, k, NT, preferred_element_type=F32)
        parts = []
        for h in range(2):
            distance = jnp.abs(turned[at, h : h + 1] - logs[h : h + 1, :])
            head_scores = scores[h * rows : (h + 1) * rows, :]
            part = head_scores * jnp.exp(-distance)
            twice = part[:, at] + jnp.where(diagonal, head_scores[:, at], 0.0)
            sides = [part[:, : at.start], twice, part[:, at.stop :]]
            part = jnp.concatenate([side for side in sides if side.shape[1]], axis=1)
            parts.append(part.astype(BF16))
        mixed = jnp.dot(jnp.concatenate(parts, axis=0), v, preferred_element_type=F32)
        retained = retained + jnp.where(half, mixed[rows:, :], mixed[:rows, :])
        centred = retained - head_mean(retained)
        normed = centred * lax.rsqrt(head_mean(centred * centred) + EPSILON)
        gate = jax.nn.silu(pair[at, 128:256].astype(F32))
        rows_in[at, 128:256] = (normed * head_gain[...] * gate).astype(BF16)
        average, squares = sums[at, 0:1], sums[at, 1:2]
        scaled = (convolved[at, :] - average) * lax.rsqrt(squares - average * average + EPSILON)
        rows_in[at, 0:128] = jax.nn.silu(scaled * channel_gain[...]).astype(BF16)

    def half_of(which):
        return jnp.concatenate(
            [
                rows_in[pl.ds(pl.multiple_of(k * 192 + which * 96, 32), 96), :]
                for k in range(4)
            ],
            axis=0,
        )

    mine[...] = half_of(core[0])

    def write(lanes, part):
        sent[:, lanes] = part.astype(BF16)

    out_rows(y[0], half_of(1 - core[0]), weight, write)


def join_kernel(y, mine, arrived, weight, out):
    def write(lanes, part):
        out[:, lanes] = (part + arrived[:, lanes].astype(F32)).astype(BF16)

    out_rows(y[0], mine[...], weight, write)


def ring(x, axis, shift):
    count = lax.axis_size(axis)
    return lax.ppermute(x, axis, [(i, (i + shift) % count) for i in range(count)])


def copies(x, axes, count):
    return lax.all_to_all(
        jnp.broadcast_to(x[None], (count, *x.shape)), axes, 0, 0, tiled=True
    )


def body(
    tokens,
    input_gain,
    branch_value,
    branch_gate,
    query_weight,
    key_weight,
    value_weight,
    swish_weight,
    kernel_taps,
    channel_gain,
    decay_logs,
    start_state,
    head_gain,
    output_conv,
    output_heads,
):
    core = lax.axis_index("c").astype(jnp.int32)[None]
    y = lax.axis_index("y").astype(jnp.int32)[None]
    high = lax.axis_index("zh").astype(jnp.int32)[None]
    low = lax.axis_index(("zl", "y")).astype(jnp.int32)[None]

    place = lax.axis_index(("x", "c"))
    count = lax.axis_size(SP)
    edge = lax.ppermute(
        jnp.where(place == 7, tokens[80:96], tokens[0:16]),
        ALL,
        [(i * 8 + 7, i * 8 + 15) for i in range(count - 1)]
        + [(i * 8 + 8, i * 8) for i in range(count - 1)],
    )
    shard = call(
        shard_kernel,
        shape((32, 1008), BF16),
        (),
        (
            key_weight,
            value_weight,
            branch_value,
            branch_gate,
            query_weight,
            swish_weight,
            output_conv.T,
            output_heads.T,
        ),
        grant=56,
    )
    tail = jnp.pad(output_heads[112:], ((0, 0), (0, 96)))
    normed = call(
        norm_kernel,
        shape((4, 112, 2048), BF16),
        (),
        (tokens, input_gain[None]),
        scratch=(
            pltpu.VMEM((96, 2048), BF16),
            pltpu.VMEM((1, 2048), F32),
            pltpu.VMEM((96, 2048), BF16),
            pltpu.SemaphoreType.DMA((4,)),
        ),
        far=(0, 1),
        out_far=(0,),
    )
    edge, normed = lax.optimization_barrier((edge, normed))
    normed = call(
        edge_kernel,
        shape((4, 112, 2048), BF16),
        (),
        (edge, input_gain[None], normed),
        scratch=(pltpu.VMEM((16, 2048), BF16), pltpu.SemaphoreType.DMA((4,))),
        far=(2,),
        out_far=(0,),
        aliases={2: 0},
    )
    shard, normed = lax.optimization_barrier((shard, normed))
    own = lax.all_to_all(normed, "x", 0, 0, tiled=True).reshape(448, 2048)
    rows = lax.all_gather(shard, ("zh", "zl"), axis=0, tiled=True)
    own, rows = lax.optimization_barrier((own, rows))
    other = ring(own, "c", 1)
    state_weight = copies(rows[:, :256], "y", 4).reshape(2048, 256)
    gate_piece, rest_piece = rows[:, 256:512], rows[:, 512:]
    gate_pieces = (gate_piece,) + tuple(ring(gate_piece, "y", d) for d in (1, 2, 3))
    rest_pieces = (rest_piece,) + tuple(ring(rest_piece, "y", d) for d in (1, 2, 3))

    full = shape((768, 128), F32)
    both, sent, running = call(
        states_kernel,
        (shape((768, 256), BF16), shape((16, 160, 128), BF16), shape((8, 768), F32)),
        (core,),
        (own, other, state_weight, decay_logs, tail),
        scratch=(
            pltpu.VMEM((768, 256), BF16),
            pltpu.VMEM((8, 768), F32),
            pltpu.VMEM((160, 128), BF16),
            pltpu.SemaphoreType.DMA((18,)),
        ),
        out_far=(0, 1, 2),
    )
    inner = lax.all_to_all(sent, ("zl", "y"), 0, 0, tiled=True)
    sent = call(
        level_kernel,
        shape((4, 208, 128), BF16),
        (low,),
        (inner,),
        scratch=(pltpu.VMEM((208, 128), BF16), pltpu.SemaphoreType.DMA((4,))),
        out_far=(0,),
    )
    outer = lax.all_to_all(sent, "zh", 0, 0, tiled=True)
    convolved, moments = call(
        conv_kernel,
        (full, shape((2, 768), F32)),
        (core, y),
        (own, other, *gate_pieces, kernel_taps),
        scratch=(
            pltpu.VMEM((800, 128), F32),
            pltpu.VMEM((768, 128), F32),
            pltpu.VMEM((2, 768), F32),
            pltpu.SemaphoreType.DMA((2,)),
        ),
        out_far=(0, 1),
    )
    moments = lax.all_gather(moments, ("x", "c"))
    mine, sent, weight = call(
        mixers_kernel,
        (shape((384, 256), BF16), shape((384, 2048), BF16), shape((4, 512, 256), BF16)),
        (core, y, low, high),
        (
            own,
            other,
            *rest_pieces,
            inner,
            outer,
            both,
            running,
            start_state,
            head_gain[None],
            convolved,
            moments,
            channel_gain[None],
        ),
        scratch=(
            pltpu.VMEM((16, 2048), BF16),
            pltpu.VMEM((768, 256), BF16),
            pltpu.VMEM((768, 256), BF16),
            pltpu.VMEM((768, 256), BF16),
            pltpu.VMEM((8, 768), F32),
            pltpu.VMEM((2, 2, 64, 64), F32),
            pltpu.VMEM((1, 128), F32),
            pltpu.VMEM((768, 128), F32),
            pltpu.VMEM((8, 2, 768), F32),
            pltpu.VMEM((1, 128), F32),
            pltpu.SemaphoreType.DMA((7,)),
        ),
        far=(8, 9, 10, 11, 12, 13, 14),
    )
    arrived = ring(sent, "c", 1)
    joined = call(join_kernel, shape((384, 2048), BF16), (y,), (mine, arrived, weight))
    parts = lax.all_to_all(joined.reshape(4, 96, 2048), "x", 0, 0, tiled=True)
    return call(last_kernel, shape((96, 2048), BF16), (), (parts,))


def solution(mesh):
    split = Mesh(mesh.devices.reshape(4, 4, 4, 4, 2), ALL)
    in_specs = (
        P(ALL, None),
        P(),
        P(SP, ("x", "c")),
        P(SP, ("x", "c")),
        P(SP, ("x", "c")),
        P(SP, ("x", "c")),
        P(SP, ("x", "c")),
        P(SP, ("x", "c")),
        P(None, ("x", "c")),
        P(("x", "c")),
        P(("x", "c"), SP),
        P(None, ("x", "c"), None, None),
        P(("x", "c")),
        P(("x", "c"), SP),
        P(("x", "c"), SP),
    )

    return jax.shard_map(
        body, mesh=split, in_specs=in_specs, out_specs=P(ALL, None), check_vma=False
    )
```

```python
import jax
import jax.numpy as jnp
from jax import lax
from jax.experimental import pallas as pl
from jax.experimental.pallas import tpu as pltpu
from jax.sharding import Mesh
from jax.sharding import PartitionSpec as P

DC = 1024
EPSILON = 1e-06
F32 = jnp.float32
BF16 = jnp.bfloat16
SP = ("zh", "zl", "y")
ALL = ("zh", "zl", "y", "x", "c")
NT = (((1,), (1,)), ((), ()))
TN = (((0,), (0,)), ((), ()))
VMEM = pl.BlockSpec(memory_space=pltpu.VMEM)
SMEM = pl.BlockSpec(memory_space=pltpu.SMEM)
HBM = pl.BlockSpec(memory_space=pltpu.HBM)


def call(kernel, out_shape, scalars, arrays, scratch=(), grant=20, far=(), out_far=(), aliases={}):
    def specs(count, away):
        return [HBM if i in away else VMEM for i in range(count)]

    arrays = [
        pltpu.with_memory_space_constraint(a, pltpu.HBM) if i in far else a
        for i, a in enumerate(arrays)
    ]
    if isinstance(out_shape, tuple):
        out_shape = tuple(
            pltpu.HBM(s.shape, s.dtype) if i in out_far else s for i, s in enumerate(out_shape)
        )
    elif out_far:
        out_shape = pltpu.HBM(out_shape.shape, out_shape.dtype)
    outs = specs(len(out_shape), out_far) if isinstance(out_shape, tuple) else specs(1, out_far)[0]
    return pl.pallas_call(
        kernel,
        out_shape=out_shape,
        in_specs=[SMEM] * len(scalars) + specs(len(arrays), far),
        out_specs=outs,
        scratch_shapes=scratch,
        compiler_params=pltpu.CompilerParams(vmem_limit_bytes=grant * 1024 * 1024),
        input_output_aliases=aliases,
    )(*scalars, *arrays)


def start_copies(pairs, semaphores):
    copies = [
        pltpu.make_async_copy(source, target, semaphores.at[i])
        for i, (source, target) in enumerate(pairs)
    ]
    for copy in copies:
        copy.start()
    return copies


def shape(dims, dtype):
    return jax.ShapeDtypeStruct(dims, dtype)


def swap_groups(read, write, rows):
    group = lax.broadcasted_iota(jnp.int32, (rows, 128), 1) // 32
    for outer in range(4):
        for inner in range(4):
            made = None
            for k in range(4):
                moved = read(outer, k)
                turn = ((k - inner) * 32) % 128
                if turn:
                    moved = pltpu.roll(moved, turn, 1)
                made = moved if made is None else jnp.where(group == k, moved, made)
            write(outer, inner, made)


def shard_kernel(k, v, bv, bg, q, s, oc, oh, out):
    for i, part in enumerate((k, v, bv, bg, q, s, oc)):
        out[:, i * 128 : i * 128 + 128] = part[...]
    out[:, 896:1008] = oh[:, 0:112]


def normed_rows(source, at, gain, out, to):
    rows = 16
    x = source[at, :].astype(F32)
    inverse = lax.rsqrt(jnp.mean(x * x, axis=1, keepdims=True) + EPSILON)
    normed = x * inverse * gain[...]

    def read(zh, zl):
        z = zh * 4 + zl
        return normed[:, z * 128 : z * 128 + 128]

    def write(zh, y, made):
        where = (y * 4 + zh) * 128
        out[to, where : where + 128] = made.astype(BF16)

    swap_groups(read, write, rows)


def norm_kernel(tokens_far, gain_far, out_far, tokens, gain, out, semaphores):
    for copy in start_copies(((tokens_far, tokens), (gain_far, gain)), semaphores):
        copy.wait()

    def step(i, carry):
        at = pl.ds(pl.multiple_of(i * 16, 16), 16)
        normed_rows(tokens, at, gain, out, at)
        return carry

    lax.fori_loop(0, 6, step, 0, unroll=2)
    pairs = [(out, out_far.at[k, 0:96, :]) for k in range(4)]
    for copy in start_copies(pairs, semaphores):
        copy.wait()


def edge_kernel(edge, gain, given_far, out_far, out, semaphores):
    normed_rows(edge, slice(0, 16), gain, out, slice(0, 16))
    pairs = [(out, out_far.at[k, 96:112, :]) for k in range(4)]
    for copy in start_copies(pairs, semaphores):
        copy.wait()


def last_kernel(parts, out):
    rows = 16

    def step(i, carry):
        at = pl.ds(pl.multiple_of(i * rows, rows), rows)
        total = parts[0, at, :].astype(F32)
        for k in range(1, 4):
            total = total + parts[k, at, :].astype(F32)

        def read(zh, y):
            where = (y * 4 + zh) * 128
            return total[:, where : where + 128]

        def write(zh, zl, made):
            where = (zh * 4 + zl) * 128
            out[at, where : where + 128] = made.astype(BF16)

        swap_groups(read, write, rows)
        return carry

    lax.fori_loop(0, 6, step, 0, unroll=2)


def lane_is_second(rows):
    return lax.broadcasted_iota(jnp.int32, (rows, 128), 1) >= 64


def by_lane(running):
    turned = jnp.transpose(running)
    return jnp.where(lane_is_second(turned.shape[0]), turned[:, 1:2], turned[:, 0:1])


def put_rows(core, own, other, target):
    for k in range(4):
        mine = pl.ds(pl.multiple_of(k * 192 + core * 96, 32), 96)
        theirs = pl.ds(pl.multiple_of(k * 192 + (1 - core) * 96, 32), 96)
        part = slice(k * 112, k * 112 + 96)
        target[mine, :] = own[part, :].astype(BF16)
        target[theirs, :] = other[part, :].astype(BF16)


def summed(x):
    lane = lax.broadcasted_iota(jnp.int32, x.shape, 1)
    shift = 1
    while shift < x.shape[1]:
        x = x + jnp.where(lane >= shift, pltpu.roll(x, shift, 1), 0.0)
        shift *= 2
    return x


def states_kernel(
    core,
    own,
    other,
    weight,
    decay,
    tail,
    both_far,
    message_far,
    running_far,
    both,
    running,
    message,
    semaphores,
):
    running[...] = summed(jnp.concatenate([decay[...], jnp.zeros((6, 768), F32)], axis=0))
    w = weight[...]
    put_rows(
        core[0],
        jnp.dot(own[...], w, preferred_element_type=F32),
        jnp.dot(other[...], w, preferred_element_type=F32),
        both,
    )
    kept = start_copies(
        ((both, both_far), (running, running_far)), semaphores.at[pl.ds(16, 2)]
    )
    logs = by_lane(running[...])
    closing = logs[767:768, :]
    k = both[:, 0:128].astype(F32) * 0.125
    v = both[:, 128:256]
    second = lane_is_second(64)
    ahead = lax.dot_general(
        (k * jnp.exp(closing - logs)).astype(BF16), v, TN, preferred_element_type=F32
    )
    back = lax.dot_general((k * jnp.exp(logs)).astype(BF16), v, TN, preferred_element_type=F32)
    parts = (
        (slice(0, 64), jnp.where(second, ahead[64:, :], ahead[:64, :]).astype(BF16)),
        (slice(64, 128), jnp.where(second, back[64:, :], back[:64, :]).astype(BF16)),
        (slice(128, 144), log_rows(closing)),
        (slice(144, 160), tail[...]),
    )
    for at, part in parts:
        message[at, :] = part
    kept += start_copies([(message, message_far.at[k]) for k in range(16)], semaphores)
    for copy in kept:
        copy.wait()


def log_rows(log):
    high = log.astype(BF16)
    low = (log - high.astype(F32)).astype(BF16)
    first = lax.broadcasted_iota(jnp.int32, (16, 128), 0) < 8
    return jnp.where(first, high.astype(F32), low.astype(F32)).astype(BF16)


def scan_states(gathered, count, position):
    def log_of(m):
        return gathered[m, 128:129, :].astype(F32) + gathered[m, 136:137, :].astype(F32)

    def one_way(order, rows):
        state = jnp.zeros((64, 128), F32)
        log = jnp.zeros((1, 128), F32)
        held, held_log = state, log
        for m in order:
            here = position == m
            held = jnp.where(here, state, held)
            held_log = jnp.where(here, log, held_log)
            own = log_of(m)
            state = jnp.exp(own) * state + gathered[m, rows, :].astype(F32)
            log = log + own
        return held, held_log, state, log

    ahead = one_way(range(count), slice(0, 64))
    back = one_way(reversed(range(count)), slice(64, 128))
    return ahead, back


def level_kernel(position, gathered, message_far, message, semaphores):
    ahead, back = scan_states(gathered, 16, position[0])
    parts = [
        (slice(0, 64), ahead[2].astype(BF16)),
        (slice(64, 128), back[2].astype(BF16)),
        (slice(128, 144), log_rows(ahead[3])),
    ]
    group = lax.broadcasted_iota(jnp.int32, (16, 128), 1) // 32
    for y in range(4):
        made = gathered[y, 144:160, :].astype(F32)
        for zl in range(1, 4):
            moved = pltpu.roll(gathered[zl * 4 + y, 144:160, :].astype(F32), zl * 32, 1)
            made = jnp.where(group == zl, moved, made)
        parts.append((slice(144 + y * 16, 160 + y * 16), made.astype(BF16)))
    for at, part in parts:
        message[at, :] = part
    for copy in start_copies([(message, message_far.at[k]) for k in range(4)], semaphores):
        copy.wait()


def column_block(position, shift):
    return pl.ds(pl.multiple_of(((position + 4 - shift) % 4) * 512, 512), 512)


def by_piece(y, rows, pieces, lanes):
    total = None
    for shift, piece in enumerate(pieces):
        part = jnp.dot(
            rows[:, column_block(y, shift)], piece[:, lanes], preferred_element_type=F32
        )
        total = part if total is None else total + part
    return total


def conv_kernel(core, y, own, other, p0, p1, p2, p3, taps, convolved_far, moments_far, padded, convolved, moments, semaphores):
    pieces = (p0, p1, p2, p3)

    def rows_of(rows):
        both = by_piece(y[0], rows, pieces, slice(0, 256))
        return (both[:, :128] * jax.nn.sigmoid(both[:, 128:])).astype(BF16).astype(F32)

    first, second = rows_of(own), rows_of(other)
    for k in range(4):
        mine = pl.ds(pl.multiple_of(16 + k * 192 + core[0] * 96, 16), 96)
        theirs = pl.ds(pl.multiple_of(16 + k * 192 + (1 - core[0]) * 96, 16), 96)
        padded[mine, :] = first[k * 112 : k * 112 + 96, :]
        padded[theirs, :] = second[k * 112 : k * 112 + 96, :]
    is_second = jnp.full((16, 128), core[0], jnp.int32) == 1
    padded[0:16, :] = jnp.where(is_second, first[432:448, :], second[432:448, :])
    padded[784:800, :] = jnp.where(is_second, second[96:112, :], first[96:112, :])
    rows = 128
    first_lane = lax.broadcasted_iota(jnp.int32, (rows, 128), 1) == 0
    for i in range(6):
        total = None
        for j in range(31):
            start = i * rows + j + 1
            term = taps[j : j + 1, :] * padded[start : start + rows, :]
            total = term if total is None else total + term
        convolved[i * rows : (i + 1) * rows, :] = total
        s1 = jnp.sum(total, axis=1, keepdims=True)
        s2 = jnp.sum(total * total, axis=1, keepdims=True)
        turned = jnp.transpose(jnp.where(first_lane, s1, s2))
        moments[0:1, i * rows : (i + 1) * rows] = turned[0:1]
        moments[1:2, i * rows : (i + 1) * rows] = turned[1:2]
    pairs = ((convolved, convolved_far), (moments, moments_far))
    for copy in start_copies(pairs, semaphores):
        copy.wait()


def out_rows(y, rows, weight, write):
    for shift in range(4):
        part = lax.dot_general(rows, weight[shift], NT, preferred_element_type=F32)
        write(column_block(y, shift), part)


def mixers_kernel(
    core,
    y,
    low,
    high,
    own,
    other,
    p0,
    p1,
    p2,
    p3,
    inner,
    outer,
    both_far,
    running_far,
    start_far,
    head_gain_far,
    convolved_far,
    moments_far,
    channel_gain_far,
    mine,
    sent,
    weight,
    spare,
    pair,
    rows_in,
    both,
    running,
    start,
    head_gain,
    convolved,
    moments,
    channel_gain,
    semaphores,
):
    pieces = (p0, p1, p2, p3)
    loads = start_copies(
        (
            (both_far, both),
            (running_far, running),
            (start_far, start),
            (head_gain_far, head_gain),
            (convolved_far, convolved),
            (moments_far, moments),
            (channel_gain_far, channel_gain),
        ),
        semaphores,
    )
    put_rows(
        core[0],
        by_piece(y[0], own, pieces, slice(0, 256)),
        by_piece(y[0], other, pieces, slice(0, 256)),
        pair,
    )
    for load in loads:
        load.wait()
    near = scan_states(inner, 16, low[0])
    far = scan_states(outer, 4, high[0])
    second = lane_is_second(64)

    def entering(way):
        begun = jnp.concatenate([start[way, 0], start[way, 1]], axis=1)
        state = far[way][0] + jnp.exp(far[way][1]) * begun
        state = near[way][0] + jnp.exp(near[way][1]) * state
        return jnp.concatenate(
            [jnp.where(second, 0.0, state), jnp.where(second, state, 0.0)], axis=0
        ).astype(BF16)

    forward, backward = entering(0), entering(1)
    logs = running[...]
    turned = jnp.transpose(logs)
    sums = moments[0]
    for k in range(1, 8):
        sums = sums + moments[k]
    sums = jnp.transpose(jnp.concatenate([sums, jnp.zeros((6, 768), F32)], axis=0)) / DC
    for yy in range(4):
        for zh in range(4):
            where = yy * 512 + zh * 128
            spare[:, where : where + 128] = outer[zh, 144 + yy * 16 : 160 + yy * 16, :]
    for shift, piece in enumerate(pieces):
        last = jnp.transpose(spare[:, column_block(y[0], shift)].astype(F32)).astype(BF16)
        weight[shift, :, 0:240] = piece[:, 256:496]
        weight[shift, :, 240:256] = last

    k = (both[:, 0:128].astype(F32) * 0.125).astype(BF16)
    v = both[:, 128:256]
    rows = 128
    zero = jnp.zeros((), BF16)
    half = lane_is_second(rows)
    diagonal = lax.broadcasted_iota(jnp.int32, (rows, rows), 0) == (
        lax.broadcasted_iota(jnp.int32, (rows, rows), 1)
    )

    def head_mean(x):
        first = jnp.sum(jnp.where(half, 0.0, x), axis=1, keepdims=True)
        last = jnp.sum(jnp.where(half, x, 0.0), axis=1, keepdims=True)
        return jnp.where(half, last, first) / 64

    for i in range(6):
        at = slice(i * rows, (i + 1) * rows)
        q = pair[at, 0:128]
        log = jnp.where(half, turned[at, 1:2], turned[at, 0:1])
        closing = jnp.where(half[0:1], turned[767:768, 1:2], turned[767:768, 0:1])
        retained = jnp.exp(log) * jnp.dot(q, forward, preferred_element_type=F32)
        retained = retained + jnp.exp(closing - log) * jnp.dot(
            q, backward, preferred_element_type=F32
        )
        stacked = jnp.concatenate(
            [jnp.where(half, zero, q), jnp.where(half, q, zero)], axis=0
        )
        scores = lax.dot_general(stacked, k, NT, preferred_element_type=F32)
        parts = []
        for h in range(2):
            distance = jnp.abs(turned[at, h : h + 1] - logs[h : h + 1, :])
            head_scores = scores[h * rows : (h + 1) * rows, :]
            part = head_scores * jnp.exp(-distance)
            twice = part[:, at] + jnp.where(diagonal, head_scores[:, at], 0.0)
            sides = [part[:, : at.start], twice, part[:, at.stop :]]
            part = jnp.concatenate([side for side in sides if side.shape[1]], axis=1)
            parts.append(part.astype(BF16))
        mixed = jnp.dot(jnp.concatenate(parts, axis=0), v, preferred_element_type=F32)
        retained = retained + jnp.where(half, mixed[rows:, :], mixed[:rows, :])
        centred = retained - head_mean(retained)
        normed = centred * lax.rsqrt(head_mean(centred * centred) + EPSILON)
        gate = jax.nn.silu(pair[at, 128:256].astype(F32))
        rows_in[at, 128:256] = (normed * head_gain[...] * gate).astype(BF16)
        average, squares = sums[at, 0:1], sums[at, 1:2]
        scaled = (convolved[at, :] - average) * lax.rsqrt(squares - average * average + EPSILON)
        rows_in[at, 0:128] = jax.nn.silu(scaled * channel_gain[...]).astype(BF16)

    def half_of(which):
        return jnp.concatenate(
            [
                rows_in[pl.ds(pl.multiple_of(k * 192 + which * 96, 32), 96), :]
                for k in range(4)
            ],
            axis=0,
        )

    mine[...] = half_of(core[0])

    def write(lanes, part):
        sent[:, lanes] = part.astype(BF16)

    out_rows(y[0], half_of(1 - core[0]), weight, write)


def join_kernel(y, mine, arrived, weight, out):
    def write(lanes, part):
        out[:, lanes] = (part + arrived[:, lanes].astype(F32)).astype(BF16)

    out_rows(y[0], mine[...], weight, write)


def ring(x, axis, shift):
    count = lax.axis_size(axis)
    return lax.ppermute(x, axis, [(i, (i + shift) % count) for i in range(count)])


def copies(x, axes, count):
    return lax.all_to_all(
        jnp.broadcast_to(x[None], (count, *x.shape)), axes, 0, 0, tiled=True
    )


def body(
    tokens,
    input_gain,
    branch_value,
    branch_gate,
    query_weight,
    key_weight,
    value_weight,
    swish_weight,
    kernel_taps,
    channel_gain,
    decay_logs,
    start_state,
    head_gain,
    output_conv,
    output_heads,
):
    core = lax.axis_index("c").astype(jnp.int32)[None]
    y = lax.axis_index("y").astype(jnp.int32)[None]
    high = lax.axis_index("zh").astype(jnp.int32)[None]
    low = lax.axis_index(("zl", "y")).astype(jnp.int32)[None]

    place = lax.axis_index(("x", "c"))
    count = lax.axis_size(SP)
    edge = lax.ppermute(
        jnp.where(place == 7, tokens[80:96], tokens[0:16]),
        ALL,
        [(i * 8 + 7, i * 8 + 15) for i in range(count - 1)]
        + [(i * 8 + 8, i * 8) for i in range(count - 1)],
    )
    shard = call(
        shard_kernel,
        shape((32, 1008), BF16),
        (),
        (
            key_weight,
            value_weight,
            branch_value,
            branch_gate,
            query_weight,
            swish_weight,
            output_conv.T,
            output_heads.T,
        ),
        grant=56,
    )
    tail = jnp.pad(output_heads[112:], ((0, 0), (0, 96)))
    normed = call(
        norm_kernel,
        shape((4, 112, 2048), BF16),
        (),
        (tokens, input_gain[None]),
        scratch=(
            pltpu.VMEM((96, 2048), BF16),
            pltpu.VMEM((1, 2048), F32),
            pltpu.VMEM((96, 2048), BF16),
            pltpu.SemaphoreType.DMA((4,)),
        ),
        far=(0, 1),
        out_far=(0,),
    )
    edge, normed = lax.optimization_barrier((edge, normed))
    normed = call(
        edge_kernel,
        shape((4, 112, 2048), BF16),
        (),
        (edge, input_gain[None], normed),
        scratch=(pltpu.VMEM((16, 2048), BF16), pltpu.SemaphoreType.DMA((4,))),
        far=(2,),
        out_far=(0,),
        aliases={2: 0},
    )
    shard, normed = lax.optimization_barrier((shard, normed))
    own = lax.all_to_all(normed, "x", 0, 0, tiled=True).reshape(448, 2048)
    rows = lax.all_gather(shard, ("zh", "zl"), axis=0, tiled=True)
    own, rows = lax.optimization_barrier((own, rows))
    other = ring(own, "c", 1)
    state_weight = copies(rows[:, :256], "y", 4).reshape(2048, 256)
    gate_piece, rest_piece = rows[:, 256:512], rows[:, 512:]
    gate_pieces = (gate_piece,) + tuple(ring(gate_piece, "y", d) for d in (1, 2, 3))
    rest_pieces = (rest_piece,) + tuple(ring(rest_piece, "y", d) for d in (1, 2, 3))

    full = shape((768, 128), F32)
    both, sent, running = call(
        states_kernel,
        (shape((768, 256), BF16), shape((16, 160, 128), BF16), shape((8, 768), F32)),
        (core,),
        (own, other, state_weight, decay_logs, tail),
        scratch=(
            pltpu.VMEM((768, 256), BF16),
            pltpu.VMEM((8, 768), F32),
            pltpu.VMEM((160, 128), BF16),
            pltpu.SemaphoreType.DMA((18,)),
        ),
        out_far=(0, 1, 2),
    )
    inner = lax.all_to_all(sent, ("zl", "y"), 0, 0, tiled=True)
    sent = call(
        level_kernel,
        shape((4, 208, 128), BF16),
        (low,),
        (inner,),
        scratch=(pltpu.VMEM((208, 128), BF16), pltpu.SemaphoreType.DMA((4,))),
        out_far=(0,),
    )
    outer = lax.all_to_all(sent, "zh", 0, 0, tiled=True)
    convolved, moments = call(
        conv_kernel,
        (full, shape((2, 768), F32)),
        (core, y),
        (own, other, *gate_pieces, kernel_taps),
        scratch=(
            pltpu.VMEM((800, 128), F32),
            pltpu.VMEM((768, 128), F32),
            pltpu.VMEM((2, 768), F32),
            pltpu.SemaphoreType.DMA((2,)),
        ),
        out_far=(0, 1),
    )
    moments = lax.all_gather(moments, ("x", "c"))
    mine, sent, weight = call(
        mixers_kernel,
        (shape((384, 256), BF16), shape((384, 2048), BF16), shape((4, 512, 256), BF16)),
        (core, y, low, high),
        (
            own,
            other,
            *rest_pieces,
            inner,
            outer,
            both,
            running,
            start_state,
            head_gain[None],
            convolved,
            moments,
            channel_gain[None],
        ),
        scratch=(
            pltpu.VMEM((16, 2048), BF16),
            pltpu.VMEM((768, 256), BF16),
            pltpu.VMEM((768, 256), BF16),
            pltpu.VMEM((768, 256), BF16),
            pltpu.VMEM((8, 768), F32),
            pltpu.VMEM((2, 2, 64, 64), F32),
            pltpu.VMEM((1, 128), F32),
            pltpu.VMEM((768, 128), F32),
            pltpu.VMEM((8, 2, 768), F32),
            pltpu.VMEM((1, 128), F32),
            pltpu.SemaphoreType.DMA((7,)),
        ),
        far=(8, 9, 10, 11, 12, 13, 14),
    )
    arrived = ring(sent, "c", 1)
    joined = call(join_kernel, shape((384, 2048), BF16), (y,), (mine, arrived, weight))
    parts = lax.all_to_all(joined.reshape(4, 96, 2048), "x", 0, 0, tiled=True)
    return call(last_kernel, shape((96, 2048), BF16), (), (parts,))


def solution(mesh):
    split = Mesh(mesh.devices.reshape(4, 4, 4, 4, 2), ALL)
    in_specs = (
        P(ALL, None),
        P(),
        P(SP, ("x", "c")),
        P(SP, ("x", "c")),
        P(SP, ("x", "c")),
        P(SP, ("x", "c")),
        P(SP, ("x", "c")),
        P(SP, ("x", "c")),
        P(None, ("x", "c")),
        P(("x", "c")),
        P(("x", "c"), SP),
        P(None, ("x", "c"), None, None),
        P(("x", "c")),
        P(("x", "c"), SP),
        P(("x", "c"), SP),
    )

    return jax.shard_map(
        body, mesh=split, in_specs=in_specs, out_specs=P(ALL, None), check_vma=False
    )
```
